32 devices in a mesh: sp: 8 (over z, y), tp: 4 (over x, core).
Axes of the slice: x: 2, y: 2, z: 4, core: 2. Of those that a mesh axis runs over, the one named last changes fastest.
Arguments:
- tokens: bfloat16 [8192, 2048], P('sp', 'tp'), may hold values from -6 to 6
- mix_gain: float32 [2048], replicated, may hold values from 0.1 to 1.9
- query_weight: bfloat16 [2048, 1024], P('sp', 'tp'), may hold values from -0.125 to 0.125
- key_weight: bfloat16 [2048, 256], P('sp', 'tp'), may hold values from -0.125 to 0.125
- value_weight: bfloat16 [2048, 256], P('sp', 'tp'), may hold values from -0.125 to 0.125
- conv_value_weight: bfloat16 [2048, 1024], P('sp', 'tp'), may hold values from -0.125 to 0.125
- conv_gate_weight: bfloat16 [2048, 1024], P('sp', 'tp'), may hold values from -0.125 to 0.125
- query_gain: float32 [64], replicated, may hold values from 0.1 to 1.9
- key_gain: float32 [64], replicated, may hold values from 0.1 to 1.9
- sink_logit: float32 [16], P('tp'), may hold values from 3 to 7
- conv_taps: float32 [31, 1024], P(None, 'tp'), may hold values from -1 to 1
- conv_gain: float32 [1024], P('tp'), may hold values from 0.1 to 1.9
- attn_proj: bfloat16 [1024, 2048], P('tp', 'sp'), may hold values from -1.5 to 1.5
- conv_proj: bfloat16 [1024, 2048], P('tp', 'sp'), may hold values from -0.1875 to 0.1875
Outputs:
- mixed: bfloat16 [8192, 2048], P(('sp', 'tp'))
The draws below stay inside these ranges and needn't reach their ends.
All inputs are finite; a program needn't handle non-finite values.
Results may differ from the reference program's by a relative error of at most 0.0079.
Values may be sent and summed in bfloat16 or wider, within the bound.
A program may use at most 128 MiB of HBM per device.

```python
import jax
import jax.numpy as jnp
from jax import lax

MODEL_DIM = 2048
QUERY_HEADS = 16
KEY_HEADS = 4
HEAD_DIM = 64
CHANNELS = 1024
KERNEL = 31
WINDOW = 128
LOCAL_TOKENS = 1024
TOKENS = 8192
CONV_REACH = 15


def levels(key, shape, shards, low, high):
    level = 1.0
    for dim, shards_of in shards:
        heights = jax.random.uniform(jax.random.fold_in(jax.random.fold_in(key, 6), dim), (shards_of,), jnp.float32, low / len(shards), high / len(shards))
        level = level * jnp.repeat(jnp.exp(heights), shape[dim] // shards_of).reshape((-1,) + (1,) * (len(shape) - 1 - dim))
    return level


def scatter_about(rng, shape, deviation, most, cuts=(), kind=jnp.bfloat16):
    drawn = jax.random.normal(rng, shape, jnp.float32) * deviation
    if len(cuts) > 0:
        drawn = levels(rng, shape, cuts, -0.22, 0.18) * drawn
    return jnp.clip(drawn, min=-most, max=most).astype(kind)


def setup_inputs(seed: int = 0) -> dict:
    seeds = jax.random.split(jax.random.key(seed), 15)
    return {
        "tokens": scatter_about(seeds[0], (TOKENS, MODEL_DIM), 1.0, 6.0, ((0, 8), (1, 4))),
        "mix_gain": jnp.clip(1.0 + 0.18 * jax.random.normal(seeds[1], (MODEL_DIM,), jnp.float32), 0.1, 1.9),
        "query_weight": scatter_about(seeds[2], (MODEL_DIM, QUERY_HEADS * HEAD_DIM), MODEL_DIM ** -0.5, 0.125, ((0, 8), (1, 4))),
        "key_weight": scatter_about(seeds[3], (MODEL_DIM, KEY_HEADS * HEAD_DIM), MODEL_DIM ** -0.5, 0.125, ((0, 8), (1, 4))),
        "value_weight": scatter_about(seeds[4], (MODEL_DIM, KEY_HEADS * HEAD_DIM), MODEL_DIM ** -0.5, 0.125, ((0, 8), (1, 4))),
        "conv_value_weight": scatter_about(seeds[5], (MODEL_DIM, CHANNELS), MODEL_DIM ** -0.5, 0.125, ((0, 8), (1, 4))),
        "conv_gate_weight": scatter_about(seeds[6], (MODEL_DIM, CHANNELS), MODEL_DIM ** -0.5, 0.125, ((0, 8), (1, 4))),
        "query_gain": jnp.clip(1.0 + 0.18 * jax.random.normal(seeds[7], (HEAD_DIM,), jnp.float32), 0.1, 1.9),
        "key_gain": jnp.clip(1.0 + 0.18 * jax.random.normal(seeds[8], (HEAD_DIM,), jnp.float32), 0.1, 1.9),
        "sink_logit": jnp.clip(3.0 + 4.0 * jax.random.uniform(seeds[9], (QUERY_HEADS,), jnp.float32) ** levels(seeds[9], (QUERY_HEADS,), ((0, 4),), -0.2, 0.2), 3.0, 7.0),
        "conv_taps": scatter_about(seeds[10], (KERNEL, CHANNELS), KERNEL ** -0.5, 1.0, ((1, 4),), jnp.float32),
        "conv_gain": jnp.clip(1.0 + 0.18 * jax.random.normal(seeds[11], (CHANNELS,), jnp.float32), 0.1, 1.9),
        "attn_proj": scatter_about(seeds[12], (QUERY_HEADS * HEAD_DIM, MODEL_DIM), (QUERY_HEADS * HEAD_DIM // 64) ** -0.5, 1.5, ((0, 4), (1, 8))),
        "conv_proj": scatter_about(seeds[13], (CHANNELS, MODEL_DIM), CHANNELS ** -0.5, 0.1875, ((0, 4), (1, 8))),
    }


EPSILON = 0.1

def unit_rows(values, gain):
    return values * lax.rsqrt(lax.optimization_barrier(jnp.mean(values * values, axis=-1, keepdims=True)) + EPSILON) * gain

def attend(queries, keys, values, sinks, offset, total):
    scale = queries.shape[-1] ** (-0.5)
    scores = jnp.einsum('qkgd,skd->kgqs', queries.astype(jnp.float32), keys.astype(jnp.float32)) * scale
    query_pos = offset + jnp.arange(queries.shape[0], dtype=jnp.int32)
    key_pos = offset - WINDOW + jnp.arange(keys.shape[0], dtype=jnp.int32)
    allowed = (jnp.abs(key_pos[None, :] - query_pos[:, None]) <= WINDOW) & (key_pos[None, :] >= 0) & (key_pos[None, :] < total)
    weights = jnp.where(allowed, jnp.exp(scores), 0.0)
    denominator = lax.optimization_barrier(jnp.sum(weights, axis=-1, keepdims=True)) + jnp.exp(sinks).reshape(keys.shape[1], -1, 1, 1)
    shares = (weights / denominator).astype(jnp.bfloat16)
    result = jnp.einsum('kgqs,skd->qkgd', shares.astype(jnp.float32), values.astype(jnp.float32))
    return result.reshape(queries.shape[0], -1).astype(jnp.bfloat16)

def depthwise(extended, kernel_taps, count):
    result = jnp.zeros((count, kernel_taps.shape[1]), jnp.float32)
    for offset in range(kernel_taps.shape[0]):
        result = result + kernel_taps[offset] * extended[offset:offset + count].astype(jnp.float32)
    return result

def reference(tokens, mix_gain, query_weight, key_weight, value_weight, conv_value_weight, conv_gate_weight, query_gain, key_gain, sink_logit, conv_taps, conv_gain, attn_proj, conv_proj):
    total = tokens.shape[0]
    normed = unit_rows(tokens.astype(jnp.float32), mix_gain).astype(jnp.bfloat16)
    query = jnp.dot(normed, query_weight, preferred_element_type=jnp.float32)
    key_part = jnp.dot(normed, key_weight, preferred_element_type=jnp.float32)
    value_part = jnp.dot(normed, value_weight, preferred_element_type=jnp.float32)
    conv_value = jnp.dot(normed, conv_value_weight, preferred_element_type=jnp.float32)
    conv_gate = jnp.dot(normed, conv_gate_weight, preferred_element_type=jnp.float32)
    group = QUERY_HEADS // KEY_HEADS
    queries = unit_rows(query.reshape(total, KEY_HEADS, group, HEAD_DIM), query_gain).astype(jnp.bfloat16)
    keys = unit_rows(key_part.reshape(total, KEY_HEADS, HEAD_DIM), key_gain).astype(jnp.bfloat16)
    values = value_part.reshape(total, KEY_HEADS, HEAD_DIM).astype(jnp.bfloat16)
    padded_keys = jnp.pad(keys, ((WINDOW, WINDOW), (0, 0), (0, 0)))
    padded_values = jnp.pad(values, ((WINDOW, WINDOW), (0, 0), (0, 0)))

    def one_block(index):
        begin = (index * LOCAL_TOKENS).astype(jnp.int32)
        block_queries = lax.dynamic_slice_in_dim(queries, begin, LOCAL_TOKENS, 0)
        block_keys = lax.dynamic_slice_in_dim(padded_keys, begin, LOCAL_TOKENS + 2 * WINDOW, 0)
        block_values = lax.dynamic_slice_in_dim(padded_values, begin, LOCAL_TOKENS + 2 * WINDOW, 0)
        return attend(block_queries, block_keys, block_values, sink_logit, begin, total)
    attended = lax.map(one_block, jnp.arange(total // LOCAL_TOKENS, dtype=jnp.int32)).reshape(total, -1)
    gated = (conv_value * jax.nn.sigmoid(conv_gate)).astype(jnp.bfloat16)
    extended = jnp.pad(gated, ((CONV_REACH, CONV_REACH), (0, 0)))
    convolved = depthwise(extended, conv_taps, total)
    center = lax.optimization_barrier(jnp.mean(convolved, axis=1, keepdims=True))
    centered = convolved - center
    spread = lax.optimization_barrier(jnp.mean(centered * centered, axis=1, keepdims=True))
    featured = jax.nn.silu(centered * lax.rsqrt(spread + EPSILON) * conv_gain).astype(jnp.bfloat16)
    summed = jnp.dot(attended, attn_proj, preferred_element_type=jnp.float32) + jnp.dot(featured, conv_proj, preferred_element_type=jnp.float32)
    return summed.astype(jnp.bfloat16)
```

```python
import functools

import jax
import jax.numpy as jnp
from jax import lax
from jax.experimental import pallas as pl
from jax.experimental.pallas import tpu as pltpu
from jax.sharding import PartitionSpec as P

WINDOW = 128


EPSILON = 0.1


def padded(value, sides, width):
    for axis, dim in sides:
        size, length = (lax.axis_size(axis), value.shape[dim])
        up = [(i, (i + 1) % size) for i in range(size - 1)]
        down = [(j, i) for i, j in up]
        last = lax.slice_in_dim(value, length - width, length, axis=dim)
        leading = lax.slice_in_dim(value, 0, width, axis=dim)
        before = lax.ppermute(last, axis, up)
        after = lax.ppermute(leading, axis, down)
        value = jnp.concatenate([before, value, after], axis=dim)
    return value


def unit_rows(values, gain):
    return values * lax.rsqrt(jnp.mean(values * values, axis=-1, keepdims=True) + EPSILON) * gain


def attend(queries, keys, values, sinks, offset, total):
    count, local_kv, group, size = queries.shape
    scale = size ** (-0.5)
    blocks = count // WINDOW
    span = 3 * WINDOW

    def windows(rows):
        cut = rows.reshape(blocks + 2, WINDOW, local_kv, size)
        return jnp.concatenate([cut[:blocks], cut[1 : blocks + 1], cut[2:]], axis=1)

    cut_queries = queries.reshape(blocks, WINDOW, local_kv, group, size)
    scores = jnp.einsum(
        "bqkgd,bskd->bkgqs", cut_queries, windows(keys), preferred_element_type=jnp.float32
    )
    query_row = jnp.arange(WINDOW, dtype=jnp.int32)[None, :, None]
    key_row = jnp.arange(span, dtype=jnp.int32)[None, None, :] - WINDOW
    key_pos = offset + WINDOW * jnp.arange(blocks, dtype=jnp.int32)[:, None, None] + key_row
    allowed = (jnp.abs(key_row - query_row) <= WINDOW) & (key_pos >= 0) & (key_pos < total)
    weights = jnp.where(allowed[:, None, None], jnp.exp(scores * scale), 0.0)
    denominator = jnp.sum(weights, axis=-1) + jnp.exp(sinks).reshape(local_kv, group, 1)
    shares = (weights / denominator[..., None]).astype(jnp.bfloat16)
    result = jnp.einsum(
        "bkgqs,bskd->bqkgd", shares, windows(values), preferred_element_type=jnp.float32
    )
    return result.reshape(count, -1).astype(jnp.bfloat16)


def depthwise(extended, kernel_taps, count):
    result = jnp.zeros((count, kernel_taps.shape[1]), jnp.float32)
    for offset in range(kernel_taps.shape[0]):
        result = result + kernel_taps[offset] * extended[offset : offset + count]
    return result


def snake(size):
    if size % 2:
        return (lambda index: index), (lambda place: place)
    half = size // 2

    def place_of(index):
        odd = index % 2
        return (index // 2) * (1 - odd) + (size - 1 - index // 2) * odd

    def index_of(place):
        back = place // half
        return 2 * place * (1 - back) + (2 * (size - 1 - place) + 1) * back

    return place_of, index_of


def plain(size):
    return (lambda index: index), (lambda place: place)


def gather_kernel(rings, *refs):
    count = len(rings)
    shards, outs = refs[:count], refs[count : 2 * count]
    local_sem = refs[2 * count]
    sems = refs[2 * count + 1 :]
    barrier = pltpu.get_barrier_semaphore()
    plans = []
    for number, (axis, size, dim, order) in enumerate(rings):
        place_of, index_of = order(size)
        place = place_of(lax.axis_index(axis))
        at = lambda shift, p=place, f=index_of, n=size: f((p + shift + n) % n)
        plans.append((axis, size, dim, at, shards[number], outs[number], sems[2 * number : 2 * number + 2]))
        for shift in (1, -1):
            pl.semaphore_signal(
                barrier, inc=1, device_id={axis: at(shift)}, device_id_type=pl.DeviceIdType.MESH
            )

    def window(out, dim, shard, index, low, high):
        rows, columns = shard.shape
        if dim == 0:
            begin = pl.multiple_of(index * rows + low, 16)
            return out.at[pl.ds(begin, high - low), :]
        return out.at[pl.ds(low, high - low), pl.ds(pl.multiple_of(index * columns, 128), columns)]

    local = []
    for number, (axis, size, dim, at, shard, out, _) in enumerate(plans):
        copy = pltpu.make_async_copy(
            shard, window(out, dim, shard, at(0), 0, shard.shape[0]), local_sem.at[number]
        )
        copy.start()
        local.append(copy)
    pl.semaphore_wait(barrier, 2 * count)

    def hop(plan, step, way):
        axis, size, dim, at, shard, out, (send, recv) = plan
        rows = shard.shape[0]
        low, high = 0, rows
        if 2 * step == size:
            low, high = (0, rows // 2) if way == 1 else (rows // 2, rows)
        owner = at(-way * (step - 1))
        target = window(out, dim, shard, owner, low, high)
        source = shard.at[pl.ds(low, high - low), :] if step == 1 else target
        slot = 2 * (step - 1) + (way + 1) // 2
        return pltpu.make_async_remote_copy(
            src_ref=source,
            dst_ref=target,
            send_sem=send.at[slot],
            recv_sem=recv.at[slot],
            device_id={axis: at(way)},
            device_id_type=pl.DeviceIdType.MESH,
        )

    pending = {}
    steps = [(n, s) for n, plan in enumerate(plans) for s in range(1, plan[1] // 2 + 1)]
    steps.sort(key=lambda item: ((item[1] - 1) / (plans[item[0]][1] // 2), -plans[item[0]][1]))
    for number, step in steps:
        for way in (1, -1):
            if step > 1:
                pending[number, step - 1, way].wait_recv()
            copy = hop(plans[number], step, way)
            copy.start()
            pending[number, step, way] = copy
    for number, plan in enumerate(plans):
        for way in (1, -1):
            pending[number, plan[1] // 2, way].wait_recv()
    for copy in pending.values():
        copy.wait_send()
    for copy in local:
        copy.wait()


def gather_both(tokens, joined):
    tp, sp = lax.axis_size("tp"), lax.axis_size("sp")
    rings = (("tp", tp, 1, plain), ("sp", sp, 0, snake))
    sems = []
    for _, size, _, _ in rings:
        sems += [pltpu.SemaphoreType.DMA((2 * (size // 2),))] * 2
    return pl.pallas_call(
        functools.partial(gather_kernel, rings),
        out_shape=(
            jax.ShapeDtypeStruct((tokens.shape[0], tokens.shape[1] * tp), tokens.dtype),
            jax.ShapeDtypeStruct((joined.shape[0] * sp, joined.shape[1]), joined.dtype),
        ),
        in_specs=[pl.BlockSpec(memory_space=pltpu.VMEM)] * 2,
        out_specs=[pl.BlockSpec(memory_space=pl.ANY)] * 2,
        scratch_shapes=[pltpu.SemaphoreType.DMA((2,))] + sems,
        compiler_params=pltpu.CompilerParams(collective_id=0, has_side_effects=True),
    )(tokens, joined)


LANES = 128
MESH = pl.DeviceIdType.MESH


def remote(source, target, sems, where):
    return pltpu.make_async_remote_copy(
        src_ref=source,
        dst_ref=target,
        send_sem=sems[0],
        recv_sem=sems[1],
        device_id=where,
        device_id_type=MESH,
    )


def contract_last(left, right):
    return lax.dot_general(
        left, right, (((1,), (1,)), ((), ())), preferred_element_type=jnp.float32
    )


def matmul(left, right):
    return jnp.dot(left, right, preferred_element_type=jnp.float32)


def lane_index(shape):
    return lax.broadcasted_iota(jnp.int32, shape, len(shape) - 1)


def row_index(shape):
    return lax.broadcasted_iota(jnp.int32, shape, len(shape) - 2)


def aligned(value, multiple):
    return value if isinstance(value, int) else pl.multiple_of(value, multiple)


class Ring:
    def __init__(self, size, groups, sems):
        place_of, index_of = snake(size)
        place = place_of(lax.axis_index("sp"))
        self.at = lambda shift: index_of((place + shift + size) % size)
        self.half = size // 2
        self.groups = groups
        self.sems = sems
        self.copies = {}
        self.done = []
        self.queue = [
            (group, step, piece, way)
            for group, (pieces, _) in enumerate(groups)
            for step in range(1, self.half + 1)
            for piece in range(len(pieces))
            for way in (1, -1)
            if self.sent(group, step, piece, way)
        ]

    def sent(self, group, step, piece, way):
        if step < self.half:
            return True
        return step == self.half and (piece in self.groups[group][1]) == (way == 1)

    def send(self, group, step, piece, way):
        ref = self.groups[group][0][piece](self.at(-way * (step - 1)))
        copy = remote(ref, ref, next(self.sems), {"sp": self.at(way)})
        copy.start()
        self.copies[group, step, piece, way] = copy

    def first(self, group):
        for piece in range(len(self.groups[group][0])):
            for way in (1, -1):
                self.send(group, 1, piece, way)

    def advance(self, number, arrived=None):
        for _ in range(min(number, len(self.queue))):
            group, step, piece, way = self.queue.pop(0)
            self.copies[group, step, piece, way].wait_recv()
            if step < self.half and self.sent(group, step + 1, piece, way):
                self.send(group, step + 1, piece, way)
            if arrived is not None:
                arrived(group, step, piece, way)

    def through(self, group, step, arrived=None):
        number = sum(1 for item in self.queue if item[:2] <= (group, step))
        self.advance(number, arrived)

    def slot(self, step, way):
        return 2 * self.half - 1 if step == self.half else 2 * step - (1 if way == 1 else 0)

    def owner(self, slot):
        step = (slot + 1) // 2
        return self.at(-step if slot % 2 else step)


def fused_kernel(
    sp,
    tokens,
    query_w,
    key_w,
    value_w,
    conv_value_w,
    conv_gate_w,
    attn_p,
    conv_p,
    gains,
    sinks,
    taps,
    out,
    whole,
    normed,
    query_all,
    kv_all,
    value_all,
    gate_all,
    attn_all,
    conv_all,
    attn_other,
    conv_other,
    spread_heads,
    band,
    eye,
    gated,
    edge_out,
    edge_in,
    convolved,
    stat_out,
    stat_in,
    stat_rows,
    queries,
    key_low,
    key_high,
    value_low,
    value_high,
    halo_out,
    halo_in,
    mixers,
    mixers_other,
    part_out,
    part_in,
    near_sum,
    local_sem,
    send_sem,
    recv_sem,
):
    count, features = tokens.shape
    depth, width = query_w.shape
    model = features * 4
    columns = attn_p.shape[1]
    block = count // 4
    pad = gated.shape[1] - count
    reach = (taps.shape[0] - 1) // 2
    half_pad = pad // 2
    head = LANES // 2
    channels = taps.shape[1]
    s, t = lax.axis_index("sp"), lax.axis_index("tp")
    a, c = t // 2, t % 2
    inner, outer = t + 1 - 2 * c, (t + 2) % 4
    cross = outer + 1 - 2 * c
    number = iter(range(10**6))

    def sem_pairs():
        while True:
            i = next(number)
            yield send_sem.at[i], recv_sem.at[i]

    sems = sem_pairs()
    sent = []

    def push(source, target, where):
        copy = remote(source, target, next(sems), where)
        copy.start()
        sent.append(copy)
        return copy

    def rows_of(owner, low, high):
        return pl.ds(pl.multiple_of(owner * depth + low, 16), high - low)

    def kv_columns(owner):
        return pl.ds(pl.multiple_of(owner * depth, LANES), depth)

    cut = depth * 3 // 4
    ring = Ring(
        sp,
        (
            (
                (
                    lambda o: value_all.at[rows_of(o, 0, depth), :],
                    lambda o: gate_all.at[rows_of(o, 0, depth), :],
                ),
                (0,),
            ),
            (
                (
                    lambda o: query_all.at[rows_of(o, 0, cut), :],
                    lambda o: query_all.at[rows_of(o, cut, depth), :],
                    lambda o: kv_all.at[:, kv_columns(o)],
                ),
                (0,),
            ),
            ((lambda o: attn_all.at[o], lambda o: conv_all.at[o]), (0,)),
        ),
        sems,
    )

    local = []
    for i, (source, target) in enumerate(
        (
            (tokens, whole.at[t]),
            (conv_value_w, value_all.at[rows_of(s, 0, depth), :]),
            (conv_gate_w, gate_all.at[rows_of(s, 0, depth), :]),
            (query_w, query_all.at[rows_of(s, 0, depth), :]),
            (key_w, kv_all.at[pl.ds(0, head), kv_columns(s)]),
            (value_w, kv_all.at[pl.ds(head, head), kv_columns(s)]),
            (attn_p, attn_all.at[s]),
            (conv_p, conv_all.at[s]),
        )
    ):
        copy = pltpu.make_async_copy(source, target, local_sem.at[i])
        copy.start()
        local.append(copy)

    barrier = pltpu.get_barrier_semaphore()
    following, preceding = (s + 1) % sp, (s + sp - 1) % sp
    near_devices = [{"sp": ring.at(1)}, {"sp": ring.at(-1)}, {"sp": following}, {"sp": preceding}]
    near_devices += [{"tp": inner}, {"tp": outer}, {"tp": cross}]
    for where in near_devices:
        pl.semaphore_signal(barrier, inc=1, device_id=where, device_id_type=MESH)
    for copy in local:
        copy.wait()
    pl.semaphore_wait(barrier, len(near_devices))

    ring.first(0)
    mine = [whole.at[t, pl.ds(i * block, block), :] for i in range(4)]
    over = [push(ref, ref, {"tp": outer}) for ref in mine]
    beside = push(whole.at[t], whole.at[t], {"tp": inner})

    square = (width, width)
    spread_heads[...] = jnp.where(
        row_index(square) // head == lane_index(square) // head, 1.0 / head, 0.0
    ).astype(jnp.bfloat16)
    tile = (LANES, LANES)
    row, lane = row_index(tile), lane_index(tile)
    band[0] = (lane >= row).astype(jnp.float32)
    band[1] = (lane <= row).astype(jnp.float32)
    eye[...] = (lane == row).astype(jnp.float32)
    ones_low = jnp.where(lane < head, 1.0, 0.0)
    for i in range(value_low.shape[0] // LANES):
        rows = pl.ds(i * LANES, LANES)
        low, high = ones_low, 1.0 - ones_low
        if i == 0:
            low, high = (jnp.where(s > 0, v, 0.0) for v in (low, high))
        if i == value_low.shape[0] // LANES - 1:
            low, high = (jnp.where(s < sp - 1, v, 0.0) for v in (low, high))
        value_low[rows, LANES:] = low.astype(jnp.bfloat16)
        value_high[rows, LANES:] = high.astype(jnp.bfloat16)

    step_rows = 64

    def norm_rows(i, carry):
        rows = pl.ds(pl.multiple_of(i * step_rows, step_rows), step_rows)
        total = jnp.zeros((step_rows, LANES), jnp.float32)
        for j in range(4):
            for k in range(features // LANES):
                x = whole[j, rows, k * LANES : (k + 1) * LANES].astype(jnp.float32)
                total = total + x * x
        mean = jnp.sum(total, axis=1, keepdims=True) * (1.0 / model)
        scale = jnp.broadcast_to(lax.rsqrt(mean + EPSILON), (step_rows, LANES))
        for j in range(4):
            for k in range(features // LANES):
                x = whole[j, rows, k * LANES : (k + 1) * LANES].astype(jnp.float32)
                at = j * features + k * LANES
                gain = gains[:, at : at + LANES]
                normed[rows, at : at + LANES] = (x * scale * gain).astype(jnp.bfloat16)
        return carry

    def norm_block(i):
        over[i].wait_recv()
        source = whole.at[outer, pl.ds(i * block, block), :]
        forwards.append(push(source, source, {"tp": inner}))
        if i == 0:
            beside.wait_recv()
        forwards[i].wait_recv()
        per = block // step_rows
        lax.fori_loop(i * per, (i + 1) * per, norm_rows, 0)

    forwards = []
    half = ring.half
    ring.through(0, 1)
    norm_block(0)
    for step in range(2, half):
        ring.through(0, step)
        if step == half - 1:
            ring.first(1)
        if step == 2:
            norm_block(1)
        if step == 3:
            norm_block(2)
    for i in range(len(forwards), 4):
        norm_block(i)
    ring.through(0, half)
    ring.through(1, 1)

    def gate_block(i):
        left = normed[i * block : (i + 1) * block, :]
        value = matmul(left, value_all[...])
        gate = matmul(left, gate_all[...])
        result = (value * jax.nn.sigmoid(gate)).astype(jnp.bfloat16)
        wide = result.astype(jnp.float32)
        for j in range(channels // LANES):
            gated[j, i * block + half_pad : (i + 1) * block + half_pad, :] = wide[
                :, j * LANES : (j + 1) * LANES
            ]
        if i == 0:
            edge_out[0] = result[:half_pad, :]
        if i == 3:
            edge_out[1] = result[block - half_pad :, :]

    gate_block(0)
    gate_block(3)
    edges = [
        push(edge_out.at[1], edge_in.at[0], {"sp": following}),
        push(edge_out.at[0], edge_in.at[1], {"sp": preceding}),
    ]
    gate_block(1)
    ring.advance(2)
    gate_block(2)
    ring.advance(2)

    def conv_rows(i, carry):
        start = i * LANES
        parts = []
        for j in range(channels // LANES):
            lanes = slice(j * LANES, (j + 1) * LANES)
            total = jnp.zeros((LANES, LANES), jnp.float32)
            first = half_pad - reach
            for shift in range(8):
                offsets = [o for o in range(first, first + 2 * reach + 1) if o % 8 == shift]
                high = offsets[-1] - shift
                rows = gated[j, pl.ds(start + shift, LANES + high), :]
                for o in offsets:
                    tap = taps[o - first : o - first + 1, lanes]
                    total = total + tap * rows[o - shift : o - shift + LANES]
            convolved[pl.ds(pl.multiple_of(start, LANES), LANES), lanes] = total
            parts.append(total)
        mean = jnp.sum(sum(parts[1:], parts[0]), axis=1, keepdims=True) * (1.0 / channels)
        squares = [jnp.square(part - mean) for part in parts]
        square_sum = jnp.sum(sum(squares[1:], squares[0]), axis=1, keepdims=True)
        stat_out[pl.ds(i, 1), :] = jnp.sum(mean * eye[...], axis=0, keepdims=True)
        stat_out[pl.ds(i + count // LANES, 1), :] = jnp.sum(
            square_sum * eye[...], axis=0, keepdims=True
        )
        return carry

    blocks = count // LANES
    quarter = blocks // 4
    lax.fori_loop(quarter, 2 * quarter, conv_rows, 0)
    ring.through(1, 2)
    lax.fori_loop(2 * quarter, 3 * quarter, conv_rows, 0)
    for side, edge in enumerate(edges):
        edge.wait_recv()
        inside = s > 0 if side == 0 else s < sp - 1
        values = jnp.where(inside, edge_in[side].astype(jnp.float32), 0.0)
        start = 0 if side == 0 else count + half_pad
        for j in range(channels // LANES):
            gated[j, start : start + half_pad, :] = values[:, j * LANES : (j + 1) * LANES]
    lax.fori_loop(0, quarter, conv_rows, 0)
    ring.advance(2)
    lax.fori_loop(3 * quarter, blocks, conv_rows, 0)
    stats = [
        push(stat_out, stat_in.at[i], {"tp": peer}) for i, peer in enumerate((inner, outer, cross))
    ]
    ring.through(1, half - 1)
    ring.first(2)
    for stat in stats:
        stat.wait_recv()
    every = [stat_out[...]] + [stat_in[i] for i in range(3)]
    means = [v[:blocks] for v in every]
    center = (means[0] + means[1] + means[2] + means[3]) * 0.25
    spread = sum(v[blocks:] for v in every) + channels * sum(jnp.square(m - center) for m in means)
    stat_rows[:blocks] = center
    stat_rows[blocks:] = lax.rsqrt(spread * (1.0 / (channels * 4)) + EPSILON)

    def feature_rows(i, carry):
        rows = pl.ds(pl.multiple_of(i * LANES, LANES), LANES)
        middle = jnp.sum(stat_rows[pl.ds(i, 1), :] * eye[...], axis=1, keepdims=True)
        scale = jnp.sum(stat_rows[pl.ds(i + blocks, 1), :] * eye[...], axis=1, keepdims=True)
        for j in range(channels // LANES):
            lanes = slice(j * LANES, (j + 1) * LANES)
            gain = gains[:, model + j * LANES : model + (j + 1) * LANES]
            value = (convolved[rows, lanes] - middle) * scale * gain
            mixers[rows, width + j * LANES : width + (j + 1) * LANES] = (
                value * jax.nn.sigmoid(value)
            ).astype(jnp.bfloat16)
        return carry

    lax.fori_loop(0, blocks, feature_rows, 0)
    far, near = (1 - a) * 2, a * 2
    give = [
        pl.ds(pl.multiple_of((base + 1 - c) * block, block), block) for base in (far, near)
    ]
    keep = [pl.ds(pl.multiple_of((base + c) * block, block), block) for base in (far, near)]
    given_features = [
        push(mixers.at[give[f], width:], mixers_other.at[f, :, width:], {"tp": inner})
        for f in range(2)
    ]
    ring.through(1, half)

    base = model + channels

    def key_value_block(i):
        keys, vals = kv_all[:head, :], kv_all[head:, :]
        weights = jnp.concatenate([keys, vals, vals, keys], axis=0)
        part = contract_last(normed[i * block : (i + 1) * block, :], weights)
        scaled = part * head_scale(part) * gains[:, base + width : base + 2 * width]
        lanes = lane_index(part.shape)
        result = jnp.where((lanes < head) | (lanes >= 3 * head), scaled, part)
        low, high = result[:, :LANES], result[:, LANES:]
        is_low = lane_index(low.shape) < head
        rows = slice(WINDOW + i * block, WINDOW + (i + 1) * block)
        store_key_values(rows, low, high, is_low)
        if i == 0:
            halo_out[0] = low[:WINDOW].astype(jnp.bfloat16)
        if i == 3:
            halo_out[1] = low[block - WINDOW :].astype(jnp.bfloat16)

    def head_scale(part):
        squares = part * part
        high = squares.astype(jnp.bfloat16)
        low = (squares - high.astype(jnp.float32)).astype(jnp.bfloat16)
        mean = matmul(high, spread_heads[...]) + matmul(low, spread_heads[...])
        return lax.rsqrt(mean + EPSILON)

    def store_key_values(rows, low, high, is_low):
        key_low[rows, :] = jnp.where(is_low, low, 0.0).astype(jnp.bfloat16)
        value_high[rows, :LANES] = jnp.where(is_low, 0.0, low).astype(jnp.bfloat16)
        value_low[rows, :LANES] = jnp.where(is_low, high, 0.0).astype(jnp.bfloat16)
        key_high[rows, :] = jnp.where(is_low, 0.0, high).astype(jnp.bfloat16)

    def query_block(rows):
        part = matmul(normed[rows, :], query_all[...])
        queries[rows, :] = (part * head_scale(part) * gains[:, base : base + width]).astype(
            jnp.bfloat16
        )

    def arrived(group, step, piece, way):
        slot = ring.slot(step, way)
        share(slot, piece)

    shared = {}

    def share(slot, piece):
        owner = ring.owner(slot)
        whole_ref, other_ref = ((attn_all, attn_other), (conv_all, conv_other))[piece]
        shared[slot, piece] = push(whole_ref.at[owner], other_ref.at[owner], {"tp": inner})

    key_value_block(0)
    key_value_block(3)
    halos = [
        push(halo_out.at[1], halo_in.at[0], {"sp": following}),
        push(halo_out.at[0], halo_in.at[1], {"sp": preceding}),
    ]
    share(0, 0)
    share(0, 1)
    key_value_block(1)
    ring.advance(2, arrived)
    key_value_block(2)
    ring.advance(2, arrived)
    query_block(give[0])
    query_block(keep[0])
    for side, halo in enumerate(halos):
        halo.wait_recv()
        inside = s > 0 if side == 0 else s < sp - 1
        low = halo_in[side].astype(jnp.float32)
        high = pltpu.roll(low, head, 1)
        is_low = lane_index(low.shape) < head
        start = 0 if side == 0 else WINDOW + count
        rows = slice(start, start + WINDOW)
        key_low[rows, :] = jnp.where(is_low, low, 0.0).astype(jnp.bfloat16)
        key_high[rows, :] = jnp.where(is_low, 0.0, high).astype(jnp.bfloat16)
        value_low[rows, :LANES] = jnp.where(is_low & inside, high, 0.0).astype(jnp.bfloat16)
        value_high[rows, :LANES] = jnp.where(is_low | ~inside, 0.0, low).astype(jnp.bfloat16)

    exponent = head ** (-0.5) * 1.4426950408889634
    head_lanes = lane_index((1, LANES)) < head
    sink_rows = [
        jnp.exp(jnp.where(head_lanes, sinks[2 * i], sinks[2 * i + 1])) for i in range(2)
    ]

    def attend_rows(first):
        def body(i, carry):
            start = pl.multiple_of(first + i * WINDOW, WINDOW)
            rows = pl.ds(start, WINDOW)
            left = jnp.concatenate([queries[rows, :LANES], queries[rows, LANES:]], axis=0)
            shares, vals = [], []
            for j in range(3):
                span = pl.ds(pl.multiple_of(start + j * WINDOW, WINDOW), WINDOW)
                right = jnp.concatenate([key_low[span, :], key_high[span, :]], axis=0)
                weight = jnp.exp2(contract_last(left, right) * exponent)
                if j != 1:
                    mask = band[j // 2]
                    mask = jnp.concatenate([mask, mask], axis=0)
                    weight = weight * jnp.concatenate([mask, mask], axis=1)
                shares.append(weight.astype(jnp.bfloat16))
                vals += [value_low[span, :], value_high[span, :]]
            total = matmul(jnp.concatenate(shares, axis=1), jnp.concatenate(vals, axis=0))
            for j in range(2):
                piece = total[j * WINDOW : (j + 1) * WINDOW]
                mixers[rows, j * LANES : (j + 1) * LANES] = (
                    piece[:, :LANES] / (piece[:, LANES:] + sink_rows[j])
                ).astype(jnp.bfloat16)
            return carry

        lax.fori_loop(0, block // WINDOW, body, 0)

    def attend_half(f, base):
        attend_rows((base + 1 - c) * block)
        copy = push(mixers.at[give[f], :width], mixers_other.at[f, :, :width], {"tp": inner})
        ring.advance(2, arrived)
        attend_rows((base + c) * block)
        return copy

    given_heads = attend_half(0, far)
    ring.advance(2, arrived)

    def project(f, slot):
        owner = ring.owner(slot)
        left = jnp.concatenate([mixers[keep[f], :], mixers_other[f]], axis=1)
        right = jnp.concatenate(
            [attn_all[owner], conv_all[owner], attn_other[owner], conv_other[owner]], axis=0
        )
        return matmul(left, right)

    parts = []

    def send_part(slot):
        for piece in range(2):
            shared[slot, piece].wait_recv()
        part_out[slot] = project(0, slot).astype(jnp.bfloat16)
        parts.append(push(part_out.at[slot], part_in.at[slot], {"tp": outer}))

    given_features[0].wait_recv()
    given_heads.wait_recv()

    def ready():
        return [k for k in range(len(parts), sp) if all((k, p) in shared for p in range(2))]

    def send_ready(most=sp):
        for k in ready()[:most]:
            if k == len(parts):
                send_part(k)

    send_ready()
    query_block(give[1])
    ring.advance(2, arrived)
    query_block(keep[1])
    ring.advance(2, arrived)
    send_ready()
    given_heads = attend_half(1, near)
    ring.advance(2, arrived)
    send_ready()
    given_features[1].wait_recv()
    given_heads.wait_recv()
    for slot in range(len(parts)):
        near_sum[slot] = project(1, slot)
    done = len(parts)
    while len(parts) < sp:
        ring.advance(2, arrived)
        send_ready()
    for slot in range(done, sp):
        near_sum[slot] = project(1, slot)
    for slot in range(sp):
        parts[slot].wait_recv()
        owner = ring.owner(slot)
        out[:, pl.ds(pl.multiple_of(owner * columns, LANES), columns)] = (
            near_sum[slot] + part_in[slot].astype(jnp.float32)
        ).astype(jnp.bfloat16)
    for copy in sent:
        copy.wait_send()
    for copy in ring.copies.values():
        copy.wait_send()


def fits(sp, tp, tokens, query_weight, key_weight, conv_weight, attn_proj, taps, head):
    return (
        tp == 4
        and sp % 2 == 0
        and sp >= 6
        and tokens.shape[0] % (4 * 2 * WINDOW) == 0
        and tokens.shape[1] % LANES == 0
        and WINDOW == LANES
        and 2 * head == LANES
        and key_weight.shape[1] == head
        and query_weight.shape[1] == 4 * head
        and conv_weight.shape[1] == 4 * head
        and query_weight.shape[0] % LANES == 0
        and attn_proj.shape[1] % LANES == 0
        and taps.shape[0] <= 31
    )


def fused(
    tokens,
    mix_gain,
    query_weight,
    key_weight,
    value_weight,
    conv_value_weight,
    conv_gate_weight,
    query_gain,
    key_gain,
    sink_logit,
    conv_taps,
    conv_gain,
    attn_proj,
    conv_proj,
):
    sp = lax.axis_size("sp")
    count, features = tokens.shape
    model = features * 4
    depth, width = query_weight.shape
    head = query_gain.shape[0]
    channels = conv_taps.shape[1]
    columns = attn_proj.shape[1]
    block = count // 4
    plain_lanes = jnp.ones((2 * head,), jnp.float32)
    gains = jnp.concatenate(
        [mix_gain, conv_gain] + [query_gain] * 4 + [key_gain, plain_lanes, key_gain]
    ).reshape(1, -1)
    bf16, f32 = jnp.bfloat16, jnp.float32
    copies = 160
    half_pad = 16
    scratch = [
        pltpu.VMEM((4, count, features), bf16),
        pltpu.VMEM((count, model), bf16),
        pltpu.VMEM((model, width), bf16),
        pltpu.VMEM((2 * head, model), bf16),
        pltpu.VMEM((model, channels), bf16),
        pltpu.VMEM((model, channels), bf16),
        pltpu.VMEM((sp, width, columns), bf16),
        pltpu.VMEM((sp, channels, columns), bf16),
        pltpu.VMEM((sp, width, columns), bf16),
        pltpu.VMEM((sp, channels, columns), bf16),
        pltpu.VMEM((width, width), bf16),
        pltpu.VMEM((2, LANES, LANES), f32),
        pltpu.VMEM((LANES, LANES), f32),
        pltpu.VMEM((channels // LANES, count + 2 * half_pad, LANES), f32),
        pltpu.VMEM((2, half_pad, channels), bf16),
        pltpu.VMEM((2, half_pad, channels), bf16),
        pltpu.VMEM((count, channels), f32),
        pltpu.VMEM((2 * count // LANES, LANES), f32),
        pltpu.VMEM((3, 2 * count // LANES, LANES), f32),
        pltpu.VMEM((2 * count // LANES, LANES), f32),
        pltpu.VMEM((count, width), bf16),
        pltpu.VMEM((count + 2 * WINDOW, LANES), bf16),
        pltpu.VMEM((count + 2 * WINDOW, LANES), bf16),
        pltpu.VMEM((count + 2 * WINDOW, 2 * LANES), bf16),
        pltpu.VMEM((count + 2 * WINDOW, 2 * LANES), bf16),
        pltpu.VMEM((2, WINDOW, LANES), bf16),
        pltpu.VMEM((2, WINDOW, LANES), bf16),
        pltpu.VMEM((count, width + channels), bf16),
        pltpu.VMEM((2, block, width + channels), bf16),
        pltpu.VMEM((sp, block, columns), bf16),
        pltpu.VMEM((sp, block, columns), bf16),
        pltpu.VMEM((sp, block, columns), f32),
        pltpu.SemaphoreType.DMA((8,)),
        pltpu.SemaphoreType.DMA((copies,)),
        pltpu.SemaphoreType.DMA((copies,)),
    ]
    anywhere = pl.BlockSpec(memory_space=pl.ANY)
    vmem = pl.BlockSpec(memory_space=pltpu.VMEM)
    return pl.pallas_call(
        functools.partial(fused_kernel, sp),
        out_shape=jax.ShapeDtypeStruct((block, model), bf16),
        in_specs=[anywhere] * 8 + [vmem, pl.BlockSpec(memory_space=pltpu.SMEM), vmem],
        out_specs=vmem,
        scratch_shapes=scratch,
        compiler_params=pltpu.CompilerParams(
            collective_id=1, has_side_effects=True, vmem_limit_bytes=56 * 2**20
        ),
    )(
        tokens,
        query_weight,
        key_weight.T,
        value_weight.T,
        conv_value_weight,
        conv_gate_weight,
        attn_proj,
        conv_proj,
        gains,
        sink_logit,
        conv_taps,
    )


def on_device(
    tokens,
    mix_gain,
    query_weight,
    key_weight,
    value_weight,
    conv_value_weight,
    conv_gate_weight,
    query_gain,
    key_gain,
    sink_logit,
    conv_taps,
    conv_gain,
    attn_proj,
    conv_proj,
):
    if fits(
        lax.axis_size("sp"),
        lax.axis_size("tp"),
        tokens,
        query_weight,
        key_weight,
        conv_value_weight,
        attn_proj,
        conv_taps,
        query_gain.shape[0],
    ):
        return fused(
            tokens,
            mix_gain,
            query_weight,
            key_weight,
            value_weight,
            conv_value_weight,
            conv_gate_weight,
            query_gain,
            key_gain,
            sink_logit,
            conv_taps,
            conv_gain,
            attn_proj,
            conv_proj,
        )
    count = tokens.shape[0]
    shards = (query_weight, conv_value_weight, conv_gate_weight, key_weight, value_weight)
    whole, joined = gather_both(tokens, jnp.concatenate(shards, axis=1))
    normed = unit_rows(whole.astype(jnp.float32), mix_gain).astype(jnp.bfloat16)
    product = jnp.dot(normed, joined, preferred_element_type=jnp.float32)
    cuts = []
    for shard in shards[:-1]:
        cuts.append((cuts[-1] if cuts else 0) + shard.shape[1])
    query, conv_value, conv_gate, key_part, value_part = jnp.split(product, cuts, axis=1)
    head_size = query_gain.shape[0]
    local_kv = key_part.shape[1] // head_size
    group = query.shape[1] // head_size // local_kv
    queries = unit_rows(query.reshape(count, local_kv, group, head_size), query_gain).astype(
        jnp.bfloat16
    )
    keys_normed = (
        unit_rows(key_part.reshape(count, local_kv, head_size), key_gain)
        .astype(jnp.bfloat16)
        .reshape(count, -1)
    )
    values_cast = value_part.astype(jnp.bfloat16)
    gated = (conv_value * jax.nn.sigmoid(conv_gate)).astype(jnp.bfloat16)
    reach = (conv_taps.shape[0] - 1) // 2
    kv_width = keys_normed.shape[1]
    paired = jnp.concatenate([keys_normed, values_cast], axis=1)
    extended = padded(paired, (("sp", 0),), WINDOW)
    key_rows = extended[:, :kv_width]
    value_rows = extended[:, kv_width:]
    conv_rows = padded(gated, (("sp", 0),), reach)
    offset = lax.axis_index("sp") * count
    total = count * lax.axis_size("sp")
    span_rows = key_rows.shape[0]
    attended = attend(
        queries,
        key_rows.reshape(span_rows, local_kv, head_size),
        value_rows.reshape(span_rows, local_kv, head_size),
        sink_logit,
        offset,
        total,
    )
    convolved = depthwise(conv_rows, conv_taps, count)
    channels, tp = conv_taps.shape[1], lax.axis_size("tp")
    local_mean = jnp.mean(convolved, axis=1)
    local_square = jnp.sum(jnp.square(convolved - local_mean[:, None]), axis=1)
    slot = (jnp.arange(tp) == lax.axis_index("tp")).astype(jnp.float32)[:, None, None]
    every = lax.psum(slot * jnp.stack([local_mean, local_square])[None], "tp")
    center = jnp.mean(every[:, 0], axis=0)
    spread = jnp.sum(every[:, 1] + channels * jnp.square(every[:, 0] - center), axis=0)
    spread = spread / (channels * tp)
    centered = convolved - center[:, None]
    featured = jax.nn.silu(centered * lax.rsqrt(spread[:, None] + EPSILON) * conv_gain).astype(
        jnp.bfloat16
    )
    stacked, _ = lax.optimization_barrier((jnp.concatenate([attn_proj, conv_proj], axis=0), joined))
    proj_full = lax.all_gather(stacked, "sp", axis=1, tiled=True)
    mixers = jnp.concatenate([attended, featured], axis=1)
    partial = jnp.dot(mixers, proj_full, preferred_element_type=jnp.float32).astype(jnp.bfloat16)
    return lax.psum_scatter(partial, "tp", scatter_dimension=0, tiled=True)


def solution(mesh):
    placed = (
        P("sp", "tp"),
        P(),
        P("sp", "tp"),
        P("sp", "tp"),
        P("sp", "tp"),
        P("sp", "tp"),
        P("sp", "tp"),
        P(),
        P(),
        P("tp"),
        P(None, "tp"),
        P("tp"),
        P("tp", "sp"),
        P("tp", "sp"),
    )
    return jax.shard_map(
        on_device, mesh=mesh, in_specs=placed, out_specs=P(("sp", "tp"), None), check_vma=False
    )
```

```python
import functools
import types

import jax
import jax.numpy as jnp
from jax import lax
from jax.experimental import pallas as pl
from jax.experimental.pallas import tpu as pltpu
from jax.sharding import PartitionSpec as P

WINDOW = 128


EPSILON = 0.1


def padded(value, sides, width):
    for axis, dim in sides:
        size, length = (lax.axis_size(axis), value.shape[dim])
        up = [(i, (i + 1) % size) for i in range(size - 1)]
        down = [(j, i) for i, j in up]
        last = lax.slice_in_dim(value, length - width, length, axis=dim)
        leading = lax.slice_in_dim(value, 0, width, axis=dim)
        before = lax.ppermute(last, axis, up)
        after = lax.ppermute(leading, axis, down)
        value = jnp.concatenate([before, value, after], axis=dim)
    return value


def unit_rows(values, gain):
    return values * lax.rsqrt(jnp.mean(values * values, axis=-1, keepdims=True) + EPSILON) * gain


def attend(queries, keys, values, sinks, offset, total):
    count, local_kv, group, size = queries.shape
    scale = size ** (-0.5)
    blocks = count // WINDOW
    span = 3 * WINDOW

    def windows(rows):
        cut = rows.reshape(blocks + 2, WINDOW, local_kv, size)
        return jnp.concatenate([cut[:blocks], cut[1 : blocks + 1], cut[2:]], axis=1)

    cut_queries = queries.reshape(blocks, WINDOW, local_kv, group, size)
    scores = jnp.einsum(
        "bqkgd,bskd->bkgqs", cut_queries, windows(keys), preferred_element_type=jnp.float32
    )
    query_row = jnp.arange(WINDOW, dtype=jnp.int32)[None, :, None]
    key_row = jnp.arange(span, dtype=jnp.int32)[None, None, :] - WINDOW
    key_pos = offset + WINDOW * jnp.arange(blocks, dtype=jnp.int32)[:, None, None] + key_row
    allowed = (jnp.abs(key_row - query_row) <= WINDOW) & (key_pos >= 0) & (key_pos < total)
    weights = jnp.where(allowed[:, None, None], jnp.exp(scores * scale), 0.0)
    denominator = jnp.sum(weights, axis=-1) + jnp.exp(sinks).reshape(local_kv, group, 1)
    shares = (weights / denominator[..., None]).astype(jnp.bfloat16)
    result = jnp.einsum(
        "bkgqs,bskd->bqkgd", shares, windows(values), preferred_element_type=jnp.float32
    )
    return result.reshape(count, -1).astype(jnp.bfloat16)


def depthwise(extended, kernel_taps, count):
    result = jnp.zeros((count, kernel_taps.shape[1]), jnp.float32)
    for offset in range(kernel_taps.shape[0]):
        result = result + kernel_taps[offset] * extended[offset : offset + count]
    return result


def snake(size):
    if size % 2:
        return (lambda index: index), (lambda place: place)
    half = size // 2

    def place_of(index):
        odd = index % 2
        return (index // 2) * (1 - odd) + (size - 1 - index // 2) * odd

    def index_of(place):
        back = place // half
        return 2 * place * (1 - back) + (2 * (size - 1 - place) + 1) * back

    return place_of, index_of


def plain(size):
    return (lambda index: index), (lambda place: place)


def gather_kernel(rings, *refs):
    count = len(rings)
    shards, outs = refs[:count], refs[count : 2 * count]
    local_sem = refs[2 * count]
    sems = refs[2 * count + 1 :]
    barrier = pltpu.get_barrier_semaphore()
    plans = []
    for number, (axis, size, dim, order) in enumerate(rings):
        place_of, index_of = order(size)
        place = place_of(lax.axis_index(axis))
        at = lambda shift, p=place, f=index_of, n=size: f((p + shift + n) % n)
        plans.append((axis, size, dim, at, shards[number], outs[number], sems[2 * number : 2 * number + 2]))
        for shift in (1, -1):
            pl.semaphore_signal(
                barrier, inc=1, device_id={axis: at(shift)}, device_id_type=pl.DeviceIdType.MESH
            )

    def window(out, dim, shard, index, low, high):
        rows, columns = shard.shape
        if dim == 0:
            begin = pl.multiple_of(index * rows + low, 16)
            return out.at[pl.ds(begin, high - low), :]
        return out.at[pl.ds(low, high - low), pl.ds(pl.multiple_of(index * columns, 128), columns)]

    local = []
    for number, (axis, size, dim, at, shard, out, _) in enumerate(plans):
        copy = pltpu.make_async_copy(
            shard, window(out, dim, shard, at(0), 0, shard.shape[0]), local_sem.at[number]
        )
        copy.start()
        local.append(copy)
    pl.semaphore_wait(barrier, 2 * count)

    def hop(plan, step, way):
        axis, size, dim, at, shard, out, (send, recv) = plan
        rows = shard.shape[0]
        low, high = 0, rows
        if 2 * step == size:
            low, high = (0, rows // 2) if way == 1 else (rows // 2, rows)
        owner = at(-way * (step - 1))
        target = window(out, dim, shard, owner, low, high)
        source = shard.at[pl.ds(low, high - low), :] if step == 1 else target
        slot = 2 * (step - 1) + (way + 1) // 2
        return pltpu.make_async_remote_copy(
            src_ref=source,
            dst_ref=target,
            send_sem=send.at[slot],
            recv_sem=recv.at[slot],
            device_id={axis: at(way)},
            device_id_type=pl.DeviceIdType.MESH,
        )

    pending = {}
    steps = [(n, s) for n, plan in enumerate(plans) for s in range(1, plan[1] // 2 + 1)]
    steps.sort(key=lambda item: ((item[1] - 1) / (plans[item[0]][1] // 2), -plans[item[0]][1]))
    for number, step in steps:
        for way in (1, -1):
            if step > 1:
                pending[number, step - 1, way].wait_recv()
            copy = hop(plans[number], step, way)
            copy.start()
            pending[number, step, way] = copy
    for number, plan in enumerate(plans):
        for way in (1, -1):
            pending[number, plan[1] // 2, way].wait_recv()
    for copy in pending.values():
        copy.wait_send()
    for copy in local:
        copy.wait()


def gather_both(tokens, joined):
    tp, sp = lax.axis_size("tp"), lax.axis_size("sp")
    rings = (("tp", tp, 1, plain), ("sp", sp, 0, snake))
    sems = []
    for _, size, _, _ in rings:
        sems += [pltpu.SemaphoreType.DMA((2 * (size // 2),))] * 2
    return pl.pallas_call(
        functools.partial(gather_kernel, rings),
        out_shape=(
            jax.ShapeDtypeStruct((tokens.shape[0], tokens.shape[1] * tp), tokens.dtype),
            jax.ShapeDtypeStruct((joined.shape[0] * sp, joined.shape[1]), joined.dtype),
        ),
        in_specs=[pl.BlockSpec(memory_space=pltpu.VMEM)] * 2,
        out_specs=[pl.BlockSpec(memory_space=pl.ANY)] * 2,
        scratch_shapes=[pltpu.SemaphoreType.DMA((2,))] + sems,
        compiler_params=pltpu.CompilerParams(collective_id=0, has_side_effects=True),
    )(tokens, joined)


LANES = 128
MESH = pl.DeviceIdType.MESH


def remote(source, target, sems, where):
    return pltpu.make_async_remote_copy(
        src_ref=source,
        dst_ref=target,
        send_sem=sems[0],
        recv_sem=sems[1],
        device_id=where,
        device_id_type=MESH,
    )


def contract_last(left, right):
    return lax.dot_general(
        left, right, (((1,), (1,)), ((), ())), preferred_element_type=jnp.float32
    )


def matmul(left, right):
    return jnp.dot(left, right, preferred_element_type=jnp.float32)


def lane_index(shape):
    return lax.broadcasted_iota(jnp.int32, shape, len(shape) - 1)


def row_index(shape):
    return lax.broadcasted_iota(jnp.int32, shape, len(shape) - 2)


def aligned(value, multiple):
    return value if isinstance(value, int) else pl.multiple_of(value, multiple)


class Ring:
    def __init__(self, size, groups, sems):
        place_of, index_of = snake(size)
        place = place_of(lax.axis_index("sp"))
        self.at = lambda shift: index_of((place + shift + size) % size)
        self.half = size // 2
        self.groups = groups
        self.sems = sems
        self.copies = {}
        self.arrived = None

    def sent(self, group, step, piece, way):
        if step < self.half:
            return True
        return step == self.half and (piece in self.groups[group][1]) == (way == 1)

    def send(self, group, step, piece, way, source=None):
        ref = self.groups[group][0][piece](self.at(-way * (step - 1)))
        copy = remote(ref if source is None else source, ref, next(self.sems), {"sp": self.at(way)})
        copy.start()
        self.copies[group, step, piece, way] = copy

    def first(self, group, sources=None):
        for piece in range(len(self.groups[group][0])):
            for way in (1, -1):
                self.send(group, 1, piece, way, None if sources is None else sources[piece])

    def take(self, group, step, piece=None):
        for number in range(len(self.groups[group][0])):
            for way in (1, -1):
                if piece not in (None, number) or not self.sent(group, step, number, way):
                    continue
                with jax.named_scope(f"ring{group}_{step}_{number}"):
                    self.copies[group, step, number, way].wait_recv()
                if self.sent(group, step + 1, number, way):
                    self.send(group, step + 1, number, way)
                if self.arrived is not None:
                    self.arrived(group, step, number, way)

    def slot(self, step, way):
        return 2 * self.half - 1 if step == self.half else 2 * step - (1 if way == 1 else 0)

    def owner(self, slot):
        step = (slot + 1) // 2
        return self.at(-step if slot % 2 else step)


def scoped(name):
    def wrap(call):
        def inner(*args):
            with jax.named_scope(name):
                return call(*args)

        return inner

    return wrap


def fused_kernel(sp, names, *all_refs):
    ref = types.SimpleNamespace(**dict(zip(names, all_refs)))
    tokens, query_w, taps_w = ref.tokens, ref.query_w, ref.conv_taps
    whole, normed, gated, convolved = ref.whole, ref.normed, ref.gated, ref.convolved
    query_all, kv_all = ref.query_all, ref.kv_all
    value_all, gate_all = ref.value_all, ref.gate_all
    proj_all, proj_other = ref.proj_all, ref.proj_other
    taps, sinks, mix_rows, conv_gains = ref.taps, ref.sinks, ref.mix_rows, ref.conv_gains
    spread_heads, head_gains = ref.spread_heads, ref.head_gains
    band, eye = ref.band, ref.eye
    stat_out, stat_in, stat_rows = ref.stat_out, ref.stat_in, ref.stat_rows
    queries = ref.queries
    key_low, key_high = ref.key_low, ref.key_high
    value_low, value_high = ref.value_low, ref.value_high
    mixers, mixers_other = ref.mixers, ref.mixers_other
    near_out, far_in, far_out = ref.near_out, ref.far_in, ref.far_out

    count, features = tokens.shape
    depth, width = query_w.shape
    model = features * 4
    columns = ref.attn_p.shape[1]
    block = count // 4
    half_pad = (gated.shape[1] - count) // 2
    reach = (taps.shape[0] - 1) // 2
    head = LANES // 2
    channels = taps.shape[1]
    blocks = count // LANES
    s, t = lax.axis_index("sp"), lax.axis_index("tp")
    a, c = t // 2, t % 2
    inner, outer = t + 1 - 2 * c, (t + 2) % 4
    cross = outer + 1 - 2 * c
    send_sem, recv_sem, local_sem = ref.send_sem, ref.recv_sem, ref.local_sem

    def sem_pairs():
        for i in range(recv_sem.shape[0]):
            yield send_sem, recv_sem.at[i]

    sems = sem_pairs()
    sent = []

    def push(source, target, where):
        copy = remote(source, target, next(sems), where)
        copy.start()
        sent.append(copy)
        return copy

    def rows_of(owner, low, high):
        return pl.ds(pl.multiple_of(owner * depth + low, 16), high - low)

    def kv_columns(owner):
        return pl.ds(pl.multiple_of(owner * depth, LANES), depth)

    def out_columns(owner):
        return pl.ds(pl.multiple_of(owner * columns, LANES), columns)

    cut = depth // 2
    ring = Ring(
        sp,
        (
            (
                (
                    lambda o: value_all.at[rows_of(o, 0, depth), :],
                    lambda o: gate_all.at[rows_of(o, 0, depth), :],
                ),
                (0,),
            ),
            (
                (
                    lambda o: kv_all.at[pl.ds(0, head), kv_columns(o)],
                    lambda o: kv_all.at[pl.ds(head, head), kv_columns(o)],
                ),
                (0,),
            ),
            (
                (
                    lambda o: query_all.at[rows_of(o, 0, cut), :],
                    lambda o: query_all.at[rows_of(o, cut, depth), :],
                ),
                (0,),
            ),
            (
                (
                    lambda o: proj_all.at[o, pl.ds(0, width), :],
                    lambda o: proj_all.at[o, pl.ds(width, channels), :],
                ),
                (0,),
            ),
        ),
        sems,
    )
    half = ring.half

    barrier = pltpu.get_barrier_semaphore()
    following, preceding = (s + 1) % sp, (s + sp - 1) % sp
    near_devices = [{"sp": ring.at(1)}, {"sp": ring.at(-1)}, {"sp": following}, {"sp": preceding}]
    near_devices += [{"tp": inner}, {"tp": outer}, {"tp": cross}]
    for where in near_devices:
        pl.semaphore_signal(barrier, inc=1, device_id=where, device_id_type=MESH)
    local = []
    for i, (source, target) in enumerate(
        (
            (tokens, whole.at[t]),
            (ref.key_w, kv_all.at[pl.ds(0, head), kv_columns(s)]),
            (ref.value_w, kv_all.at[pl.ds(head, head), kv_columns(s)]),
            (ref.mix_gain, mix_rows),
            (query_w, query_all.at[rows_of(s, 0, depth), :]),
            (ref.conv_value_w, value_all.at[rows_of(s, 0, depth), :]),
            (ref.conv_gate_w, gate_all.at[rows_of(s, 0, depth), :]),
            (ref.attn_p, proj_all.at[s, pl.ds(0, width), :]),
            (ref.conv_p, proj_all.at[s, pl.ds(width, channels), :]),
            (taps_w, taps),
            (ref.sink_logit, sinks),
            (ref.conv_gain, conv_gains),
            (ref.query_gain, ref.query_gains),
            (ref.key_gain, ref.key_gains),
        )
    ):
        copy = pltpu.make_async_copy(source, target, local_sem.at[i])
        copy.start()
        local.append(copy)
    with jax.named_scope("wait_barrier"):
        pl.semaphore_wait(barrier, len(near_devices))

    ring.first(0, (ref.conv_value_w, ref.conv_gate_w))
    over = []
    for i in range(4):
        rows = pl.ds(i * block, block)
        over.append(push(tokens.at[rows, :], whole.at[t, rows, :], {"tp": outer}))
    beside = push(tokens, whole.at[t], {"tp": inner})
    with jax.named_scope("wait_local"):
        for copy in local:
            copy.wait()

    square = (width, width)
    spread_heads[...] = jnp.where(
        row_index(square) // head == lane_index(square) // head, 1.0 / head, 0.0
    ).astype(jnp.bfloat16)
    tile = (LANES, LANES)
    row, lane = row_index(tile), lane_index(tile)
    band[0] = (lane >= row).astype(jnp.float32)
    band[1] = (lane <= row).astype(jnp.float32)
    eye[...] = (lane == row).astype(jnp.float32)
    query_gain, key_gain = ref.query_gains[...], ref.key_gains[...]
    plain_lanes = jnp.ones_like(key_gain)
    head_gains[0:1, :] = jnp.concatenate([query_gain] * 4, axis=1)
    head_gains[1:2, :] = jnp.concatenate([key_gain, plain_lanes, plain_lanes, key_gain], axis=1)
    ones_low = jnp.where(lane < head, 1.0, 0.0)
    for i in range(value_low.shape[0] // LANES):
        rows = pl.ds(i * LANES, LANES)
        low, high = ones_low, 1.0 - ones_low
        if i == 0:
            low, high = (jnp.where(s > 0, v, 0.0) for v in (low, high))
        if i == value_low.shape[0] // LANES - 1:
            low, high = (jnp.where(s < sp - 1, v, 0.0) for v in (low, high))
        value_low[rows, LANES:] = low.astype(jnp.bfloat16)
        value_high[rows, LANES:] = high.astype(jnp.bfloat16)

    step_rows = 64

    def norm_rows(i, carry):
        rows = pl.ds(pl.multiple_of(i * step_rows, step_rows), step_rows)
        total = jnp.zeros((step_rows, LANES), jnp.float32)
        for j in range(4):
            for k in range(features // LANES):
                x = whole[j, rows, k * LANES : (k + 1) * LANES].astype(jnp.float32)
                total = total + x * x
        mean = jnp.sum(total, axis=1, keepdims=True) * (1.0 / model)
        scale = jnp.broadcast_to(lax.rsqrt(mean + EPSILON), (step_rows, LANES))
        for j in range(4):
            for k in range(features // LANES):
                x = whole[j, rows, k * LANES : (k + 1) * LANES].astype(jnp.float32)
                place = j * (features // LANES) + k
                gain = mix_rows[place : place + 1, :]
                normed[rows, place * LANES : (place + 1) * LANES] = (x * scale * gain).astype(
                    jnp.bfloat16
                )
        return carry

    forwards = []

    def forward_tokens(i):
        with jax.named_scope("wait_over"):
            over[i].wait_recv()
        source = whole.at[outer, pl.ds(i * block, block), :]
        forwards.append(push(source, source, {"tp": inner}))

    def norm_block(i):
        with jax.named_scope("wait_forward"):
            if i == 0:
                beside.wait_recv()
            forwards[i].wait_recv()
        with jax.named_scope("norm"):
            per = block // step_rows
            lax.fori_loop(i * per, (i + 1) * per, norm_rows, 0)

    edge_out, edge_in = ref.edge_out, ref.edge_in

    @scoped("gate")
    def gate_block(i):
        left = normed[i * block : (i + 1) * block, :]
        value = matmul(left, value_all[...])
        gate = matmul(left, gate_all[...])
        result = (value * jax.nn.sigmoid(gate)).astype(jnp.bfloat16)
        wide = result.astype(jnp.float32)
        for j in range(channels // LANES):
            gated[j, i * block + half_pad : (i + 1) * block + half_pad, :] = wide[
                :, j * LANES : (j + 1) * LANES
            ]
        if i == 0:
            edge_out[0] = result[:half_pad, :]
        if i == 3:
            edge_out[1] = result[block - half_pad :, :]

    def conv_rows(i, carry):
        start = i * LANES
        parts = []
        for j in range(channels // LANES):
            lanes = slice(j * LANES, (j + 1) * LANES)
            total = jnp.zeros((LANES, LANES), jnp.float32)
            first = half_pad - reach
            for shift in range(8):
                offsets = [o for o in range(first, first + 2 * reach + 1) if o % 8 == shift]
                high = offsets[-1] - shift
                rows = gated[j, pl.ds(start + shift, LANES + high), :]
                for o in offsets:
                    tap = taps[o - first : o - first + 1, lanes]
                    total = total + tap * rows[o - shift : o - shift + LANES]
            convolved[pl.ds(pl.multiple_of(start, LANES), LANES), lanes] = total
            parts.append(total)
        mean = jnp.sum(sum(parts[1:], parts[0]), axis=1, keepdims=True) * (1.0 / channels)
        squares = [jnp.square(part - mean) for part in parts]
        square_sum = jnp.sum(sum(squares[1:], squares[0]), axis=1, keepdims=True)
        stat_out[pl.ds(i, 1), :] = jnp.sum(mean * eye[...], axis=0, keepdims=True)
        stat_out[pl.ds(i + blocks, 1), :] = jnp.sum(square_sum * eye[...], axis=0, keepdims=True)
        return carry

    @scoped("conv")
    def convolve(low, high):
        lax.fori_loop(low, high, conv_rows, 0)

    quarter = blocks // 4

    def fill_edges():
        for side, edge in enumerate(edges):
            with jax.named_scope("wait_edge"):
                edge.wait_recv()
            inside = s > 0 if side == 0 else s < sp - 1
            values = jnp.where(inside, edge_in[side].astype(jnp.float32), 0.0)
            start = 0 if side == 0 else count + half_pad
            for j in range(channels // LANES):
                gated[j, start : start + half_pad, :] = values[:, j * LANES : (j + 1) * LANES]

    def head_scale(part):
        mean = matmul((part * part).astype(jnp.bfloat16), spread_heads[...])
        return lax.rsqrt(mean + EPSILON)

    halo_out, halo_in = ref.halo_out, ref.halo_in

    @scoped("keys")
    def key_value_block(i):
        keys, vals = kv_all[:head, :], kv_all[head:, :]
        weights = jnp.concatenate([keys, vals, vals, keys], axis=0)
        part = contract_last(normed[i * block : (i + 1) * block, :], weights)
        scaled = part * head_scale(part) * head_gains[1:2, :]
        is_low = lane_index((block, LANES)) < head
        rows = slice(WINDOW + i * block, WINDOW + (i + 1) * block)
        key_low[rows, :] = jnp.where(is_low, scaled[:, :LANES], 0.0).astype(jnp.bfloat16)
        value_high[rows, :LANES] = jnp.where(is_low, 0.0, part[:, :LANES]).astype(jnp.bfloat16)
        value_low[rows, :LANES] = jnp.where(is_low, part[:, LANES:], 0.0).astype(jnp.bfloat16)
        key_high[rows, :] = jnp.where(is_low, 0.0, scaled[:, LANES:]).astype(jnp.bfloat16)
        if i in (0, 3):
            low = jnp.where(is_low, scaled[:, :LANES], part[:, :LANES]).astype(jnp.bfloat16)
            halo_out[i // 3] = low[:WINDOW] if i == 0 else low[block - WINDOW :]

    ring.take(0, 1)
    forward_tokens(0)
    norm_block(0)
    ring.take(0, 2)
    ring.first(1)
    forward_tokens(1)
    norm_block(1)
    for step in range(3, half):
        ring.take(0, step)
    ring.take(1, 1)
    ring.first(2)
    forward_tokens(2)
    norm_block(2)
    ring.take(0, half)
    gate_block(0)
    ring.take(1, 2)
    forward_tokens(3)
    gate_block(1)
    ring.take(2, 1, 0)
    norm_block(3)
    ring.take(2, 1, 1)
    gate_block(3)
    edges = [
        push(edge_out.at[1], edge_in.at[0], {"sp": following}),
        push(edge_out.at[0], edge_in.at[1], {"sp": preceding}),
    ]
    for step in range(3, half):
        ring.take(1, step)
    gate_block(2)
    ring.take(2, 2, 0)
    convolve(quarter, 2 * quarter)
    ring.take(2, 2, 1)
    ring.take(1, half)
    key_value_block(0)
    key_value_block(3)
    halos = [
        push(halo_out.at[1], halo_in.at[0], {"sp": following}),
        push(halo_out.at[0], halo_in.at[1], {"sp": preceding}),
    ]
    for step in range(3, half):
        ring.take(2, step, 0)
        convolve(2 * quarter, 3 * quarter) if step == 3 else None
        ring.take(2, step, 1)
    ring.first(3)
    fill_edges()
    convolve(0, quarter)
    convolve(3 * quarter, blocks)
    stats = [
        push(stat_out, stat_in.at[i], {"tp": peer}) for i, peer in enumerate((inner, outer, cross))
    ]
    key_value_block(1)
    key_value_block(2)
    for stat in stats:
        with jax.named_scope("wait_stat"):
            stat.wait_recv()
    every = [stat_out[...]] + [stat_in[i] for i in range(3)]
    means = [v[:blocks] for v in every]
    center = (means[0] + means[1] + means[2] + means[3]) * 0.25
    spread = sum(v[blocks:] for v in every) + channels * sum(jnp.square(m - center) for m in means)
    stat_rows[:blocks] = center
    stat_rows[blocks:] = lax.rsqrt(spread * (1.0 / (channels * 4)) + EPSILON)

    def feature_rows(i, carry):
        rows = pl.ds(pl.multiple_of(i * LANES, LANES), LANES)
        middle = jnp.sum(stat_rows[pl.ds(i, 1), :] * eye[...], axis=1, keepdims=True)
        scale = jnp.sum(stat_rows[pl.ds(i + blocks, 1), :] * eye[...], axis=1, keepdims=True)
        for j in range(channels // LANES):
            lanes = slice(j * LANES, (j + 1) * LANES)
            value = (convolved[rows, lanes] - middle) * scale * conv_gains[j : j + 1, :]
            mixers[rows, width + j * LANES : width + (j + 1) * LANES] = (
                value * jax.nn.sigmoid(value)
            ).astype(jnp.bfloat16)
        return carry

    starts = ((1 - a) * 2, a * 2)
    give = [pl.ds(pl.multiple_of((base + 1 - c) * block, block), block) for base in starts]
    keep = [pl.ds(pl.multiple_of((base + c) * block, block), block) for base in starts]

    @scoped("features")
    def features_of(f):
        low = starts[f] * (block // LANES)
        lax.fori_loop(low, low + blocks // 2, feature_rows, 0)
        return push(mixers.at[give[f], width:], mixers_other.at[f, :, width:], {"tp": inner})

    given_features = [features_of(0)]
    ring.take(2, half)

    @scoped("queries")
    def query_block(rows):
        part = matmul(normed[rows, :], query_all[...])
        queries[rows, :] = (part * head_scale(part) * head_gains[0:1, :]).astype(jnp.bfloat16)

    shared = {}

    def share(slot, piece):
        owner = ring.owner(slot)
        rows = pl.ds(piece * width, width if piece == 0 else channels)
        pair = shared.get(slot) or next(sems)
        shared[slot] = pair
        copy = remote(
            proj_all.at[owner, rows, :], proj_other.at[owner, rows, :], pair, {"tp": inner}
        )
        copy.start()
        sent.append(copy)

    ring.arrived = lambda group, step, piece, way: share(ring.slot(step, way), piece)
    share(0, 0)
    share(0, 1)
    query_block(give[0])
    query_block(keep[0])
    ring.take(3, 1, 0)
    for side, halo in enumerate(halos):
        with jax.named_scope("wait_halo"):
            halo.wait_recv()
        inside = s > 0 if side == 0 else s < sp - 1
        low = halo_in[side].astype(jnp.float32)
        high = pltpu.roll(low, head, 1)
        is_low = lane_index(low.shape) < head
        start = 0 if side == 0 else WINDOW + count
        rows = slice(start, start + WINDOW)
        key_low[rows, :] = jnp.where(is_low, low, 0.0).astype(jnp.bfloat16)
        key_high[rows, :] = jnp.where(is_low, 0.0, high).astype(jnp.bfloat16)
        value_low[rows, :LANES] = jnp.where(is_low & inside, high, 0.0).astype(jnp.bfloat16)
        value_high[rows, :LANES] = jnp.where(is_low | ~inside, 0.0, low).astype(jnp.bfloat16)

    exponent = head ** (-0.5) * 1.4426950408889634
    head_lanes = lane_index((1, LANES)) < head
    sink_rows = [
        jnp.exp(jnp.where(head_lanes, sinks[2 * i], sinks[2 * i + 1])) for i in range(2)
    ]

    @scoped("attend")
    def attend_rows(first):
        for i in range(block // WINDOW):
            start = pl.multiple_of(first + i * WINDOW, WINDOW)
            rows = pl.ds(start, WINDOW)
            left = jnp.concatenate([queries[rows, :LANES], queries[rows, LANES:]], axis=0)
            shares, vals = [], []
            for j in range(3):
                span = pl.ds(pl.multiple_of(start + j * WINDOW, WINDOW), WINDOW)
                right = jnp.concatenate([key_low[span, :], key_high[span, :]], axis=0)
                weight = jnp.exp2(contract_last(left, right) * exponent)
                if j != 1:
                    mask = band[j // 2]
                    mask = jnp.concatenate([mask, mask], axis=0)
                    weight = weight * jnp.concatenate([mask, mask], axis=1)
                shares.append(weight.astype(jnp.bfloat16))
                vals += [value_low[span, :], value_high[span, :]]
            total = matmul(jnp.concatenate(shares, axis=1), jnp.concatenate(vals, axis=0))
            for j in range(2):
                piece = total[j * WINDOW : (j + 1) * WINDOW]
                mixers[rows, j * LANES : (j + 1) * LANES] = (
                    piece[:, :LANES] / (piece[:, LANES:] + sink_rows[j])
                ).astype(jnp.bfloat16)

    def attend_given(f):
        attend_rows((starts[f] + 1 - c) * block)
        return push(mixers.at[give[f], :width], mixers_other.at[f, :, :width], {"tp": inner})

    def attend_kept(f):
        attend_rows((starts[f] + c) * block)

    @scoped("project")
    def project(f, slot):
        owner = ring.owner(slot)
        left = jnp.concatenate([mixers[keep[f], :], mixers_other[f]], axis=1)
        right = jnp.concatenate([proj_all[owner], proj_other[owner]], axis=0)
        return matmul(left, right)

    parts = []

    def send_part(slot):
        with jax.named_scope("wait_shared"):
            block_ref = proj_other.at[ring.owner(slot)]
            remote(block_ref, block_ref, shared[slot], {"tp": inner}).wait_recv()
        far_out[slot] = project(0, slot).astype(jnp.bfloat16)
        parts.append(
            push(far_out.at[slot], far_in.at[:, out_columns(ring.owner(slot))], {"tp": outer})
        )

    def keep_part(slot):
        near_out[:, out_columns(ring.owner(slot))] = project(1, slot)

    given_heads = [attend_given(0)]
    attend_kept(0)
    with jax.named_scope("wait_given"):
        given_features[0].wait_recv()
        given_heads[0].wait_recv()
    send_part(0)
    ring.take(3, 1, 1)
    given_features.append(features_of(1))
    send_part(1)
    send_part(2)
    query_block(give[1])
    ring.take(3, 2, 0)
    query_block(keep[1])
    given_heads.append(attend_given(1))
    attend_kept(1)
    with jax.named_scope("wait_given"):
        given_features[1].wait_recv()
        given_heads[1].wait_recv()
    ring.take(3, 2, 1)
    waiting = [0, 1, 2]
    for step in range(2, half + 1):
        keep_part(waiting.pop(0))
        slots = (2 * step - 1, 2 * step) if step < half else (2 * step - 1,)
        for slot in slots:
            send_part(slot)
            waiting.append(slot)
        if step < half:
            keep_part(waiting.pop(0))
            ring.take(3, step + 1, 0)
            if step + 1 < half:
                keep_part(waiting.pop(0))
            ring.take(3, step + 1, 1)
    for slot in waiting:
        keep_part(slot)
    for slot in range(sp):
        with jax.named_scope(f"wait_part{slot}"):
            parts[slot].wait_recv()
    with jax.named_scope("wait_sends"):
        for copy in sent:
            copy.wait_send()
        for copy in ring.copies.values():
            copy.wait_send()


def recv_count(sp):
    pieces = 4 * 2 * (2 * (sp // 2 - 1) + 1)
    return pieces + 2 * sp + 9 + 2 + 2 + 3 + 4


def fits(sp, tp, tokens, query_weight, key_weight, conv_weight, attn_proj, taps, head):
    return (
        tp == 4
        and sp % 2 == 0
        and sp >= 6
        and tokens.shape[0] % (4 * 2 * WINDOW) == 0
        and tokens.shape[1] % LANES == 0
        and WINDOW == LANES
        and 2 * head == LANES
        and key_weight.shape[1] == head
        and query_weight.shape[1] == 4 * head
        and conv_weight.shape[1] == 4 * head
        and query_weight.shape[0] % LANES == 0
        and attn_proj.shape[1] % LANES == 0
        and taps.shape[0] <= 31
    )


def fused(
    tokens,
    mix_gain,
    query_weight,
    key_weight,
    value_weight,
    conv_value_weight,
    conv_gate_weight,
    query_gain,
    key_gain,
    sink_logit,
    conv_taps,
    conv_gain,
    attn_proj,
    conv_proj,
):
    sp = lax.axis_size("sp")
    count, features = tokens.shape
    model = features * 4
    depth, width = query_weight.shape
    head = query_gain.shape[0]
    channels = conv_taps.shape[1]
    columns = attn_proj.shape[1]
    block = count // 4
    bf16, f32 = jnp.bfloat16, jnp.float32
    half_pad = 16
    stat = 2 * count // LANES
    padded_rows = count + 2 * WINDOW
    vmem, dma = pltpu.VMEM, pltpu.SemaphoreType.DMA
    inputs = dict(
        tokens=tokens,
        query_w=query_weight,
        key_w=key_weight.T,
        value_w=value_weight.T,
        conv_value_w=conv_value_weight,
        conv_gate_w=conv_gate_weight,
        attn_p=attn_proj,
        conv_p=conv_proj,
        mix_gain=mix_gain.reshape(-1, LANES),
        conv_gain=conv_gain.reshape(-1, LANES),
        query_gain=query_gain.reshape(1, -1),
        key_gain=key_gain.reshape(1, -1),
        sink_logit=sink_logit,
        conv_taps=conv_taps,
    )
    outputs = dict(
        near_out=vmem((block, model), f32),
        far_in=vmem((block, model), bf16),
    )
    scratch = dict(
        whole=vmem((4, count, features), bf16),
        normed=vmem((count, model), bf16),
        query_all=vmem((model, width), bf16),
        kv_all=vmem((2 * head, model), bf16),
        value_all=vmem((model, channels), bf16),
        gate_all=vmem((model, channels), bf16),
        proj_all=vmem((sp, width + channels, columns), bf16),
        proj_other=vmem((sp, width + channels, columns), bf16),
        taps=vmem(conv_taps.shape, f32),
        sinks=pltpu.SMEM(sink_logit.shape, f32),
        mix_rows=vmem((model // LANES, LANES), f32),
        conv_gains=vmem((channels // LANES, LANES), f32),
        query_gains=vmem((1, head), f32),
        key_gains=vmem((1, head), f32),
        head_gains=vmem((2, width), f32),
        spread_heads=vmem((width, width), bf16),
        band=vmem((2, LANES, LANES), f32),
        eye=vmem((LANES, LANES), f32),
        gated=vmem((channels // LANES, count + 2 * half_pad, LANES), f32),
        edge_out=vmem((2, half_pad, channels), bf16),
        edge_in=vmem((2, half_pad, channels), bf16),
        convolved=vmem((count, channels), f32),
        stat_out=vmem((stat, LANES), f32),
        stat_in=vmem((3, stat, LANES), f32),
        stat_rows=vmem((stat, LANES), f32),
        queries=vmem((count, width), bf16),
        key_low=vmem((padded_rows, LANES), bf16),
        key_high=vmem((padded_rows, LANES), bf16),
        value_low=vmem((padded_rows, 2 * LANES), bf16),
        value_high=vmem((padded_rows, 2 * LANES), bf16),
        halo_out=vmem((2, WINDOW, LANES), bf16),
        halo_in=vmem((2, WINDOW, LANES), bf16),
        mixers=vmem((count, width + channels), bf16),
        mixers_other=vmem((2, block, width + channels), bf16),
        far_out=vmem((sp, block, columns), bf16),
        local_sem=dma((14,)),
        send_sem=dma,
        recv_sem=dma((recv_count(sp),)),
    )
    near, far = pl.pallas_call(
        functools.partial(fused_kernel, sp, (*inputs, *outputs, *scratch)),
        out_shape=tuple(outputs.values()),
        in_specs=[pl.BlockSpec(memory_space=pltpu.HBM)] * len(inputs),
        out_specs=[pl.BlockSpec(memory_space=pltpu.VMEM)] * 2,
        scratch_shapes=list(scratch.values()),
        compiler_params=pltpu.CompilerParams(
            collective_id=1, has_side_effects=True, vmem_limit_bytes=60 * 2**20 + 2**19
        ),
    )(*inputs.values())
    return (near + far.astype(f32)).astype(bf16)


def on_device(
    tokens,
    mix_gain,
    query_weight,
    key_weight,
    value_weight,
    conv_value_weight,
    conv_gate_weight,
    query_gain,
    key_gain,
    sink_logit,
    conv_taps,
    conv_gain,
    attn_proj,
    conv_proj,
):
    if fits(
        lax.axis_size("sp"),
        lax.axis_size("tp"),
        tokens,
        query_weight,
        key_weight,
        conv_value_weight,
        attn_proj,
        conv_taps,
        query_gain.shape[0],
    ):
        return fused(
            tokens,
            mix_gain,
            query_weight,
            key_weight,
            value_weight,
            conv_value_weight,
            conv_gate_weight,
            query_gain,
            key_gain,
            sink_logit,
            conv_taps,
            conv_gain,
            attn_proj,
            conv_proj,
        )
    count = tokens.shape[0]
    shards = (query_weight, conv_value_weight, conv_gate_weight, key_weight, value_weight)
    whole, joined = gather_both(tokens, jnp.concatenate(shards, axis=1))
    normed = unit_rows(whole.astype(jnp.float32), mix_gain).astype(jnp.bfloat16)
    product = jnp.dot(normed, joined, preferred_element_type=jnp.float32)
    cuts = []
    for shard in shards[:-1]:
        cuts.append((cuts[-1] if cuts else 0) + shard.shape[1])
    query, conv_value, conv_gate, key_part, value_part = jnp.split(product, cuts, axis=1)
    head_size = query_gain.shape[0]
    local_kv = key_part.shape[1] // head_size
    group = query.shape[1] // head_size // local_kv
    queries = unit_rows(query.reshape(count, local_kv, group, head_size), query_gain).astype(
        jnp.bfloat16
    )
    keys_normed = (
        unit_rows(key_part.reshape(count, local_kv, head_size), key_gain)
        .astype(jnp.bfloat16)
        .reshape(count, -1)
    )
    values_cast = value_part.astype(jnp.bfloat16)
    gated = (conv_value * jax.nn.sigmoid(conv_gate)).astype(jnp.bfloat16)
    reach = (conv_taps.shape[0] - 1) // 2
    kv_width = keys_normed.shape[1]
    paired = jnp.concatenate([keys_normed, values_cast], axis=1)
    extended = padded(paired, (("sp", 0),), WINDOW)
    key_rows = extended[:, :kv_width]
    value_rows = extended[:, kv_width:]
    conv_rows = padded(gated, (("sp", 0),), reach)
    offset = lax.axis_index("sp") * count
    total = count * lax.axis_size("sp")
    span_rows = key_rows.shape[0]
    attended = attend(
        queries,
        key_rows.reshape(span_rows, local_kv, head_size),
        value_rows.reshape(span_rows, local_kv, head_size),
        sink_logit,
        offset,
        total,
    )
    convolved = depthwise(conv_rows, conv_taps, count)
    channels, tp = conv_taps.shape[1], lax.axis_size("tp")
    local_mean = jnp.mean(convolved, axis=1)
    local_square = jnp.sum(jnp.square(convolved - local_mean[:, None]), axis=1)
    slot = (jnp.arange(tp) == lax.axis_index("tp")).astype(jnp.float32)[:, None, None]
    every = lax.psum(slot * jnp.stack([local_mean, local_square])[None], "tp")
    center = jnp.mean(every[:, 0], axis=0)
    spread = jnp.sum(every[:, 1] + channels * jnp.square(every[:, 0] - center), axis=0)
    spread = spread / (channels * tp)
    centered = convolved - center[:, None]
    featured = jax.nn.silu(centered * lax.rsqrt(spread[:, None] + EPSILON) * conv_gain).astype(
        jnp.bfloat16
    )
    stacked, _ = lax.optimization_barrier((jnp.concatenate([attn_proj, conv_proj], axis=0), joined))
    proj_full = lax.all_gather(stacked, "sp", axis=1, tiled=True)
    mixers = jnp.concatenate([attended, featured], axis=1)
    partial = jnp.dot(mixers, proj_full, preferred_element_type=jnp.float32).astype(jnp.bfloat16)
    return lax.psum_scatter(partial, "tp", scatter_dimension=0, tiled=True)


def solution(mesh):
    placed = (
        P("sp", "tp"),
        P(),
        P("sp", "tp"),
        P("sp", "tp"),
        P("sp", "tp"),
        P("sp", "tp"),
        P("sp", "tp"),
        P(),
        P(),
        P("tp"),
        P(None, "tp"),
        P("tp"),
        P("tp", "sp"),
        P("tp", "sp"),
    )
    return jax.shard_map(
        on_device, mesh=mesh, in_specs=placed, out_specs=P(("sp", "tp"), None), check_vma=False
    )
```

```python
import functools
import types

import jax
import jax.numpy as jnp
from jax import lax
from jax.experimental import pallas as pl
from jax.experimental.pallas import tpu as pltpu
from jax.sharding import PartitionSpec as P

WINDOW = 128


EPSILON = 0.1


def padded(value, sides, width):
    for axis, dim in sides:
        size, length = (lax.axis_size(axis), value.shape[dim])
        up = [(i, (i + 1) % size) for i in range(size - 1)]
        down = [(j, i) for i, j in up]
        last = lax.slice_in_dim(value, length - width, length, axis=dim)
        leading = lax.slice_in_dim(value, 0, width, axis=dim)
        before = lax.ppermute(last, axis, up)
        after = lax.ppermute(leading, axis, down)
        value = jnp.concatenate([before, value, after], axis=dim)
    return value


def unit_rows(values, gain):
    return values * lax.rsqrt(jnp.mean(values * values, axis=-1, keepdims=True) + EPSILON) * gain


def attend(queries, keys, values, sinks, offset, total):
    count, local_kv, group, size = queries.shape
    scale = size ** (-0.5)
    blocks = count // WINDOW
    span = 3 * WINDOW

    def windows(rows):
        cut = rows.reshape(blocks + 2, WINDOW, local_kv, size)
        return jnp.concatenate([cut[:blocks], cut[1 : blocks + 1], cut[2:]], axis=1)

    cut_queries = queries.reshape(blocks, WINDOW, local_kv, group, size)
    scores = jnp.einsum(
        "bqkgd,bskd->bkgqs", cut_queries, windows(keys), preferred_element_type=jnp.float32
    )
    query_row = jnp.arange(WINDOW, dtype=jnp.int32)[None, :, None]
    key_row = jnp.arange(span, dtype=jnp.int32)[None, None, :] - WINDOW
    key_pos = offset + WINDOW * jnp.arange(blocks, dtype=jnp.int32)[:, None, None] + key_row
    allowed = (jnp.abs(key_row - query_row) <= WINDOW) & (key_pos >= 0) & (key_pos < total)
    weights = jnp.where(allowed[:, None, None], jnp.exp(scores * scale), 0.0)
    denominator = jnp.sum(weights, axis=-1) + jnp.exp(sinks).reshape(local_kv, group, 1)
    shares = (weights / denominator[..., None]).astype(jnp.bfloat16)
    result = jnp.einsum(
        "bkgqs,bskd->bqkgd", shares, windows(values), preferred_element_type=jnp.float32
    )
    return result.reshape(count, -1).astype(jnp.bfloat16)


def depthwise(extended, kernel_taps, count):
    result = jnp.zeros((count, kernel_taps.shape[1]), jnp.float32)
    for offset in range(kernel_taps.shape[0]):
        result = result + kernel_taps[offset] * extended[offset : offset + count]
    return result


def snake(size):
    if size % 2:
        return (lambda index: index), (lambda place: place)
    half = size // 2

    def place_of(index):
        odd = index % 2
        return (index // 2) * (1 - odd) + (size - 1 - index // 2) * odd

    def index_of(place):
        back = place // half
        return 2 * place * (1 - back) + (2 * (size - 1 - place) + 1) * back

    return place_of, index_of


def plain(size):
    return (lambda index: index), (lambda place: place)


def gather_kernel(rings, *refs):
    count = len(rings)
    shards, outs = refs[:count], refs[count : 2 * count]
    local_sem = refs[2 * count]
    sems = refs[2 * count + 1 :]
    barrier = pltpu.get_barrier_semaphore()
    plans = []
    for number, (axis, size, dim, order) in enumerate(rings):
        place_of, index_of = order(size)
        place = place_of(lax.axis_index(axis))
        at = lambda shift, p=place, f=index_of, n=size: f((p + shift + n) % n)
        plans.append((axis, size, dim, at, shards[number], outs[number], sems[2 * number : 2 * number + 2]))
        for shift in (1, -1):
            pl.semaphore_signal(
                barrier, inc=1, device_id={axis: at(shift)}, device_id_type=pl.DeviceIdType.MESH
            )

    def window(out, dim, shard, index, low, high):
        rows, columns = shard.shape
        if dim == 0:
            begin = pl.multiple_of(index * rows + low, 16)
            return out.at[pl.ds(begin, high - low), :]
        return out.at[pl.ds(low, high - low), pl.ds(pl.multiple_of(index * columns, 128), columns)]

    local = []
    for number, (axis, size, dim, at, shard, out, _) in enumerate(plans):
        copy = pltpu.make_async_copy(
            shard, window(out, dim, shard, at(0), 0, shard.shape[0]), local_sem.at[number]
        )
        copy.start()
        local.append(copy)
    pl.semaphore_wait(barrier, 2 * count)

    def hop(plan, step, way):
        axis, size, dim, at, shard, out, (send, recv) = plan
        rows = shard.shape[0]
        low, high = 0, rows
        if 2 * step == size:
            low, high = (0, rows // 2) if way == 1 else (rows // 2, rows)
        owner = at(-way * (step - 1))
        target = window(out, dim, shard, owner, low, high)
        source = shard.at[pl.ds(low, high - low), :] if step == 1 else target
        slot = 2 * (step - 1) + (way + 1) // 2
        return pltpu.make_async_remote_copy(
            src_ref=source,
            dst_ref=target,
            send_sem=send.at[slot],
            recv_sem=recv.at[slot],
            device_id={axis: at(way)},
            device_id_type=pl.DeviceIdType.MESH,
        )

    pending = {}
    steps = [(n, s) for n, plan in enumerate(plans) for s in range(1, plan[1] // 2 + 1)]
    steps.sort(key=lambda item: ((item[1] - 1) / (plans[item[0]][1] // 2), -plans[item[0]][1]))
    for number, step in steps:
        for way in (1, -1):
            if step > 1:
                pending[number, step - 1, way].wait_recv()
            copy = hop(plans[number], step, way)
            copy.start()
            pending[number, step, way] = copy
    for number, plan in enumerate(plans):
        for way in (1, -1):
            pending[number, plan[1] // 2, way].wait_recv()
    for copy in pending.values():
        copy.wait_send()
    for copy in local:
        copy.wait()


def gather_both(tokens, joined):
    tp, sp = lax.axis_size("tp"), lax.axis_size("sp")
    rings = (("tp", tp, 1, plain), ("sp", sp, 0, snake))
    sems = []
    for _, size, _, _ in rings:
        sems += [pltpu.SemaphoreType.DMA((2 * (size // 2),))] * 2
    return pl.pallas_call(
        functools.partial(gather_kernel, rings),
        out_shape=(
            jax.ShapeDtypeStruct((tokens.shape[0], tokens.shape[1] * tp), tokens.dtype),
            jax.ShapeDtypeStruct((joined.shape[0] * sp, joined.shape[1]), joined.dtype),
        ),
        in_specs=[pl.BlockSpec(memory_space=pltpu.VMEM)] * 2,
        out_specs=[pl.BlockSpec(memory_space=pl.ANY)] * 2,
        scratch_shapes=[pltpu.SemaphoreType.DMA((2,))] + sems,
        compiler_params=pltpu.CompilerParams(collective_id=0, has_side_effects=True),
    )(tokens, joined)


LANES = 128
MESH = pl.DeviceIdType.MESH


def remote(source, target, sems, where):
    return pltpu.make_async_remote_copy(
        src_ref=source,
        dst_ref=target,
        send_sem=sems[0],
        recv_sem=sems[1],
        device_id=where,
        device_id_type=MESH,
    )


def contract_last(left, right):
    return lax.dot_general(
        left, right, (((1,), (1,)), ((), ())), preferred_element_type=jnp.float32
    )


def matmul(left, right):
    return jnp.dot(left, right, preferred_element_type=jnp.float32)


def lane_index(shape):
    return lax.broadcasted_iota(jnp.int32, shape, len(shape) - 1)


def row_index(shape):
    return lax.broadcasted_iota(jnp.int32, shape, len(shape) - 2)


def aligned(value, multiple):
    return value if isinstance(value, int) else pl.multiple_of(value, multiple)


class Ring:
    def __init__(self, size, groups, sems):
        place_of, index_of = snake(size)
        place = place_of(lax.axis_index("sp"))
        self.at = lambda shift: index_of((place + shift + size) % size)
        self.half = size // 2
        self.groups = groups
        self.sems = sems
        self.copies = {}
        self.arrived = None

    def part(self, group, step, piece, way):
        whole, up, down = self.groups[group][piece]
        if step < self.half:
            return whole
        return None if step > self.half else up if way == 1 else down

    def send(self, group, step, piece, way, source=None):
        ref = self.part(group, step, piece, way)(self.at(-way * (step - 1)))
        copy = remote(ref if source is None else source, ref, next(self.sems), {"sp": self.at(way)})
        copy.start()
        self.copies[group, step, piece, way] = copy

    def first(self, group, sources=None):
        for piece in range(len(self.groups[group])):
            for way in (1, -1):
                self.send(group, 1, piece, way, None if sources is None else sources[piece])

    def take(self, group, step, piece=None):
        for number in range(len(self.groups[group])):
            for way in (1, -1):
                if piece not in (None, number) or self.part(group, step, number, way) is None:
                    continue
                with jax.named_scope(f"ring{group}_{step}_{number}"):
                    self.copies[group, step, number, way].wait_recv()
                if self.part(group, step + 1, number, way) is not None:
                    self.send(group, step + 1, number, way)
                if self.arrived is not None:
                    self.arrived(group, step, number, way)

    def slot(self, step, way):
        return 2 * self.half - 1 if step == self.half else 2 * step - (1 if way == 1 else 0)

    def owner(self, slot):
        step = (slot + 1) // 2
        return self.at(-step if slot % 2 else step)


def scoped(name):
    def wrap(call):
        def inner(*args):
            with jax.named_scope(name):
                return call(*args)

        return inner

    return wrap


def fused_kernel(sp, names, *all_refs):
    ref = types.SimpleNamespace(**dict(zip(names, all_refs)))
    tokens, query_w, taps_w = ref.tokens, ref.query_w, ref.conv_taps
    whole, normed, gated, convolved = ref.whole, ref.normed, ref.gated, ref.convolved
    query_all, kv_all = ref.query_all, ref.kv_all
    value_all, gate_all = ref.value_all, ref.gate_all
    proj_all, proj_other = ref.proj_all, ref.proj_other
    taps, sinks, mix_rows, conv_gains = ref.taps, ref.sinks, ref.mix_rows, ref.conv_gains
    spread_heads, head_gains = ref.spread_heads, ref.head_gains
    band, eye = ref.band, ref.eye
    stat_out, stat_in, stat_rows = ref.stat_out, ref.stat_in, ref.stat_rows
    queries, query_part = ref.queries, ref.query_part
    key_low, key_high = ref.key_low, ref.key_high
    value_low, value_high = ref.value_low, ref.value_high
    mixers, mixers_other = ref.mixers, ref.mixers_other
    near_out, far_in, far_out = ref.near_out, ref.far_in, ref.far_out

    count, features = tokens.shape
    depth, width = query_w.shape
    model = features * 4
    columns = ref.attn_p.shape[1]
    thin = columns // 2
    block = count // 4
    half_pad = (gated.shape[1] - count) // 2
    reach = (taps.shape[0] - 1) // 2
    head = LANES // 2
    channels = taps.shape[1]
    blocks = count // LANES
    s, t = lax.axis_index("sp"), lax.axis_index("tp")
    a, c = t // 2, t % 2
    inner, outer = t + 1 - 2 * c, (t + 2) % 4
    cross = outer + 1 - 2 * c
    send_sem, recv_sem, local_sem = ref.send_sem, ref.recv_sem, ref.local_sem

    def sem_pairs():
        for i in range(recv_sem.shape[0]):
            yield send_sem, recv_sem.at[i]

    sems = sem_pairs()
    sent = []

    def push(source, target, where, pair=None):
        copy = remote(source, target, pair or next(sems), where)
        copy.start()
        sent.append(copy)
        return copy

    def rows_of(owner, low, high):
        return pl.ds(pl.multiple_of(owner * depth + low, 16), high - low)

    def kv_columns(owner):
        return pl.ds(pl.multiple_of(owner * depth, LANES), depth)

    def out_columns(owner):
        return pl.ds(pl.multiple_of(owner * columns, LANES), columns)

    cut = depth // 2

    def value_piece(o):
        return value_all.at[rows_of(o, 0, depth), :]

    def gate_piece(o):
        return gate_all.at[rows_of(o, 0, depth), :]

    def kv_piece(low, high):
        return lambda o: kv_all.at[pl.ds(low, high - low), kv_columns(o)]

    def query_piece(low, high):
        return lambda o: query_all.at[rows_of(o, low, high), :]

    def proj_piece(piece):
        return lambda o: proj_all.at[o, piece]

    early, late = query_piece(0, cut), query_piece(cut, depth)
    left_piece, right_piece = proj_piece(0), proj_piece(1)
    ring = Ring(
        sp,
        (
            ((value_piece, value_piece, None), (gate_piece, None, gate_piece)),
            ((kv_piece(0, 2 * head), kv_piece(0, head), kv_piece(head, 2 * head)),),
            ((early, early, None), (late, None, late)),
            ((left_piece, left_piece, None), (right_piece, None, right_piece)),
        ),
        sems,
    )
    half = ring.half

    barrier = pltpu.get_barrier_semaphore()
    following, preceding = (s + 1) % sp, (s + sp - 1) % sp
    near_devices = [{"sp": ring.at(1)}, {"sp": ring.at(-1)}, {"sp": following}, {"sp": preceding}]
    near_devices += [{"tp": inner}, {"tp": outer}, {"tp": cross}]
    for where in near_devices:
        pl.semaphore_signal(barrier, inc=1, device_id=where, device_id_type=MESH)
    local = []
    for source, target in (
            (tokens, whole.at[t]),
            (ref.key_w, kv_all.at[pl.ds(0, head), kv_columns(s)]),
            (ref.value_w, kv_all.at[pl.ds(head, head), kv_columns(s)]),
            (ref.mix_gain, mix_rows),
            (query_w, query_all.at[rows_of(s, 0, depth), :]),
            (ref.conv_value_w, value_all.at[rows_of(s, 0, depth), :]),
            (ref.conv_gate_w, gate_all.at[rows_of(s, 0, depth), :]),
            (ref.attn_p.at[:, :thin], proj_all.at[s, 0, pl.ds(0, width), :]),
            (ref.attn_p.at[:, thin:], proj_all.at[s, 1, pl.ds(0, width), :]),
            (ref.conv_p.at[:, :thin], proj_all.at[s, 0, pl.ds(width, channels), :]),
            (ref.conv_p.at[:, thin:], proj_all.at[s, 1, pl.ds(width, channels), :]),
            (taps_w, taps),
            (ref.sink_logit, sinks),
            (ref.conv_gain, conv_gains),
            (ref.query_gain, ref.query_gains),
            (ref.key_gain, ref.key_gains),
    ):
        copy = pltpu.make_async_copy(source, target, local_sem)
        copy.start()
        local.append(copy)
    with jax.named_scope("wait_barrier"):
        pl.semaphore_wait(barrier, len(near_devices))

    ring.first(0, (ref.conv_value_w, ref.conv_gate_w))
    over = []
    for i in range(4):
        rows = pl.ds(i * block, block)
        over.append(push(tokens.at[rows, :], whole.at[t, rows, :], {"tp": outer}))
    beside = push(tokens, whole.at[t], {"tp": inner})
    with jax.named_scope("wait_local"):
        for copy in local:
            copy.wait()

    square = (width, width)
    spread_heads[...] = jnp.where(
        row_index(square) // head == lane_index(square) // head, 1.0 / head, 0.0
    ).astype(jnp.bfloat16)
    tile = (LANES, LANES)
    row, lane = row_index(tile), lane_index(tile)
    band[0] = (lane >= row).astype(jnp.float32)
    band[1] = (lane <= row).astype(jnp.float32)
    eye[...] = (lane == row).astype(jnp.float32)
    exponent = head ** (-0.5) * 1.4426950408889634
    query_gain, key_gain = ref.query_gains[...], ref.key_gains[...]
    plain_lanes = jnp.ones_like(key_gain)
    head_gains[0:1, :] = jnp.concatenate([query_gain * exponent] * 4, axis=1)
    head_gains[1:2, :] = jnp.concatenate([key_gain, plain_lanes, plain_lanes, key_gain], axis=1)
    ones_low = jnp.where(lane < head, 1.0, 0.0)
    for i in range(value_low.shape[0] // LANES):
        rows = pl.ds(i * LANES, LANES)
        low, high = ones_low, 1.0 - ones_low
        if i == 0:
            low, high = (jnp.where(s > 0, v, 0.0) for v in (low, high))
        if i == value_low.shape[0] // LANES - 1:
            low, high = (jnp.where(s < sp - 1, v, 0.0) for v in (low, high))
        value_low[rows, LANES:] = low.astype(jnp.bfloat16)
        value_high[rows, LANES:] = high.astype(jnp.bfloat16)

    step_rows = 64

    def norm_rows(i, carry):
        rows = pl.ds(pl.multiple_of(i * step_rows, step_rows), step_rows)
        total = jnp.zeros((step_rows, LANES), jnp.float32)
        for j in range(4):
            for k in range(features // LANES):
                x = whole[j, rows, k * LANES : (k + 1) * LANES].astype(jnp.float32)
                total = total + x * x
        mean = jnp.sum(total, axis=1, keepdims=True) * (1.0 / model)
        scale = jnp.broadcast_to(lax.rsqrt(mean + EPSILON), (step_rows, LANES))
        for j in range(4):
            for k in range(features // LANES):
                x = whole[j, rows, k * LANES : (k + 1) * LANES].astype(jnp.float32)
                place = j * (features // LANES) + k
                gain = mix_rows[place : place + 1, :]
                normed[rows, place * LANES : (place + 1) * LANES] = (x * scale * gain).astype(
                    jnp.bfloat16
                )
        return carry

    forwards = []

    def forward_tokens(i):
        with jax.named_scope("wait_over"):
            over[i].wait_recv()
        source = whole.at[outer, pl.ds(i * block, block), :]
        forwards.append(push(source, source, {"tp": inner}))

    def norm_block(i):
        with jax.named_scope("wait_forward"):
            if i == 0:
                beside.wait_recv()
            forwards[i].wait_recv()
        with jax.named_scope("norm"):
            per = block // step_rows
            lax.fori_loop(i * per, (i + 1) * per, norm_rows, 0)

    edge_out, edge_in = ref.edge_out, ref.edge_in

    @scoped("gate")
    def gate_block(i):
        left = normed[i * block : (i + 1) * block, :]
        value = matmul(left, value_all[...])
        gate = matmul(left, gate_all[...])
        result = (value * jax.nn.sigmoid(gate)).astype(jnp.bfloat16)
        wide = result.astype(jnp.float32)
        for j in range(channels // LANES):
            gated[j, i * block + half_pad : (i + 1) * block + half_pad, :] = wide[
                :, j * LANES : (j + 1) * LANES
            ]
        if i == 0:
            edge_out[0] = result[:half_pad, :]
        if i == 3:
            edge_out[1] = result[block - half_pad :, :]

    def conv_rows(i, carry):
        start = i * LANES
        parts = []
        for j in range(channels // LANES):
            lanes = slice(j * LANES, (j + 1) * LANES)
            total = jnp.zeros((LANES, LANES), jnp.float32)
            first = half_pad - reach
            for shift in range(8):
                offsets = [o for o in range(first, first + 2 * reach + 1) if o % 8 == shift]
                high = offsets[-1] - shift
                rows = gated[j, pl.ds(start + shift, LANES + high), :]
                for o in offsets:
                    tap = taps[o - first : o - first + 1, lanes]
                    total = total + tap * rows[o - shift : o - shift + LANES]
            convolved[pl.ds(pl.multiple_of(start, LANES), LANES), lanes] = total
            parts.append(total)
        mean = jnp.sum(sum(parts[1:], parts[0]), axis=1, keepdims=True) * (1.0 / channels)
        squares = [jnp.square(part - mean) for part in parts]
        square_sum = jnp.sum(sum(squares[1:], squares[0]), axis=1, keepdims=True)
        stat_out[pl.ds(i, 1), :] = jnp.sum(mean * eye[...], axis=0, keepdims=True)
        stat_out[pl.ds(i + blocks, 1), :] = jnp.sum(square_sum * eye[...], axis=0, keepdims=True)
        return carry

    @scoped("conv")
    def convolve(low, high):
        lax.fori_loop(low, high, conv_rows, 0)

    quarter = blocks // 4

    def fill_edges():
        for side, edge in enumerate(edges):
            with jax.named_scope("wait_edge"):
                edge.wait_recv()
            inside = s > 0 if side == 0 else s < sp - 1
            values = jnp.where(inside, edge_in[side].astype(jnp.float32), 0.0)
            start = 0 if side == 0 else count + half_pad
            for j in range(channels // LANES):
                gated[j, start : start + half_pad, :] = values[:, j * LANES : (j + 1) * LANES]

    def head_scale(part):
        mean = matmul((part * part).astype(jnp.bfloat16), spread_heads[...])
        return lax.rsqrt(mean + EPSILON)

    halo_out, halo_in = ref.halo_out, ref.halo_in

    @scoped("keys")
    def key_value_block(i):
        keys, vals = kv_all[:head, :], kv_all[head:, :]
        weights = jnp.concatenate([keys, vals, vals, keys], axis=0)
        part = contract_last(normed[i * block : (i + 1) * block, :], weights)
        scaled = part * head_scale(part) * head_gains[1:2, :]
        is_low = lane_index((block, LANES)) < head
        rows = slice(WINDOW + i * block, WINDOW + (i + 1) * block)
        key_low[rows, :] = jnp.where(is_low, scaled[:, :LANES], 0.0).astype(jnp.bfloat16)
        value_high[rows, :LANES] = jnp.where(is_low, 0.0, part[:, :LANES]).astype(jnp.bfloat16)
        value_low[rows, :LANES] = jnp.where(is_low, part[:, LANES:], 0.0).astype(jnp.bfloat16)
        key_high[rows, :] = jnp.where(is_low, 0.0, scaled[:, LANES:]).astype(jnp.bfloat16)
        if i in (0, 3):
            low = jnp.where(is_low, scaled[:, :LANES], part[:, :LANES]).astype(jnp.bfloat16)
            halo_out[i // 3] = low[:WINDOW] if i == 0 else low[block - WINDOW :]

    ring.take(0, 1)
    forward_tokens(0)
    norm_block(0)
    ring.take(0, 2)
    ring.first(1)
    forward_tokens(1)
    norm_block(1)
    for step in range(3, half):
        ring.take(0, step)
    ring.take(1, 1)
    ring.first(2)
    forward_tokens(2)
    norm_block(2)
    ring.take(0, half)
    gate_block(0)
    gate_block(1)
    ring.take(1, 2)
    forward_tokens(3)
    gate_block(2)
    ring.take(2, 1, 0)
    norm_block(3)
    ring.take(2, 1, 1)
    gate_block(3)
    edges = [
        push(edge_out.at[1], edge_in.at[0], {"sp": following}),
        push(edge_out.at[0], edge_in.at[1], {"sp": preceding}),
    ]
    convolve(quarter, quarter + 1)
    for step in range(3, half):
        ring.take(1, step)
    convolve(quarter + 1, 3 * quarter - 1)
    ring.take(2, 2, 0)
    convolve(3 * quarter - 1, 3 * quarter)
    convolve(1, quarter)
    ring.take(2, 2, 1)
    convolve(3 * quarter, blocks - 1)
    ring.take(1, half)
    fill_edges()
    convolve(0, 1)
    for step in range(3, half - 1):
        ring.take(2, step)
    convolve(blocks - 1, blocks)
    stat_pair, part_pair = next(sems), next(sems)
    for i, peer in enumerate((inner, outer, cross)):
        push(stat_out, stat_in.at[i], {"tp": peer}, stat_pair)
    ring.take(2, half - 1, 0)
    key_value_block(0)
    right_halo = push(halo_out.at[0], halo_in.at[1], {"sp": preceding})
    ring.take(2, half - 1, 1)
    key_value_block(3)
    halos = [push(halo_out.at[1], halo_in.at[0], {"sp": following}), right_halo]
    key_value_block(1)
    ring.first(3)
    key_value_block(2)

    def feature_rows(i, carry):
        rows = pl.ds(pl.multiple_of(i * LANES, LANES), LANES)
        middle = jnp.sum(stat_rows[pl.ds(i, 1), :] * eye[...], axis=1, keepdims=True)
        scale = jnp.sum(stat_rows[pl.ds(i + blocks, 1), :] * eye[...], axis=1, keepdims=True)
        for j in range(channels // LANES):
            lanes = slice(j * LANES, (j + 1) * LANES)
            value = (convolved[rows, lanes] - middle) * scale * conv_gains[j : j + 1, :]
            mixers[rows, width + j * LANES : width + (j + 1) * LANES] = (
                value * jax.nn.sigmoid(value)
            ).astype(jnp.bfloat16)
        return carry

    starts = ((1 - a) * 2, a * 2)
    give = [pl.ds(pl.multiple_of((base + 1 - c) * block, block), block) for base in starts]
    keep = [pl.ds(pl.multiple_of((base + c) * block, block), block) for base in starts]

    @scoped("features")
    def features_of(f):
        low = starts[f] * (block // LANES)
        lax.fori_loop(low, low + blocks // 2, feature_rows, 0)
        return push(mixers.at[give[f], width:], mixers_other.at[f, :, width:], {"tp": inner})

    @scoped("partial")
    def partial_block(i, rows):
        owners = [ring.owner(slot) for slot in range(sp - 1)]
        left = jnp.concatenate([normed[rows, kv_columns(o)] for o in owners], axis=1)
        right = jnp.concatenate([query_all[rows_of(o, 0, depth), :] for o in owners], axis=0)
        query_part[i] = matmul(left, right)

    @scoped("queries")
    def query_block(i, rows):
        owner = ring.owner(sp - 1)
        last = matmul(normed[rows, kv_columns(owner)], query_all[rows_of(owner, 0, depth), :])
        part = query_part[i] + last
        queries[rows, :] = (part * head_scale(part) * head_gains[0:1, :]).astype(jnp.bfloat16)

    far_rows = [give[0], keep[0]]
    for i, rows in enumerate(far_rows):
        partial_block(i, rows)
    with jax.named_scope("wait_stat"):
        remote(stat_in, stat_in, stat_pair, {"tp": inner}).wait_recv()
    every = [stat_out[...]] + [stat_in[i] for i in range(3)]
    means = [v[:blocks] for v in every]
    center = (means[0] + means[1] + means[2] + means[3]) * 0.25
    spread = sum(v[blocks:] for v in every) + channels * sum(jnp.square(m - center) for m in means)
    stat_rows[:blocks] = center
    stat_rows[blocks:] = lax.rsqrt(spread * (1.0 / (channels * 4)) + EPSILON)

    given_features = [features_of(0)]
    ring.take(2, half)
    for i, rows in enumerate(far_rows):
        query_block(i, rows)

    shared = {}

    def share(slot, piece):
        owner = ring.owner(slot)
        source, target = proj_all.at[owner, piece], proj_other.at[owner, piece]
        shared[slot, piece] = push(source, target, {"tp": inner})

    ring.arrived = lambda group, step, piece, way: share(ring.slot(step, way), piece)
    share(0, 0)
    share(0, 1)
    def fill_halos():
        for side, halo in enumerate(halos):
            with jax.named_scope("wait_halo"):
                halo.wait_recv()
            inside = s > 0 if side == 0 else s < sp - 1
            low = halo_in[side].astype(jnp.float32)
            high = pltpu.roll(low, head, 1)
            is_low = lane_index(low.shape) < head
            start = 0 if side == 0 else WINDOW + count
            rows = slice(start, start + WINDOW)
            key_low[rows, :] = jnp.where(is_low, low, 0.0).astype(jnp.bfloat16)
            key_high[rows, :] = jnp.where(is_low, 0.0, high).astype(jnp.bfloat16)
            value_low[rows, :LANES] = jnp.where(is_low & inside, high, 0.0).astype(jnp.bfloat16)
            value_high[rows, :LANES] = jnp.where(is_low | ~inside, 0.0, low).astype(jnp.bfloat16)

    head_lanes = lane_index((1, LANES)) < head
    sink_rows = [
        jnp.exp(jnp.where(head_lanes, sinks[2 * i], sinks[2 * i + 1])) for i in range(2)
    ]

    @scoped("attend")
    def attend_rows(first, windows):
        for i in range(windows):
            start = pl.multiple_of(first + i * WINDOW, WINDOW)
            rows = pl.ds(start, WINDOW)
            left = jnp.concatenate([queries[rows, :LANES], queries[rows, LANES:]], axis=0)
            shares, vals = [], []
            for j in range(3):
                span = pl.ds(pl.multiple_of(start + j * WINDOW, WINDOW), WINDOW)
                right = jnp.concatenate([key_low[span, :], key_high[span, :]], axis=0)
                weight = jnp.exp2(contract_last(left, right))
                if j != 1:
                    mask = band[j // 2]
                    mask = jnp.concatenate([mask, mask], axis=0)
                    weight = weight * jnp.concatenate([mask, mask], axis=1)
                shares.append(weight.astype(jnp.bfloat16))
                vals += [value_low[span, :], value_high[span, :]]
            total = matmul(jnp.concatenate(shares, axis=1), jnp.concatenate(vals, axis=0))
            for j in range(2):
                piece = total[j * WINDOW : (j + 1) * WINDOW]
                mixers[rows, j * LANES : (j + 1) * LANES] = (
                    piece[:, :LANES] / (piece[:, LANES:] + sink_rows[j])
                ).astype(jnp.bfloat16)

    def attend_given(f, low=0, size=block):
        here = pl.multiple_of((starts[f] + 1 - c) * block + low, WINDOW)
        attend_rows(here, size // WINDOW)
        target = mixers_other.at[f, pl.ds(aligned(low, WINDOW), size), :width]
        return push(mixers.at[pl.ds(here, size), :width], target, {"tp": inner})

    def attend_kept(f, low=0, size=block):
        attend_rows((starts[f] + c) * block + low, size // WINDOW)

    @scoped("project")
    def project(f, slot, pieces=(0, 1), low=0, size=block):
        owner = ring.owner(slot)
        here = pl.ds(pl.multiple_of((starts[f] + c) * block + low, WINDOW), size)
        left = jnp.concatenate(
            [mixers[here, :], mixers_other[f, pl.ds(aligned(low, WINDOW), size), :]], axis=1
        )
        right = [
            jnp.concatenate([proj_all[owner, piece], proj_other[owner, piece]], axis=0)
            for piece in pieces
        ]
        return matmul(left, jnp.concatenate(right, axis=1))

    def wait_shared(slot, piece):
        with jax.named_scope("wait_shared"):
            shared[slot, piece].wait_recv()

    def send_rows(slot, low, size):
        rows = pl.ds(aligned(low, WINDOW), size)
        result = project(0, slot, (0, 1), low, size).astype(jnp.bfloat16)
        for piece in range(2):
            far_out[slot, piece, rows, :] = result[:, piece * thin : (piece + 1) * thin]
        for piece in range(2):
            target = far_in.at[rows, half_columns(slot, piece)]
            push(far_out.at[slot, piece, rows, :], target, {"tp": outer}, part_pair)

    def send_piece(slot, piece):
        wait_shared(slot, piece)
        far_out[slot, piece] = project(0, slot, (piece,)).astype(jnp.bfloat16)
        target = far_in.at[:, half_columns(slot, piece)]
        push(far_out.at[slot, piece], target, {"tp": outer}, part_pair)

    def half_columns(slot, piece):
        begin = ring.owner(slot) * columns + piece * thin
        return pl.ds(pl.multiple_of(begin, LANES), thin)

    def keep_part(slot):
        near_out[:, out_columns(ring.owner(slot))] = project(1, slot)

    split = block // 2
    order = (a * split, (1 - a) * split)
    given_heads = [attend_given(0, order[0], split)]
    attend_kept(0, order[0], split)
    given_features[0].wait_recv()
    for piece in range(2):
        wait_shared(0, piece)
    with jax.named_scope("wait_given"):
        given_heads[0].wait_recv()
    send_rows(0, order[0], split)
    fill_halos()
    given_heads.append(attend_given(0, order[1], split))
    attend_kept(0, order[1], split)
    with jax.named_scope("wait_given"):
        given_heads[1].wait_recv()
    send_rows(0, order[1], split)

    def near_heads():
        given_heads.append(attend_given(1))

    def near_kept():
        attend_kept(1)
        with jax.named_scope("wait_given"):
            given_features[1].wait_recv()
            given_heads[2].wait_recv()

    work = [
        lambda: partial_block(0, give[1]),
        lambda: query_block(0, give[1]),
        lambda: given_features.append(features_of(1)),
        lambda: partial_block(1, keep[1]),
        lambda: query_block(1, keep[1]),
        near_heads,
        near_kept,
        lambda: keep_part(0),
    ]

    def do_work(most):
        for _ in range(min(most, len(work))):
            work.pop(0)()

    counts = {(1, 0): (1, 0), (1, 1): (1, 3), (2, 0): (1, 1), (2, 1): (1, 2)}
    for step in range(1, half + 1):
        slots = (2 * step - 1, 2 * step) if step < half else (2 * step - 1,)
        for piece in range(2):
            ring.take(3, step, piece)
            before, after = counts.get((step, piece), (1, 1))
            do_work(before)
            for slot in slots:
                send_piece(slot, piece)
            if piece == 1:
                work += [functools.partial(keep_part, slot) for slot in slots]
            do_work(after)
    do_work(len(work))
    with jax.named_scope("wait_part"):
        remote(far_in, far_in, part_pair, {"tp": outer}).wait_recv()
    with jax.named_scope("wait_sends"):
        for copy in sent:
            copy.wait_send()
        for copy in ring.copies.values():
            copy.wait_send()


def recv_count(sp):
    pieces = 7 * 2 * (sp // 2 - 1) + 4 * 2
    return pieces + 2 * sp + 9 + 2 + 2 + 2 + 2 + 3


def fits(sp, tp, tokens, query_weight, key_weight, conv_weight, attn_proj, taps, head):
    return (
        tp == 4
        and sp % 2 == 0
        and sp >= 6
        and tokens.shape[0] % (4 * 2 * WINDOW) == 0
        and tokens.shape[1] % LANES == 0
        and WINDOW == LANES
        and 2 * head == LANES
        and key_weight.shape[1] == head
        and query_weight.shape[1] == 4 * head
        and conv_weight.shape[1] == 4 * head
        and query_weight.shape[0] % LANES == 0
        and attn_proj.shape[1] % (2 * LANES) == 0
        and taps.shape[0] <= 31
    )


def fused(
    tokens,
    mix_gain,
    query_weight,
    key_weight,
    value_weight,
    conv_value_weight,
    conv_gate_weight,
    query_gain,
    key_gain,
    sink_logit,
    conv_taps,
    conv_gain,
    attn_proj,
    conv_proj,
):
    sp = lax.axis_size("sp")
    count, features = tokens.shape
    model = features * 4
    depth, width = query_weight.shape
    head = query_gain.shape[0]
    channels = conv_taps.shape[1]
    columns = attn_proj.shape[1]
    block = count // 4
    bf16, f32 = jnp.bfloat16, jnp.float32
    half_pad = 16
    stat = 2 * count // LANES
    padded_rows = count + 2 * WINDOW
    vmem, dma = pltpu.VMEM, pltpu.SemaphoreType.DMA
    inputs = dict(
        tokens=tokens,
        query_w=query_weight,
        key_w=key_weight.T,
        value_w=value_weight.T,
        conv_value_w=conv_value_weight,
        conv_gate_w=conv_gate_weight,
        attn_p=attn_proj,
        conv_p=conv_proj,
        mix_gain=mix_gain.reshape(-1, LANES),
        conv_gain=conv_gain.reshape(-1, LANES),
        query_gain=query_gain.reshape(1, -1),
        key_gain=key_gain.reshape(1, -1),
        sink_logit=sink_logit,
        conv_taps=conv_taps,
    )
    outputs = dict(
        near_out=vmem((block, model), f32),
        far_in=vmem((block, model), bf16),
    )
    scratch = dict(
        whole=vmem((4, count, features), bf16),
        normed=vmem((count, model), bf16),
        query_all=vmem((model, width), bf16),
        kv_all=vmem((2 * head, model), bf16),
        value_all=vmem((model, channels), bf16),
        gate_all=vmem((model, channels), bf16),
        proj_all=vmem((sp, 2, width + channels, columns // 2), bf16),
        proj_other=vmem((sp, 2, width + channels, columns // 2), bf16),
        taps=vmem(conv_taps.shape, f32),
        sinks=pltpu.SMEM(sink_logit.shape, f32),
        mix_rows=vmem((model // LANES, LANES), f32),
        conv_gains=vmem((channels // LANES, LANES), f32),
        query_gains=vmem((1, head), f32),
        key_gains=vmem((1, head), f32),
        head_gains=vmem((2, width), f32),
        spread_heads=vmem((width, width), bf16),
        band=vmem((2, LANES, LANES), f32),
        eye=vmem((LANES, LANES), f32),
        gated=vmem((channels // LANES, count + 2 * half_pad, LANES), f32),
        edge_out=vmem((2, half_pad, channels), bf16),
        edge_in=vmem((2, half_pad, channels), bf16),
        convolved=vmem((count, channels), f32),
        stat_out=vmem((stat, LANES), f32),
        stat_in=vmem((3, stat, LANES), f32),
        stat_rows=vmem((stat, LANES), f32),
        queries=vmem((count, width), bf16),
        query_part=vmem((2, block, width), f32),
        key_low=vmem((padded_rows, LANES), bf16),
        key_high=vmem((padded_rows, LANES), bf16),
        value_low=vmem((padded_rows, 2 * LANES), bf16),
        value_high=vmem((padded_rows, 2 * LANES), bf16),
        halo_out=vmem((2, WINDOW, LANES), bf16),
        halo_in=vmem((2, WINDOW, LANES), bf16),
        mixers=vmem((count, width + channels), bf16),
        mixers_other=vmem((2, block, width + channels), bf16),
        far_out=vmem((sp, 2, block, columns // 2), bf16),
        local_sem=dma,
        send_sem=dma,
        recv_sem=dma((recv_count(sp),)),
    )
    near, far = pl.pallas_call(
        functools.partial(fused_kernel, sp, (*inputs, *outputs, *scratch)),
        out_shape=tuple(outputs.values()),
        in_specs=[pl.BlockSpec(memory_space=pltpu.HBM)] * len(inputs),
        out_specs=[pl.BlockSpec(memory_space=pltpu.VMEM)] * 2,
        scratch_shapes=list(scratch.values()),
        compiler_params=pltpu.CompilerParams(
            collective_id=1, has_side_effects=True, vmem_limit_bytes=60 * 2**20 + 2**19
        ),
    )(*inputs.values())
    return (near + far.astype(f32)).astype(bf16)


def on_device(
    tokens,
    mix_gain,
    query_weight,
    key_weight,
    value_weight,
    conv_value_weight,
    conv_gate_weight,
    query_gain,
    key_gain,
    sink_logit,
    conv_taps,
    conv_gain,
    attn_proj,
    conv_proj,
):
    if fits(
        lax.axis_size("sp"),
        lax.axis_size("tp"),
        tokens,
        query_weight,
        key_weight,
        conv_value_weight,
        attn_proj,
        conv_taps,
        query_gain.shape[0],
    ):
        return fused(
            tokens,
            mix_gain,
            query_weight,
            key_weight,
            value_weight,
            conv_value_weight,
            conv_gate_weight,
            query_gain,
            key_gain,
            sink_logit,
            conv_taps,
            conv_gain,
            attn_proj,
            conv_proj,
        )
    count = tokens.shape[0]
    shards = (query_weight, conv_value_weight, conv_gate_weight, key_weight, value_weight)
    whole, joined = gather_both(tokens, jnp.concatenate(shards, axis=1))
    normed = unit_rows(whole.astype(jnp.float32), mix_gain).astype(jnp.bfloat16)
    product = jnp.dot(normed, joined, preferred_element_type=jnp.float32)
    cuts = []
    for shard in shards[:-1]:
        cuts.append((cuts[-1] if cuts else 0) + shard.shape[1])
    query, conv_value, conv_gate, key_part, value_part = jnp.split(product, cuts, axis=1)
    head_size = query_gain.shape[0]
    local_kv = key_part.shape[1] // head_size
    group = query.shape[1] // head_size // local_kv
    queries = unit_rows(query.reshape(count, local_kv, group, head_size), query_gain).astype(
        jnp.bfloat16
    )
    keys_normed = (
        unit_rows(key_part.reshape(count, local_kv, head_size), key_gain)
        .astype(jnp.bfloat16)
        .reshape(count, -1)
    )
    values_cast = value_part.astype(jnp.bfloat16)
    gated = (conv_value * jax.nn.sigmoid(conv_gate)).astype(jnp.bfloat16)
    reach = (conv_taps.shape[0] - 1) // 2
    kv_width = keys_normed.shape[1]
    paired = jnp.concatenate([keys_normed, values_cast], axis=1)
    extended = padded(paired, (("sp", 0),), WINDOW)
    key_rows = extended[:, :kv_width]
    value_rows = extended[:, kv_width:]
    conv_rows = padded(gated, (("sp", 0),), reach)
    offset = lax.axis_index("sp") * count
    total = count * lax.axis_size("sp")
    span_rows = key_rows.shape[0]
    attended = attend(
        queries,
        key_rows.reshape(span_rows, local_kv, head_size),
        value_rows.reshape(span_rows, local_kv, head_size),
        sink_logit,
        offset,
        total,
    )
    convolved = depthwise(conv_rows, conv_taps, count)
    channels, tp = conv_taps.shape[1], lax.axis_size("tp")
    local_mean = jnp.mean(convolved, axis=1)
    local_square = jnp.sum(jnp.square(convolved - local_mean[:, None]), axis=1)
    slot = (jnp.arange(tp) == lax.axis_index("tp")).astype(jnp.float32)[:, None, None]
    every = lax.psum(slot * jnp.stack([local_mean, local_square])[None], "tp")
    center = jnp.mean(every[:, 0], axis=0)
    spread = jnp.sum(every[:, 1] + channels * jnp.square(every[:, 0] - center), axis=0)
    spread = spread / (channels * tp)
    centered = convolved - center[:, None]
    featured = jax.nn.silu(centered * lax.rsqrt(spread[:, None] + EPSILON) * conv_gain).astype(
        jnp.bfloat16
    )
    stacked, _ = lax.optimization_barrier((jnp.concatenate([attn_proj, conv_proj], axis=0), joined))
    proj_full = lax.all_gather(stacked, "sp", axis=1, tiled=True)
    mixers = jnp.concatenate([attended, featured], axis=1)
    partial = jnp.dot(mixers, proj_full, preferred_element_type=jnp.float32).astype(jnp.bfloat16)
    return lax.psum_scatter(partial, "tp", scatter_dimension=0, tiled=True)


def solution(mesh):
    placed = (
        P("sp", "tp"),
        P(),
        P("sp", "tp"),
        P("sp", "tp"),
        P("sp", "tp"),
        P("sp", "tp"),
        P("sp", "tp"),
        P(),
        P(),
        P("tp"),
        P(None, "tp"),
        P("tp"),
        P("tp", "sp"),
        P("tp", "sp"),
    )
    return jax.shard_map(
        on_device, mesh=mesh, in_specs=placed, out_specs=P(("sp", "tp"), None), check_vma=False
    )
```

```python
import functools
import types

import jax
import jax.numpy as jnp
from jax import lax
from jax.experimental import pallas as pl
from jax.experimental.pallas import tpu as pltpu
from jax.sharding import PartitionSpec as P

WINDOW = 128


EPSILON = 0.1


def padded(value, sides, width):
    for axis, dim in sides:
        size, length = (lax.axis_size(axis), value.shape[dim])
        up = [(i, (i + 1) % size) for i in range(size - 1)]
        down = [(j, i) for i, j in up]
        last = lax.slice_in_dim(value, length - width, length, axis=dim)
        leading = lax.slice_in_dim(value, 0, width, axis=dim)
        before = lax.ppermute(last, axis, up)
        after = lax.ppermute(leading, axis, down)
        value = jnp.concatenate([before, value, after], axis=dim)
    return value


def unit_rows(values, gain):
    return values * lax.rsqrt(jnp.mean(values * values, axis=-1, keepdims=True) + EPSILON) * gain


def attend(queries, keys, values, sinks, offset, total):
    count, local_kv, group, size = queries.shape
    scale = size ** (-0.5)
    blocks = count // WINDOW
    span = 3 * WINDOW

    def windows(rows):
        cut = rows.reshape(blocks + 2, WINDOW, local_kv, size)
        return jnp.concatenate([cut[:blocks], cut[1 : blocks + 1], cut[2:]], axis=1)

    cut_queries = queries.reshape(blocks, WINDOW, local_kv, group, size)
    scores = jnp.einsum(
        "bqkgd,bskd->bkgqs", cut_queries, windows(keys), preferred_element_type=jnp.float32
    )
    query_row = jnp.arange(WINDOW, dtype=jnp.int32)[None, :, None]
    key_row = jnp.arange(span, dtype=jnp.int32)[None, None, :] - WINDOW
    key_pos = offset + WINDOW * jnp.arange(blocks, dtype=jnp.int32)[:, None, None] + key_row
    allowed = (jnp.abs(key_row - query_row) <= WINDOW) & (key_pos >= 0) & (key_pos < total)
    weights = jnp.where(allowed[:, None, None], jnp.exp(scores * scale), 0.0)
    denominator = jnp.sum(weights, axis=-1) + jnp.exp(sinks).reshape(local_kv, group, 1)
    shares = (weights / denominator[..., None]).astype(jnp.bfloat16)
    result = jnp.einsum(
        "bkgqs,bskd->bqkgd", shares, windows(values), preferred_element_type=jnp.float32
    )
    return result.reshape(count, -1).astype(jnp.bfloat16)


def depthwise(extended, kernel_taps, count):
    result = jnp.zeros((count, kernel_taps.shape[1]), jnp.float32)
    for offset in range(kernel_taps.shape[0]):
        result = result + kernel_taps[offset] * extended[offset : offset + count]
    return result


def snake(size):
    if size % 2:
        return (lambda index: index), (lambda place: place)
    half = size // 2

    def place_of(index):
        odd = index % 2
        return (index // 2) * (1 - odd) + (size - 1 - index // 2) * odd

    def index_of(place):
        back = place // half
        return 2 * place * (1 - back) + (2 * (size - 1 - place) + 1) * back

    return place_of, index_of


def plain(size):
    return (lambda index: index), (lambda place: place)


def gather_kernel(rings, *refs):
    count = len(rings)
    shards, outs = refs[:count], refs[count : 2 * count]
    local_sem = refs[2 * count]
    sems = refs[2 * count + 1 :]
    barrier = pltpu.get_barrier_semaphore()
    plans = []
    for number, (axis, size, dim, order) in enumerate(rings):
        place_of, index_of = order(size)
        place = place_of(lax.axis_index(axis))
        at = lambda shift, p=place, f=index_of, n=size: f((p + shift + n) % n)
        plans.append((axis, size, dim, at, shards[number], outs[number], sems[2 * number : 2 * number + 2]))
        for shift in (1, -1):
            pl.semaphore_signal(
                barrier, inc=1, device_id={axis: at(shift)}, device_id_type=pl.DeviceIdType.MESH
            )

    def window(out, dim, shard, index, low, high):
        rows, columns = shard.shape
        if dim == 0:
            begin = pl.multiple_of(index * rows + low, 16)
            return out.at[pl.ds(begin, high - low), :]
        return out.at[pl.ds(low, high - low), pl.ds(pl.multiple_of(index * columns, 128), columns)]

    local = []
    for number, (axis, size, dim, at, shard, out, _) in enumerate(plans):
        copy = pltpu.make_async_copy(
            shard, window(out, dim, shard, at(0), 0, shard.shape[0]), local_sem.at[number]
        )
        copy.start()
        local.append(copy)
    pl.semaphore_wait(barrier, 2 * count)

    def hop(plan, step, way):
        axis, size, dim, at, shard, out, (send, recv) = plan
        rows = shard.shape[0]
        low, high = 0, rows
        if 2 * step == size:
            low, high = (0, rows // 2) if way == 1 else (rows // 2, rows)
        owner = at(-way * (step - 1))
        target = window(out, dim, shard, owner, low, high)
        source = shard.at[pl.ds(low, high - low), :] if step == 1 else target
        slot = 2 * (step - 1) + (way + 1) // 2
        return pltpu.make_async_remote_copy(
            src_ref=source,
            dst_ref=target,
            send_sem=send.at[slot],
            recv_sem=recv.at[slot],
            device_id={axis: at(way)},
            device_id_type=pl.DeviceIdType.MESH,
        )

    pending = {}
    steps = [(n, s) for n, plan in enumerate(plans) for s in range(1, plan[1] // 2 + 1)]
    steps.sort(key=lambda item: ((item[1] - 1) / (plans[item[0]][1] // 2), -plans[item[0]][1]))
    for number, step in steps:
        for way in (1, -1):
            if step > 1:
                pending[number, step - 1, way].wait_recv()
            copy = hop(plans[number], step, way)
            copy.start()
            pending[number, step, way] = copy
    for number, plan in enumerate(plans):
        for way in (1, -1):
            pending[number, plan[1] // 2, way].wait_recv()
    for copy in pending.values():
        copy.wait_send()
    for copy in local:
        copy.wait()


def gather_both(tokens, joined):
    tp, sp = lax.axis_size("tp"), lax.axis_size("sp")
    rings = (("tp", tp, 1, plain), ("sp", sp, 0, snake))
    sems = []
    for _, size, _, _ in rings:
        sems += [pltpu.SemaphoreType.DMA((2 * (size // 2),))] * 2
    return pl.pallas_call(
        functools.partial(gather_kernel, rings),
        out_shape=(
            jax.ShapeDtypeStruct((tokens.shape[0], tokens.shape[1] * tp), tokens.dtype),
            jax.ShapeDtypeStruct((joined.shape[0] * sp, joined.shape[1]), joined.dtype),
        ),
        in_specs=[pl.BlockSpec(memory_space=pltpu.VMEM)] * 2,
        out_specs=[pl.BlockSpec(memory_space=pl.ANY)] * 2,
        scratch_shapes=[pltpu.SemaphoreType.DMA((2,))] + sems,
        compiler_params=pltpu.CompilerParams(collective_id=0, has_side_effects=True),
    )(tokens, joined)


LANES = 128
MESH = pl.DeviceIdType.MESH


def remote(source, target, sems, where):
    return pltpu.make_async_remote_copy(
        src_ref=source,
        dst_ref=target,
        send_sem=sems[0],
        recv_sem=sems[1],
        device_id=where,
        device_id_type=MESH,
    )


def contract_last(left, right):
    return lax.dot_general(
        left, right, (((1,), (1,)), ((), ())), preferred_element_type=jnp.float32
    )


def matmul(left, right):
    return jnp.dot(left, right, preferred_element_type=jnp.float32)


def lane_index(shape):
    return lax.broadcasted_iota(jnp.int32, shape, len(shape) - 1)


def row_index(shape):
    return lax.broadcasted_iota(jnp.int32, shape, len(shape) - 2)


def aligned(value, multiple):
    return value if isinstance(value, int) else pl.multiple_of(value, multiple)


class Ring:
    def __init__(self, size, groups, sems):
        place_of, index_of = snake(size)
        place = place_of(lax.axis_index("sp"))
        self.at = lambda shift: index_of((place + shift + size) % size)
        self.half = size // 2
        self.groups = groups
        self.sems = sems
        self.copies = {}
        self.arrived = None

    def part(self, group, step, piece, way):
        whole, up, down = self.groups[group][piece]
        if step < self.half:
            return whole
        return None if step > self.half else up if way == 1 else down

    def send(self, group, step, piece, way, source=None):
        ref = self.part(group, step, piece, way)(self.at(-way * (step - 1)))
        copy = remote(ref if source is None else source, ref, next(self.sems), {"sp": self.at(way)})
        copy.start()
        self.copies[group, step, piece, way] = copy

    def first(self, group, sources=None):
        for piece in range(len(self.groups[group])):
            for way in (1, -1):
                self.send(group, 1, piece, way, None if sources is None else sources[piece])

    def take(self, group, step, piece=None):
        for number in range(len(self.groups[group])):
            for way in (1, -1):
                if piece not in (None, number * 2 // len(self.groups[group])) or self.part(group, step, number, way) is None:
                    continue
                with jax.named_scope(f"ring{group}_{step}_{number}"):
                    self.copies[group, step, number, way].wait_recv()
                if self.part(group, step + 1, number, way) is not None:
                    self.send(group, step + 1, number, way)
                if self.arrived is not None:
                    self.arrived(group, step, number, way)

    def slot(self, step, way):
        return 2 * self.half - 1 if step == self.half else 2 * step - (1 if way == 1 else 0)

    def owner(self, slot):
        step = (slot + 1) // 2
        return self.at(-step if slot % 2 else step)


def scoped(name):
    def wrap(call):
        def inner(*args):
            with jax.named_scope(name):
                return call(*args)

        return inner

    return wrap


def fused_kernel(sp, names, *all_refs):
    ref = types.SimpleNamespace(**dict(zip(names, all_refs)))
    tokens, query_w, taps_w = ref.tokens, ref.query_w, ref.conv_taps
    whole, normed, gated, convolved = ref.whole, ref.normed, ref.gated, ref.convolved
    query_all, kv_all = ref.query_all, ref.kv_all
    value_all, gate_all = ref.value_all, ref.gate_all
    proj_all, proj_other = ref.proj_all, ref.proj_other
    taps, sinks, mix_rows, conv_gains = ref.taps, ref.sinks, ref.mix_rows, ref.conv_gains
    spread_heads, head_gains = ref.spread_heads, ref.head_gains
    band, eye = ref.band, ref.eye
    stat_out, stat_in, stat_rows = ref.stat_out, ref.stat_in, ref.stat_rows
    queries, query_part = ref.queries, ref.query_part
    key_low, key_high = ref.key_low, ref.key_high
    value_low, value_high = ref.value_low, ref.value_high
    mixers, mixers_other = ref.mixers, ref.mixers_other
    near_out, far_in, far_out = ref.near_out, ref.far_in, ref.far_out

    count, features = tokens.shape
    depth, width = query_w.shape
    model = features * 4
    columns = ref.attn_p.shape[1]
    thin = columns // 2
    block = count // 4
    half_pad = (gated.shape[1] - count) // 2
    reach = (taps.shape[0] - 1) // 2
    head = LANES // 2
    channels = taps.shape[1]
    blocks = count // LANES
    s, t = lax.axis_index("sp"), lax.axis_index("tp")
    a, c = t // 2, t % 2
    inner, outer = t + 1 - 2 * c, (t + 2) % 4
    cross = outer + 1 - 2 * c
    send_sem, recv_sem, local_sem = ref.send_sem, ref.recv_sem, ref.local_sem

    def sem_pairs():
        for i in range(recv_sem.shape[0]):
            yield send_sem, recv_sem.at[i]

    sems = sem_pairs()
    sent = []

    def push(source, target, where, pair=None):
        copy = remote(source, target, pair or next(sems), where)
        copy.start()
        sent.append(copy)
        return copy

    def rows_of(owner, low, high):
        return pl.ds(pl.multiple_of(owner * depth + low, 16), high - low)

    def kv_columns(owner):
        return pl.ds(pl.multiple_of(owner * depth, LANES), depth)

    def out_columns(owner):
        return pl.ds(pl.multiple_of(owner * columns, LANES), columns)

    cut = depth // 4

    def piece_of(target, low, high):
        return lambda o: target.at[rows_of(o, low, high), :]

    def split_piece(target, low, high):
        middle = (low + high) // 2
        return tuple(
            piece_of(target, *span) for span in ((low, high), (low, middle), (middle, high))
        )

    def proj_piece(piece):
        spans = ((0, width + channels), (0, width), (width, width + channels))
        return tuple(
            (lambda o, low=low, high=high: proj_all.at[o, piece, pl.ds(low, high - low), :])
            for low, high in spans
        )

    ring = Ring(
        sp,
        (
            (split_piece(value_all, 0, depth), split_piece(gate_all, 0, depth)),
            (split_piece(kv_all, 0, depth),),
            tuple(split_piece(query_all, i * cut, (i + 1) * cut) for i in range(4)),
            (proj_piece(0), proj_piece(1)),
        ),
        sems,
    )
    half = ring.half

    barrier = pltpu.get_barrier_semaphore()
    following, preceding = (s + 1) % sp, (s + sp - 1) % sp
    near_devices = [{"sp": ring.at(1)}, {"sp": ring.at(-1)}, {"sp": following}, {"sp": preceding}]
    near_devices += [{"tp": inner}, {"tp": outer}, {"tp": cross}]
    for where in near_devices:
        pl.semaphore_signal(barrier, inc=1, device_id=where, device_id_type=MESH)
    local = []
    for source, target in (
            (tokens, whole.at[t]),
            (ref.key_w, ref.kv_own.at[pl.ds(0, head), :]),
            (ref.value_w, ref.kv_own.at[pl.ds(head, head), :]),
            (ref.mix_gain, mix_rows),
            (query_w, query_all.at[rows_of(s, 0, depth), :]),
            (ref.conv_value_w, value_all.at[rows_of(s, 0, depth), :]),
            (ref.conv_gate_w, gate_all.at[rows_of(s, 0, depth), :]),
            (ref.attn_p.at[:, :thin], proj_all.at[s, 0, pl.ds(0, width), :]),
            (ref.attn_p.at[:, thin:], proj_all.at[s, 1, pl.ds(0, width), :]),
            (ref.conv_p.at[:, :thin], proj_all.at[s, 0, pl.ds(width, channels), :]),
            (ref.conv_p.at[:, thin:], proj_all.at[s, 1, pl.ds(width, channels), :]),
            (taps_w, taps),
            (ref.sink_logit, sinks),
            (ref.conv_gain, conv_gains),
            (ref.query_gain, ref.query_gains),
            (ref.key_gain, ref.key_gains),
    ):
        copy = pltpu.make_async_copy(source, target, local_sem)
        copy.start()
        local.append(copy)
    with jax.named_scope("wait_barrier"):
        pl.semaphore_wait(barrier, len(near_devices))

    ring.first(0, (ref.conv_value_w, ref.conv_gate_w))
    over = []
    row_order = (0, 3, 1, 2)
    for i in row_order:
        rows = pl.ds(i * block, block)
        over.append(push(tokens.at[rows, :], whole.at[t, rows, :], {"tp": outer}))
    beside = push(tokens, whole.at[t], {"tp": inner})
    with jax.named_scope("wait_local"):
        for copy in local:
            copy.wait()

    turned = jnp.transpose(ref.kv_own[...].astype(jnp.float32))
    kv_all[rows_of(s, 0, depth), :] = turned.astype(jnp.bfloat16)
    square = (width, width)
    spread_heads[...] = jnp.where(
        row_index(square) // head == lane_index(square) // head, 1.0 / head, 0.0
    ).astype(jnp.bfloat16)
    tile = (LANES, LANES)
    row, lane = row_index(tile), lane_index(tile)
    band[0] = (lane >= row).astype(jnp.float32)
    band[1] = (lane <= row).astype(jnp.float32)
    eye[...] = (lane == row).astype(jnp.float32)
    exponent = head ** (-0.5) * 1.4426950408889634
    query_gain, key_gain = ref.query_gains[...], ref.key_gains[...]
    plain_lanes = jnp.ones_like(key_gain)
    head_gains[0:1, :] = jnp.concatenate([query_gain * exponent] * 4, axis=1)
    head_gains[1:2, :LANES] = jnp.concatenate([key_gain, plain_lanes], axis=1)
    ones_low = jnp.where(lane < head, 1.0, 0.0)
    for i in range(value_low.shape[0] // LANES):
        rows = pl.ds(i * LANES, LANES)
        low, high = ones_low, 1.0 - ones_low
        if i == 0:
            low, high = (jnp.where(s > 0, v, 0.0) for v in (low, high))
        if i == value_low.shape[0] // LANES - 1:
            low, high = (jnp.where(s < sp - 1, v, 0.0) for v in (low, high))
        value_low[rows, LANES:] = low.astype(jnp.bfloat16)
        value_high[rows, LANES:] = high.astype(jnp.bfloat16)

    step_rows = 64

    def norm_rows(i, carry):
        rows = pl.ds(pl.multiple_of(i * step_rows, step_rows), step_rows)
        total = jnp.zeros((step_rows, LANES), jnp.float32)
        for j in range(4):
            for k in range(features // LANES):
                x = whole[j, rows, k * LANES : (k + 1) * LANES].astype(jnp.float32)
                total = total + x * x
        mean = jnp.sum(total, axis=1, keepdims=True) * (1.0 / model)
        scale = jnp.broadcast_to(lax.rsqrt(mean + EPSILON), (step_rows, LANES))
        for j in range(4):
            for k in range(features // LANES):
                x = whole[j, rows, k * LANES : (k + 1) * LANES].astype(jnp.float32)
                place = j * (features // LANES) + k
                gain = mix_rows[place : place + 1, :]
                normed[rows, place * LANES : (place + 1) * LANES] = (x * scale * gain).astype(
                    jnp.bfloat16
                )
        return carry

    forwards = []

    def forward_tokens(i):
        with jax.named_scope("wait_over"):
            over[i].wait_recv()
        source = whole.at[outer, pl.ds(row_order[i] * block, block), :]
        forwards.append(push(source, source, {"tp": inner}))

    def norm_block(i):
        with jax.named_scope("wait_forward"):
            if i == 0:
                beside.wait_recv()
            forwards[i].wait_recv()
        with jax.named_scope("norm"):
            per = block // step_rows
            begin = row_order[i] * per
            lax.fori_loop(begin, begin + per, norm_rows, 0)

    edge_out, edge_in = ref.edge_out, ref.edge_in

    @scoped("gate")
    def gate_block(i):
        left = normed[i * block : (i + 1) * block, :]
        value = matmul(left, value_all[...])
        gate = matmul(left, gate_all[...])
        result = (value * jax.nn.sigmoid(gate)).astype(jnp.bfloat16)
        wide = result.astype(jnp.float32)
        for j in range(channels // LANES):
            gated[j, i * block + half_pad : (i + 1) * block + half_pad, :] = wide[
                :, j * LANES : (j + 1) * LANES
            ]
        if i == 0:
            edge_out[0] = result[:half_pad, :]
        if i == 3:
            edge_out[1] = result[block - half_pad :, :]

    def conv_rows(i, carry):
        start = i * LANES
        parts = []
        for j in range(channels // LANES):
            lanes = slice(j * LANES, (j + 1) * LANES)
            total = jnp.zeros((LANES, LANES), jnp.float32)
            first = half_pad - reach
            for shift in range(8):
                offsets = [o for o in range(first, first + 2 * reach + 1) if o % 8 == shift]
                high = offsets[-1] - shift
                rows = gated[j, pl.ds(start + shift, LANES + high), :]
                for o in offsets:
                    tap = taps[o - first : o - first + 1, lanes]
                    total = total + tap * rows[o - shift : o - shift + LANES]
            convolved[pl.ds(pl.multiple_of(start, LANES), LANES), lanes] = total
            parts.append(total)
        mean = jnp.sum(sum(parts[1:], parts[0]), axis=1, keepdims=True) * (1.0 / channels)
        squares = [jnp.square(part - mean) for part in parts]
        square_sum = jnp.sum(sum(squares[1:], squares[0]), axis=1, keepdims=True)
        stat_out[pl.ds(i, 1), :] = jnp.sum(mean * eye[...], axis=0, keepdims=True)
        stat_out[pl.ds(i + blocks, 1), :] = jnp.sum(square_sum * eye[...], axis=0, keepdims=True)
        return carry

    @scoped("conv")
    def convolve(low, high):
        lax.fori_loop(low, high, conv_rows, 0)

    quarter = blocks // 4

    def fill_edges():
        for side, edge in enumerate(edges):
            with jax.named_scope("wait_edge"):
                edge.wait_recv()
            inside = s > 0 if side == 0 else s < sp - 1
            values = jnp.where(inside, edge_in[side].astype(jnp.float32), 0.0)
            start = 0 if side == 0 else count + half_pad
            for j in range(channels // LANES):
                gated[j, start : start + half_pad, :] = values[:, j * LANES : (j + 1) * LANES]

    def head_scale(part):
        lanes = part.shape[1]
        mean = matmul((part * part).astype(jnp.bfloat16), spread_heads[:lanes, :lanes])
        return lax.rsqrt(mean + EPSILON)

    halo_out, halo_in = ref.halo_out, ref.halo_in

    def store_key_values(rows, low, inside=None):
        high = pltpu.roll(low, head, 1)
        is_low = lane_index(low.shape) < head
        key_low[rows, :] = jnp.where(is_low, low, 0.0).astype(jnp.bfloat16)
        key_high[rows, :] = jnp.where(is_low, 0.0, high).astype(jnp.bfloat16)
        keep_low = is_low if inside is None else is_low & inside
        keep_high = ~is_low if inside is None else ~is_low & inside
        value_low[rows, :LANES] = jnp.where(keep_low, high, 0.0).astype(jnp.bfloat16)
        value_high[rows, :LANES] = jnp.where(keep_high, low, 0.0).astype(jnp.bfloat16)

    @scoped("keys")
    def key_value_block(i, edge=None):
        begin = aligned(i * block, block)
        part = matmul(normed[pl.ds(begin, block), :], kv_all[...])
        scaled = part * head_scale(part) * head_gains[1:2, :LANES]
        low = jnp.where(lane_index(part.shape) < head, scaled, part)
        store_key_values(pl.ds(aligned(begin + WINDOW, WINDOW), block), low)
        if edge is not None:
            halo_out[edge] = low.astype(jnp.bfloat16)

    def push_halo(edge, last):
        where = {"sp": (s + sp + 2 * last - 1) % sp}
        source = halo_out.at[edge, pl.ds(aligned(last * (block - WINDOW), WINDOW), WINDOW), :]
        return push(source, halo_in.at[1 - last], where)

    def fill_halo(copy, last):
        with jax.named_scope("wait_halo"):
            copy.wait_recv()
        outside = (s == 0) & (last == 1) | (s == sp - 1) & (last == 0)
        start = aligned((1 - last) * (WINDOW + count), WINDOW)
        low = halo_in[1 - last].astype(jnp.float32)
        store_key_values(pl.ds(start, WINDOW), low, ~outside)

    ring.take(0, 1)
    forward_tokens(0)
    norm_block(0)
    ring.take(0, 2)
    ring.first(1)
    forward_tokens(1)
    norm_block(1)
    for step in range(3, half):
        ring.take(0, step)
    ring.take(1, 1)
    ring.first(2)
    forward_tokens(2)
    norm_block(2)
    ring.take(0, half)
    gate_block(0)
    gate_block(3)
    edges = [
        push(edge_out.at[1], edge_in.at[0], {"sp": following}),
        push(edge_out.at[0], edge_in.at[1], {"sp": preceding}),
    ]
    ring.take(1, 2)
    forward_tokens(3)
    gate_block(1)
    ring.take(2, 1, 0)
    norm_block(3)
    ring.take(2, 1, 1)
    gate_block(2)
    convolve(1, quarter + 1)
    for step in range(3, half):
        ring.take(1, step)
    convolve(quarter + 1, 2 * quarter + 1)
    ring.take(2, 2, 0)
    convolve(2 * quarter + 1, blocks - 1)
    ring.take(2, 2, 1)
    fill_edges()
    convolve(0, 1)
    ring.take(1, half)
    convolve(blocks - 1, blocks)
    stat_pair, part_pair = next(sems), next(sems)
    for i, peer in enumerate((inner, outer, cross)):
        push(stat_out, stat_in.at[i], {"tp": peer}, stat_pair)
    for step in range(3, half - 1):
        ring.take(2, step)
    ring.take(2, half - 1, 0)
    key_value_block(3 * a, 0)
    far_halo = push_halo(0, a)
    ring.take(2, half - 1, 1)
    key_value_block(3 * (1 - a), 1)
    ring.first(3)
    near_halo = push_halo(1, 1 - a)
    key_value_block(1)
    key_value_block(2)

    def feature_rows(i, carry):
        rows = pl.ds(pl.multiple_of(i * LANES, LANES), LANES)
        middle = jnp.sum(stat_rows[pl.ds(i, 1), :] * eye[...], axis=1, keepdims=True)
        scale = jnp.sum(stat_rows[pl.ds(i + blocks, 1), :] * eye[...], axis=1, keepdims=True)
        for j in range(channels // LANES):
            lanes = slice(j * LANES, (j + 1) * LANES)
            value = (convolved[rows, lanes] - middle) * scale * conv_gains[j : j + 1, :]
            mixers[rows, width + j * LANES : width + (j + 1) * LANES] = (
                value * jax.nn.sigmoid(value)
            ).astype(jnp.bfloat16)
        return carry

    starts = ((1 - a) * 2, a * 2)
    give = [pl.ds(pl.multiple_of((base + 1 - c) * block, block), block) for base in starts]
    keep = [pl.ds(pl.multiple_of((base + c) * block, block), block) for base in starts]

    @scoped("features")
    def features_of(f):
        low = starts[f] * (block // LANES)
        lax.fori_loop(low, low + blocks // 2, feature_rows, 0)
        return push(mixers.at[give[f], width:], mixers_other.at[f, :, width:], {"tp": inner})

    @scoped("partial")
    def partial_block(f, i):
        rows = pl.ds(pl.multiple_of((starts[f] + i) * block, block), block)
        owners = [ring.owner(slot) for slot in range(sp - 1)]
        left = jnp.concatenate([normed[rows, kv_columns(o)] for o in owners], axis=1)
        right = jnp.concatenate([query_all[rows_of(o, 0, depth), :] for o in owners], axis=0)
        query_part[i * block : (i + 1) * block, :] = matmul(left, right)

    both = [pl.ds(pl.multiple_of(base * block, block), 2 * block) for base in starts]

    @scoped("queries")
    def query_rows(f):
        owner = ring.owner(sp - 1)
        last = matmul(normed[both[f], kv_columns(owner)], query_all[rows_of(owner, 0, depth), :])
        part = query_part[...] + last
        queries[both[f], :] = (part * head_scale(part) * head_gains[0:1, :]).astype(jnp.bfloat16)

    for i in range(2):
        partial_block(0, i)
    with jax.named_scope("wait_stat"):
        remote(stat_in, stat_in, stat_pair, {"tp": inner}).wait_recv()
    every = [stat_out[...]] + [stat_in[i] for i in range(3)]
    means = [v[:blocks] for v in every]
    center = (means[0] + means[1] + means[2] + means[3]) * 0.25
    spread = sum(v[blocks:] for v in every) + channels * sum(jnp.square(m - center) for m in means)
    stat_rows[:blocks] = center
    stat_rows[blocks:] = lax.rsqrt(spread * (1.0 / (channels * 4)) + EPSILON)

    given_features = [features_of(0)]
    ring.take(2, half)
    query_rows(0)

    shared = {}

    def share(slot, piece):
        owner = ring.owner(slot)
        source, target = proj_all.at[owner, piece], proj_other.at[owner, piece]
        shared[slot, piece] = push(source, target, {"tp": inner})

    def arrived(group, step, piece, way):
        if step < half or way == -1:
            share(ring.slot(step, way), piece)

    ring.arrived = arrived
    share(0, 0)
    share(0, 1)
    head_lanes = lane_index((1, LANES)) < head
    sink_rows = [
        jnp.exp(jnp.where(head_lanes, sinks[2 * i], sinks[2 * i + 1])) for i in range(2)
    ]

    @scoped("attend")
    def attend_rows(first, windows):
        starts_at = [pl.multiple_of(first + w * WINDOW, WINDOW) for w in range(windows)]
        lefts = [
            jnp.concatenate([queries[pl.ds(b, WINDOW), lanes] for lanes in halves], axis=0)
            for b in starts_at
        ]
        shares, vals = [[] for _ in range(windows)], []
        for j in range(windows + 2):
            span = pl.ds(pl.multiple_of(first + j * WINDOW, WINDOW), WINDOW)
            readers = [w for w in range(windows) if 0 <= j - w <= 2]
            left = jnp.concatenate([lefts[w] for w in readers], axis=0)
            right = jnp.concatenate([key_low[span, :], key_high[span, :]], axis=0)
            weights = jnp.exp2(contract_last(left, right))
            for n, w in enumerate(readers):
                weight = weights[n * 2 * WINDOW : (n + 1) * 2 * WINDOW]
                if j - w != 1:
                    mask = band[(j - w) // 2]
                    mask = jnp.concatenate([mask, mask], axis=0)
                    weight = weight * jnp.concatenate([mask, mask], axis=1)
                shares[w].append(weight.astype(jnp.bfloat16))
            vals.append(jnp.concatenate([value_low[span, :], value_high[span, :]], axis=0))
        for w, b in enumerate(starts_at):
            right = jnp.concatenate(vals[w : w + 3], axis=0)
            total = matmul(jnp.concatenate(shares[w], axis=1), right)
            for j in range(2):
                piece = total[j * WINDOW : (j + 1) * WINDOW]
                mixers[pl.ds(b, WINDOW), halves[j]] = (
                    piece[:, :LANES] / (piece[:, LANES:] + sink_rows[j])
                ).astype(jnp.bfloat16)

    halves = (slice(0, LANES), slice(LANES, 2 * LANES))

    def attend_given(f, low=0, size=block):
        here = pl.multiple_of((starts[f] + 1 - c) * block + low, WINDOW)
        attend_rows(here, size // WINDOW)
        target = mixers_other.at[f, pl.ds(aligned(low, WINDOW), size), :width]
        return push(mixers.at[pl.ds(here, size), :width], target, {"tp": inner})

    def attend_kept(f, low=0, size=block):
        attend_rows((starts[f] + c) * block + low, size // WINDOW)

    @scoped("project")
    def project(f, slot, pieces=(0, 1), low=0, size=block):
        owner = ring.owner(slot)
        here = pl.ds(pl.multiple_of((starts[f] + c) * block + low, WINDOW), size)
        left = jnp.concatenate(
            [mixers[here, :], mixers_other[f, pl.ds(aligned(low, WINDOW), size), :]], axis=1
        )
        right = [
            jnp.concatenate([proj_all[owner, piece], proj_other[owner, piece]], axis=0)
            for piece in pieces
        ]
        return matmul(left, jnp.concatenate(right, axis=1))

    def wait_shared(slot, piece):
        with jax.named_scope("wait_shared"):
            shared[slot, piece].wait_recv()

    def send_piece(slot, piece):
        if slot:
            wait_shared(slot, piece)
        far_out[slot, piece] = project(0, slot, (piece,)).astype(jnp.bfloat16)
        target = far_in.at[:, half_columns(slot, piece)]
        push(far_out.at[slot, piece], target, {"tp": outer}, part_pair)

    def half_columns(slot, piece):
        begin = ring.owner(slot) * columns + piece * thin
        return pl.ds(pl.multiple_of(begin, LANES), thin)

    def keep_part(slot):
        near_out[:, out_columns(ring.owner(slot))] = project(1, slot)

    fill_halo(far_halo, a)
    given_heads = [attend_given(0)]
    attend_kept(0)
    given_features[0].wait_recv()
    for piece in range(2):
        wait_shared(0, piece)
    with jax.named_scope("wait_given"):
        given_heads[0].wait_recv()
    for piece in range(2):
        send_piece(0, piece)

    def near_heads():
        fill_halo(near_halo, 1 - a)
        given_heads.append(attend_given(1))

    def near_kept():
        attend_kept(1)
        with jax.named_scope("wait_given"):
            given_features[1].wait_recv()
            given_heads[1].wait_recv()

    work = [
        lambda: partial_block(1, 0),
        lambda: partial_block(1, 1),
        lambda: query_rows(1),
        lambda: given_features.append(features_of(1)),
        near_heads,
        near_kept,
        lambda: keep_part(0),
    ]

    def do_work(most):
        for _ in range(min(most, len(work))):
            work.pop(0)()

    counts = {(1, 0): (1, 0), (1, 1): (1, 2), (2, 0): (1, 1), (2, 1): (1, 2)}
    for step in range(1, half + 1):
        slots = (2 * step - 1, 2 * step) if step < half else (2 * step - 1,)
        for piece in range(2):
            ring.take(3, step, piece)
            before, after = counts.get((step, piece), (1, 1))
            do_work(before)
            for slot in slots:
                send_piece(slot, piece)
            if piece == 1:
                work += [functools.partial(keep_part, slot) for slot in slots]
            do_work(after)
    do_work(len(work))
    with jax.named_scope("wait_part"):
        remote(far_in, far_in, part_pair, {"tp": outer}).wait_recv()
    with jax.named_scope("wait_sends"):
        for copy in sent:
            copy.wait_send()
        for copy in ring.copies.values():
            copy.wait_send()


def recv_count(sp):
    return 9 * 2 * (sp // 2) + 2 * sp + 9 + 2 + 2 + 1 + 1 + 2 + 2


def fits(sp, tp, tokens, query_weight, key_weight, conv_weight, attn_proj, taps, head):
    return (
        tp == 4
        and sp % 2 == 0
        and sp >= 6
        and tokens.shape[0] % (4 * 2 * WINDOW) == 0
        and tokens.shape[1] % LANES == 0
        and WINDOW == LANES
        and 2 * head == LANES
        and key_weight.shape[1] == head
        and query_weight.shape[1] == 4 * head
        and conv_weight.shape[1] == 4 * head
        and query_weight.shape[0] % LANES == 0
        and attn_proj.shape[1] % (2 * LANES) == 0
        and taps.shape[0] <= 31
    )


def fused(
    tokens,
    mix_gain,
    query_weight,
    key_weight,
    value_weight,
    conv_value_weight,
    conv_gate_weight,
    query_gain,
    key_gain,
    sink_logit,
    conv_taps,
    conv_gain,
    attn_proj,
    conv_proj,
):
    sp = lax.axis_size("sp")
    count, features = tokens.shape
    model = features * 4
    depth, width = query_weight.shape
    head = query_gain.shape[0]
    channels = conv_taps.shape[1]
    columns = attn_proj.shape[1]
    block = count // 4
    bf16, f32 = jnp.bfloat16, jnp.float32
    half_pad = 16
    stat = 2 * count // LANES
    padded_rows = count + 2 * WINDOW
    vmem, dma = pltpu.VMEM, pltpu.SemaphoreType.DMA
    inputs = dict(
        tokens=tokens,
        query_w=query_weight,
        key_w=key_weight.T,
        value_w=value_weight.T,
        conv_value_w=conv_value_weight,
        conv_gate_w=conv_gate_weight,
        attn_p=attn_proj,
        conv_p=conv_proj,
        mix_gain=mix_gain.reshape(-1, LANES),
        conv_gain=conv_gain.reshape(-1, LANES),
        query_gain=query_gain.reshape(1, -1),
        key_gain=key_gain.reshape(1, -1),
        sink_logit=sink_logit,
        conv_taps=conv_taps,
    )
    outputs = dict(
        near_out=vmem((block, model), f32),
        far_in=vmem((block, model), bf16),
    )
    scratch = dict(
        whole=vmem((4, count, features), bf16),
        normed=vmem((count, model), bf16),
        query_all=vmem((model, width), bf16),
        kv_own=vmem((2 * head, depth), bf16),
        kv_all=vmem((model, 2 * head), bf16),
        value_all=vmem((model, channels), bf16),
        gate_all=vmem((model, channels), bf16),
        proj_all=vmem((sp, 2, width + channels, columns // 2), bf16),
        proj_other=vmem((sp, 2, width + channels, columns // 2), bf16),
        taps=vmem(conv_taps.shape, f32),
        sinks=pltpu.SMEM(sink_logit.shape, f32),
        mix_rows=vmem((model // LANES, LANES), f32),
        conv_gains=vmem((channels // LANES, LANES), f32),
        query_gains=vmem((1, head), f32),
        key_gains=vmem((1, head), f32),
        head_gains=vmem((2, width), f32),
        spread_heads=vmem((width, width), bf16),
        band=vmem((2, LANES, LANES), f32),
        eye=vmem((LANES, LANES), f32),
        gated=vmem((channels // LANES, count + 2 * half_pad, LANES), f32),
        edge_out=vmem((2, half_pad, channels), bf16),
        edge_in=vmem((2, half_pad, channels), bf16),
        convolved=vmem((count, channels), f32),
        stat_out=vmem((stat, LANES), f32),
        stat_in=vmem((3, stat, LANES), f32),
        stat_rows=vmem((stat, LANES), f32),
        queries=vmem((count, width), bf16),
        query_part=vmem((2 * block, width), f32),
        key_low=vmem((padded_rows, LANES), bf16),
        key_high=vmem((padded_rows, LANES), bf16),
        value_low=vmem((padded_rows, 2 * LANES), bf16),
        value_high=vmem((padded_rows, 2 * LANES), bf16),
        halo_out=vmem((2, block, LANES), bf16),
        halo_in=vmem((2, WINDOW, LANES), bf16),
        mixers=vmem((count, width + channels), bf16),
        mixers_other=vmem((2, block, width + channels), bf16),
        far_out=vmem((sp, 2, block, columns // 2), bf16),
        local_sem=dma,
        send_sem=dma,
        recv_sem=dma((recv_count(sp),)),
    )
    near, far = pl.pallas_call(
        functools.partial(fused_kernel, sp, (*inputs, *outputs, *scratch)),
        out_shape=tuple(outputs.values()),
        in_specs=[pl.BlockSpec(memory_space=pltpu.HBM)] * len(inputs),
        out_specs=[pl.BlockSpec(memory_space=pltpu.VMEM)] * 2,
        scratch_shapes=list(scratch.values()),
        compiler_params=pltpu.CompilerParams(
            collective_id=1, has_side_effects=True, vmem_limit_bytes=60 * 2**20 + 2**19
        ),
    )(*inputs.values())
    return (near + far.astype(f32)).astype(bf16)


def on_device(
    tokens,
    mix_gain,
    query_weight,
    key_weight,
    value_weight,
    conv_value_weight,
    conv_gate_weight,
    query_gain,
    key_gain,
    sink_logit,
    conv_taps,
    conv_gain,
    attn_proj,
    conv_proj,
):
    if fits(
        lax.axis_size("sp"),
        lax.axis_size("tp"),
        tokens,
        query_weight,
        key_weight,
        conv_value_weight,
        attn_proj,
        conv_taps,
        query_gain.shape[0],
    ):
        return fused(
            tokens,
            mix_gain,
            query_weight,
            key_weight,
            value_weight,
            conv_value_weight,
            conv_gate_weight,
            query_gain,
            key_gain,
            sink_logit,
            conv_taps,
            conv_gain,
            attn_proj,
            conv_proj,
        )
    count = tokens.shape[0]
    shards = (query_weight, conv_value_weight, conv_gate_weight, key_weight, value_weight)
    whole, joined = gather_both(tokens, jnp.concatenate(shards, axis=1))
    normed = unit_rows(whole.astype(jnp.float32), mix_gain).astype(jnp.bfloat16)
    product = jnp.dot(normed, joined, preferred_element_type=jnp.float32)
    cuts = []
    for shard in shards[:-1]:
        cuts.append((cuts[-1] if cuts else 0) + shard.shape[1])
    query, conv_value, conv_gate, key_part, value_part = jnp.split(product, cuts, axis=1)
    head_size = query_gain.shape[0]
    local_kv = key_part.shape[1] // head_size
    group = query.shape[1] // head_size // local_kv
    queries = unit_rows(query.reshape(count, local_kv, group, head_size), query_gain).astype(
        jnp.bfloat16
    )
    keys_normed = (
        unit_rows(key_part.reshape(count, local_kv, head_size), key_gain)
        .astype(jnp.bfloat16)
        .reshape(count, -1)
    )
    values_cast = value_part.astype(jnp.bfloat16)
    gated = (conv_value * jax.nn.sigmoid(conv_gate)).astype(jnp.bfloat16)
    reach = (conv_taps.shape[0] - 1) // 2
    kv_width = keys_normed.shape[1]
    paired = jnp.concatenate([keys_normed, values_cast], axis=1)
    extended = padded(paired, (("sp", 0),), WINDOW)
    key_rows = extended[:, :kv_width]
    value_rows = extended[:, kv_width:]
    conv_rows = padded(gated, (("sp", 0),), reach)
    offset = lax.axis_index("sp") * count
    total = count * lax.axis_size("sp")
    span_rows = key_rows.shape[0]
    attended = attend(
        queries,
        key_rows.reshape(span_rows, local_kv, head_size),
        value_rows.reshape(span_rows, local_kv, head_size),
        sink_logit,
        offset,
        total,
    )
    convolved = depthwise(conv_rows, conv_taps, count)
    channels, tp = conv_taps.shape[1], lax.axis_size("tp")
    local_mean = jnp.mean(convolved, axis=1)
    local_square = jnp.sum(jnp.square(convolved - local_mean[:, None]), axis=1)
    slot = (jnp.arange(tp) == lax.axis_index("tp")).astype(jnp.float32)[:, None, None]
    every = lax.psum(slot * jnp.stack([local_mean, local_square])[None], "tp")
    center = jnp.mean(every[:, 0], axis=0)
    spread = jnp.sum(every[:, 1] + channels * jnp.square(every[:, 0] - center), axis=0)
    spread = spread / (channels * tp)
    centered = convolved - center[:, None]
    featured = jax.nn.silu(centered * lax.rsqrt(spread[:, None] + EPSILON) * conv_gain).astype(
        jnp.bfloat16
    )
    stacked, _ = lax.optimization_barrier((jnp.concatenate([attn_proj, conv_proj], axis=0), joined))
    proj_full = lax.all_gather(stacked, "sp", axis=1, tiled=True)
    mixers = jnp.concatenate([attended, featured], axis=1)
    partial = jnp.dot(mixers, proj_full, preferred_element_type=jnp.float32).astype(jnp.bfloat16)
    return lax.psum_scatter(partial, "tp", scatter_dimension=0, tiled=True)


def solution(mesh):
    placed = (
        P("sp", "tp"),
        P(),
        P("sp", "tp"),
        P("sp", "tp"),
        P("sp", "tp"),
        P("sp", "tp"),
        P("sp", "tp"),
        P(),
        P(),
        P("tp"),
        P(None, "tp"),
        P("tp"),
        P("tp", "sp"),
        P("tp", "sp"),
    )
    return jax.shard_map(
        on_device, mesh=mesh, in_specs=placed, out_specs=P(("sp", "tp"), None), check_vma=False
    )
```

```python
import functools
import types

import jax
import jax.numpy as jnp
from jax import lax
from jax.experimental import pallas as pl
from jax.experimental.pallas import tpu as pltpu
from jax.sharding import PartitionSpec as P

WINDOW = 128


EPSILON = 0.1


def padded(value, sides, width):
    for axis, dim in sides:
        size, length = (lax.axis_size(axis), value.shape[dim])
        up = [(i, (i + 1) % size) for i in range(size - 1)]
        down = [(j, i) for i, j in up]
        last = lax.slice_in_dim(value, length - width, length, axis=dim)
        leading = lax.slice_in_dim(value, 0, width, axis=dim)
        before = lax.ppermute(last, axis, up)
        after = lax.ppermute(leading, axis, down)
        value = jnp.concatenate([before, value, after], axis=dim)
    return value


def unit_rows(values, gain):
    return values * lax.rsqrt(jnp.mean(values * values, axis=-1, keepdims=True) + EPSILON) * gain


def attend(queries, keys, values, sinks, offset, total):
    count, local_kv, group, size = queries.shape
    scale = size ** (-0.5)
    blocks = count // WINDOW
    span = 3 * WINDOW

    def windows(rows):
        cut = rows.reshape(blocks + 2, WINDOW, local_kv, size)
        return jnp.concatenate([cut[:blocks], cut[1 : blocks + 1], cut[2:]], axis=1)

    cut_queries = queries.reshape(blocks, WINDOW, local_kv, group, size)
    scores = jnp.einsum(
        "bqkgd,bskd->bkgqs", cut_queries, windows(keys), preferred_element_type=jnp.float32
    )
    query_row = jnp.arange(WINDOW, dtype=jnp.int32)[None, :, None]
    key_row = jnp.arange(span, dtype=jnp.int32)[None, None, :] - WINDOW
    key_pos = offset + WINDOW * jnp.arange(blocks, dtype=jnp.int32)[:, None, None] + key_row
    allowed = (jnp.abs(key_row - query_row) <= WINDOW) & (key_pos >= 0) & (key_pos < total)
    weights = jnp.where(allowed[:, None, None], jnp.exp(scores * scale), 0.0)
    denominator = jnp.sum(weights, axis=-1) + jnp.exp(sinks).reshape(local_kv, group, 1)
    shares = (weights / denominator[..., None]).astype(jnp.bfloat16)
    result = jnp.einsum(
        "bkgqs,bskd->bqkgd", shares, windows(values), preferred_element_type=jnp.float32
    )
    return result.reshape(count, -1).astype(jnp.bfloat16)


def depthwise(extended, kernel_taps, count):
    result = jnp.zeros((count, kernel_taps.shape[1]), jnp.float32)
    for offset in range(kernel_taps.shape[0]):
        result = result + kernel_taps[offset] * extended[offset : offset + count]
    return result


def snake(size):
    if size % 2:
        return (lambda index: index), (lambda place: place)
    half = size // 2

    def place_of(index):
        odd = index % 2
        return (index // 2) * (1 - odd) + (size - 1 - index // 2) * odd

    def index_of(place):
        back = place // half
        return 2 * place * (1 - back) + (2 * (size - 1 - place) + 1) * back

    return place_of, index_of


def plain(size):
    return (lambda index: index), (lambda place: place)


def gather_kernel(rings, *refs):
    count = len(rings)
    shards, outs = refs[:count], refs[count : 2 * count]
    local_sem = refs[2 * count]
    sems = refs[2 * count + 1 :]
    barrier = pltpu.get_barrier_semaphore()
    plans = []
    for number, (axis, size, dim, order) in enumerate(rings):
        place_of, index_of = order(size)
        place = place_of(lax.axis_index(axis))
        at = lambda shift, p=place, f=index_of, n=size: f((p + shift + n) % n)
        plans.append((axis, size, dim, at, shards[number], outs[number], sems[2 * number : 2 * number + 2]))
        for shift in (1, -1):
            pl.semaphore_signal(
                barrier, inc=1, device_id={axis: at(shift)}, device_id_type=pl.DeviceIdType.MESH
            )

    def window(out, dim, shard, index, low, high):
        rows, columns = shard.shape
        if dim == 0:
            begin = pl.multiple_of(index * rows + low, 16)
            return out.at[pl.ds(begin, high - low), :]
        return out.at[pl.ds(low, high - low), pl.ds(pl.multiple_of(index * columns, 128), columns)]

    local = []
    for number, (axis, size, dim, at, shard, out, _) in enumerate(plans):
        copy = pltpu.make_async_copy(
            shard, window(out, dim, shard, at(0), 0, shard.shape[0]), local_sem.at[number]
        )
        copy.start()
        local.append(copy)
    pl.semaphore_wait(barrier, 2 * count)

    def hop(plan, step, way):
        axis, size, dim, at, shard, out, (send, recv) = plan
        rows = shard.shape[0]
        low, high = 0, rows
        if 2 * step == size:
            low, high = (0, rows // 2) if way == 1 else (rows // 2, rows)
        owner = at(-way * (step - 1))
        target = window(out, dim, shard, owner, low, high)
        source = shard.at[pl.ds(low, high - low), :] if step == 1 else target
        slot = 2 * (step - 1) + (way + 1) // 2
        return pltpu.make_async_remote_copy(
            src_ref=source,
            dst_ref=target,
            send_sem=send.at[slot],
            recv_sem=recv.at[slot],
            device_id={axis: at(way)},
            device_id_type=pl.DeviceIdType.MESH,
        )

    pending = {}
    steps = [(n, s) for n, plan in enumerate(plans) for s in range(1, plan[1] // 2 + 1)]
    steps.sort(key=lambda item: ((item[1] - 1) / (plans[item[0]][1] // 2), -plans[item[0]][1]))
    for number, step in steps:
        for way in (1, -1):
            if step > 1:
                pending[number, step - 1, way].wait_recv()
            copy = hop(plans[number], step, way)
            copy.start()
            pending[number, step, way] = copy
    for number, plan in enumerate(plans):
        for way in (1, -1):
            pending[number, plan[1] // 2, way].wait_recv()
    for copy in pending.values():
        copy.wait_send()
    for copy in local:
        copy.wait()


def gather_both(tokens, joined):
    tp, sp = lax.axis_size("tp"), lax.axis_size("sp")
    rings = (("tp", tp, 1, plain), ("sp", sp, 0, snake))
    sems = []
    for _, size, _, _ in rings:
        sems += [pltpu.SemaphoreType.DMA((2 * (size // 2),))] * 2
    return pl.pallas_call(
        functools.partial(gather_kernel, rings),
        out_shape=(
            jax.ShapeDtypeStruct((tokens.shape[0], tokens.shape[1] * tp), tokens.dtype),
            jax.ShapeDtypeStruct((joined.shape[0] * sp, joined.shape[1]), joined.dtype),
        ),
        in_specs=[pl.BlockSpec(memory_space=pltpu.VMEM)] * 2,
        out_specs=[pl.BlockSpec(memory_space=pl.ANY)] * 2,
        scratch_shapes=[pltpu.SemaphoreType.DMA((2,))] + sems,
        compiler_params=pltpu.CompilerParams(collective_id=0, has_side_effects=True),
    )(tokens, joined)


LANES = 128
MESH = pl.DeviceIdType.MESH


def remote(source, target, sems, where):
    return pltpu.make_async_remote_copy(
        src_ref=source,
        dst_ref=target,
        send_sem=sems[0],
        recv_sem=sems[1],
        device_id=where,
        device_id_type=MESH,
    )


def contract_last(left, right):
    return lax.dot_general(
        left, right, (((1,), (1,)), ((), ())), preferred_element_type=jnp.float32
    )


def matmul(left, right):
    return jnp.dot(left, right, preferred_element_type=jnp.float32)


def lane_index(shape):
    return lax.broadcasted_iota(jnp.int32, shape, len(shape) - 1)


def row_index(shape):
    return lax.broadcasted_iota(jnp.int32, shape, len(shape) - 2)


def aligned(value, multiple):
    return value if isinstance(value, int) else pl.multiple_of(value, multiple)


class Ring:
    def __init__(self, size, groups, sems):
        place_of, index_of = snake(size)
        place = place_of(lax.axis_index("sp"))
        self.at = lambda shift: index_of((place + shift + size) % size)
        self.half = size // 2
        self.groups = groups
        self.sems = sems
        self.copies = {}
        self.arrived = None

    def part(self, group, step, piece, way):
        whole, up, down = self.groups[group][piece]
        if step < self.half:
            return whole
        return None if step > self.half else up if way == 1 else down

    def send(self, group, step, piece, way, source=None, hold=False):
        ref = self.part(group, step, piece, way)(self.at(-way * (step - 1)))
        copy = remote(ref if source is None else source, ref, next(self.sems), {"sp": self.at(way)})
        self.copies[group, step, piece, way] = copy
        if not hold:
            copy.start()

    def first(self, group, sources=None, hold=False):
        for piece in range(len(self.groups[group])):
            for way in (1, -1):
                source = None if sources is None else sources[piece]
                self.send(group, 1, piece, way, source, hold)

    def start_first(self, group):
        for piece in range(len(self.groups[group])):
            for way in (1, -1):
                self.copies[group, 1, piece, way].start()

    def take(self, group, step, piece=None):
        for number in range(len(self.groups[group])):
            for way in (1, -1):
                if piece not in (None, number * 2 // len(self.groups[group])) or self.part(group, step, number, way) is None:
                    continue
                with jax.named_scope(f"ring{group}_{step}_{number}"):
                    self.copies[group, step, number, way].wait_recv()
                if self.part(group, step + 1, number, way) is not None:
                    self.send(group, step + 1, number, way)
                if self.arrived is not None:
                    self.arrived(group, step, number, way)

    def slot(self, step, way):
        return 2 * self.half - 1 if step == self.half else 2 * step - (1 if way == 1 else 0)

    def owner(self, slot):
        step = (slot + 1) // 2
        return self.at(-step if slot % 2 else step)


def scoped(name):
    def wrap(call):
        def inner(*args):
            with jax.named_scope(name):
                return call(*args)

        return inner

    return wrap


def fused_kernel(sp, names, *all_refs):
    ref = types.SimpleNamespace(**dict(zip(names, all_refs)))
    tokens, query_w, taps_w = ref.tokens, ref.query_w, ref.conv_taps
    whole, normed, gated, convolved = ref.whole, ref.normed, ref.gated, ref.convolved
    query_all, kv_all = ref.query_all, ref.kv_all
    value_all, gate_all = ref.value_all, ref.gate_all
    proj_all, proj_other = ref.proj_all, ref.proj_other
    taps, sinks, mix_rows, conv_gains = ref.taps, ref.sinks, ref.mix_rows, ref.conv_gains
    spread_heads, head_gains = ref.spread_heads, ref.head_gains
    band, eye = ref.band, ref.eye
    stat_out, stat_in, stat_rows = ref.stat_out, ref.stat_in, ref.stat_rows
    queries, query_part = ref.queries, ref.query_part
    key_low, key_high = ref.key_low, ref.key_high
    value_low, value_high = ref.value_low, ref.value_high
    mixers, mixers_other = ref.mixers, ref.mixers_other
    near_out, far_in, far_out = ref.near_out, ref.far_in, ref.far_out

    count, features = tokens.shape
    depth, width = query_w.shape
    model = features * 4
    columns = ref.attn_p.shape[1]
    thin = columns // 2
    block = count // 4
    half_pad = (gated.shape[1] - count) // 2
    reach = (taps.shape[0] - 1) // 2
    head = LANES // 2
    channels = taps.shape[1]
    blocks = count // LANES
    s, t = lax.axis_index("sp"), lax.axis_index("tp")
    a, c = t // 2, t % 2
    inner, outer = t + 1 - 2 * c, (t + 2) % 4
    cross = outer + 1 - 2 * c
    send_sem, recv_sem = ref.send_sem, ref.recv_sem
    local_sem, ahead_sem = ref.local_sem, ref.ahead_sem

    def sem_pairs():
        for i in range(recv_sem.shape[0]):
            yield send_sem, recv_sem.at[i]

    sems = sem_pairs()
    sent = []

    def push(source, target, where, pair=None):
        copy = remote(source, target, pair or next(sems), where)
        copy.start()
        sent.append(copy)
        return copy

    def rows_of(owner, low, high):
        return pl.ds(pl.multiple_of(owner * depth + low, 16), high - low)

    def kv_columns(owner):
        return pl.ds(pl.multiple_of(owner * depth, LANES), depth)

    def out_columns(owner):
        return pl.ds(pl.multiple_of(owner * columns, LANES), columns)

    cut = depth // 4

    def piece_of(target, low, high):
        return lambda o: target.at[rows_of(o, low, high), :]

    def split_piece(target, low, high):
        middle = (low + high) // 2
        return tuple(
            piece_of(target, *span) for span in ((low, high), (low, middle), (middle, high))
        )

    def proj_piece(piece):
        spans = ((0, width + channels), (0, width), (width, width + channels))
        return tuple(
            (lambda o, low=low, high=high: proj_all.at[o, piece, pl.ds(low, high - low), :])
            for low, high in spans
        )

    ring = Ring(
        sp,
        (
            (split_piece(value_all, 0, depth), split_piece(gate_all, 0, depth)),
            (split_piece(kv_all, 0, depth),),
            tuple(split_piece(query_all, i * cut, (i + 1) * cut) for i in range(4)),
            (proj_piece(0), proj_piece(1)),
        ),
        sems,
    )
    half = ring.half

    barrier = pltpu.get_barrier_semaphore()
    following, preceding = (s + 1) % sp, (s + sp - 1) % sp
    near_devices = [{"sp": ring.at(1)}, {"sp": ring.at(-1)}, {"sp": following}, {"sp": preceding}]
    near_devices += [{"tp": inner}, {"tp": outer}, {"tp": cross}]
    for where in near_devices:
        pl.semaphore_signal(barrier, inc=1, device_id=where, device_id_type=MESH)
    ahead = []
    for source, target in (
        (ref.conv_value_w, value_all.at[rows_of(s, 0, depth), :]),
        (ref.conv_gate_w, gate_all.at[rows_of(s, 0, depth), :]),
    ):
        copy = pltpu.make_async_copy(source, target, ahead_sem)
        copy.start()
        ahead.append(copy)
    local = []
    for source, target in (
            (tokens, whole.at[t]),
            (ref.key_w, ref.kv_own.at[pl.ds(0, head), :]),
            (ref.value_w, ref.kv_own.at[pl.ds(head, head), :]),
            (ref.mix_gain, mix_rows),
            (query_w, query_all.at[rows_of(s, 0, depth), :]),
            (ref.attn_p.at[:, :thin], proj_all.at[s, 0, pl.ds(0, width), :]),
            (ref.attn_p.at[:, thin:], proj_all.at[s, 1, pl.ds(0, width), :]),
            (ref.conv_p.at[:, :thin], proj_all.at[s, 0, pl.ds(width, channels), :]),
            (ref.conv_p.at[:, thin:], proj_all.at[s, 1, pl.ds(width, channels), :]),
            (taps_w, taps),
            (ref.sink_logit, sinks),
            (ref.conv_gain, conv_gains),
            (ref.query_gain, ref.query_gains),
            (ref.key_gain, ref.key_gains),
    ):
        copy = pltpu.make_async_copy(source, target, local_sem)
        copy.start()
        local.append(copy)
    with jax.named_scope("wait_barrier"):
        pl.semaphore_wait(barrier, len(near_devices))

    with jax.named_scope("wait_ahead"):
        for copy in ahead:
            copy.wait()
    ring.first(0)
    over = []
    row_order = (0, 3, 1, 2)
    for i in row_order:
        rows = pl.ds(i * block, block)
        over.append(push(tokens.at[rows, :], whole.at[t, rows, :], {"tp": outer}))
    beside = push(tokens, whole.at[t], {"tp": inner})
    with jax.named_scope("wait_local"):
        for copy in local:
            copy.wait()

    turned = jnp.transpose(ref.kv_own[...].astype(jnp.float32))
    kv_all[rows_of(s, 0, depth), :] = turned.astype(jnp.bfloat16)
    square = (width, width)
    spread_heads[...] = jnp.where(
        row_index(square) // head == lane_index(square) // head, 1.0 / head, 0.0
    ).astype(jnp.bfloat16)
    tile = (LANES, LANES)
    row, lane = row_index(tile), lane_index(tile)
    band[0] = (lane >= row).astype(jnp.float32)
    band[1] = (lane <= row).astype(jnp.float32)
    eye[...] = (lane == row).astype(jnp.float32)
    exponent = head ** (-0.5) * 1.4426950408889634
    query_gain, key_gain = ref.query_gains[...], ref.key_gains[...]
    plain_lanes = jnp.ones_like(key_gain)
    head_gains[0:1, :] = jnp.concatenate([query_gain * exponent] * 4, axis=1)
    head_gains[1:2, :LANES] = jnp.concatenate([key_gain, plain_lanes], axis=1)
    ones_low = jnp.where(lane < head, 1.0, 0.0)
    for i in range(value_low.shape[0] // LANES):
        rows = pl.ds(i * LANES, LANES)
        low, high = ones_low, 1.0 - ones_low
        if i == 0:
            low, high = (jnp.where(s > 0, v, 0.0) for v in (low, high))
        if i == value_low.shape[0] // LANES - 1:
            low, high = (jnp.where(s < sp - 1, v, 0.0) for v in (low, high))
        value_low[rows, LANES:] = low.astype(jnp.bfloat16)
        value_high[rows, LANES:] = high.astype(jnp.bfloat16)

    step_rows = 64

    def norm_rows(i, carry):
        rows = pl.ds(pl.multiple_of(i * step_rows, step_rows), step_rows)
        total = jnp.zeros((step_rows, LANES), jnp.float32)
        for j in range(4):
            for k in range(features // LANES):
                x = whole[j, rows, k * LANES : (k + 1) * LANES].astype(jnp.float32)
                total = total + x * x
        mean = jnp.sum(total, axis=1, keepdims=True) * (1.0 / model)
        scale = jnp.broadcast_to(lax.rsqrt(mean + EPSILON), (step_rows, LANES))
        for j in range(4):
            for k in range(features // LANES):
                x = whole[j, rows, k * LANES : (k + 1) * LANES].astype(jnp.float32)
                place = j * (features // LANES) + k
                gain = mix_rows[place : place + 1, :]
                normed[rows, place * LANES : (place + 1) * LANES] = (x * scale * gain).astype(
                    jnp.bfloat16
                )
        return carry

    forwards = []

    def forward_tokens(i):
        with jax.named_scope("wait_over"):
            over[i].wait_recv()
        source = whole.at[outer, pl.ds(row_order[i] * block, block), :]
        forwards.append(push(source, source, {"tp": inner}))

    def norm_block(i):
        with jax.named_scope("wait_forward"):
            if i == 0:
                beside.wait_recv()
            forwards[i].wait_recv()
        with jax.named_scope("norm"):
            per = block // step_rows
            begin = row_order[i] * per
            lax.fori_loop(begin, begin + per, norm_rows, 0)

    edge_out, edge_in = ref.edge_out, ref.edge_in

    @scoped("gate")
    def gate_block(i):
        left = normed[i * block : (i + 1) * block, :]
        value = matmul(left, value_all[...])
        gate = matmul(left, gate_all[...])
        result = (value * jax.nn.sigmoid(gate)).astype(jnp.bfloat16)
        wide = result.astype(jnp.float32)
        for j in range(channels // LANES):
            gated[j, i * block + half_pad : (i + 1) * block + half_pad, :] = wide[
                :, j * LANES : (j + 1) * LANES
            ]
        if i == 0:
            edge_out[0] = result[:half_pad, :]
        if i == 3:
            edge_out[1] = result[block - half_pad :, :]

    def conv_rows(i, carry):
        start = i * LANES
        parts = []
        for j in range(channels // LANES):
            lanes = slice(j * LANES, (j + 1) * LANES)
            total = jnp.zeros((LANES, LANES), jnp.float32)
            first = half_pad - reach
            for shift in range(8):
                offsets = [o for o in range(first, first + 2 * reach + 1) if o % 8 == shift]
                high = offsets[-1] - shift
                rows = gated[j, pl.ds(start + shift, LANES + high), :]
                for o in offsets:
                    tap = taps[o - first : o - first + 1, lanes]
                    total = total + tap * rows[o - shift : o - shift + LANES]
            convolved[pl.ds(pl.multiple_of(start, LANES), LANES), lanes] = total
            parts.append(total)
        mean = jnp.sum(sum(parts[1:], parts[0]), axis=1, keepdims=True) * (1.0 / channels)
        squares = [jnp.square(part - mean) for part in parts]
        square_sum = jnp.sum(sum(squares[1:], squares[0]), axis=1, keepdims=True)
        stat_out[pl.ds(i, 1), :] = jnp.sum(mean * eye[...], axis=0, keepdims=True)
        stat_out[pl.ds(i + blocks, 1), :] = jnp.sum(square_sum * eye[...], axis=0, keepdims=True)
        return carry

    @scoped("conv")
    def convolve(low, high):
        lax.fori_loop(low, high, conv_rows, 0)

    quarter = blocks // 4

    def fill_edges():
        for side, edge in enumerate(edges):
            with jax.named_scope("wait_edge"):
                edge.wait_recv()
            inside = s > 0 if side == 0 else s < sp - 1
            values = jnp.where(inside, edge_in[side].astype(jnp.float32), 0.0)
            start = 0 if side == 0 else count + half_pad
            for j in range(channels // LANES):
                gated[j, start : start + half_pad, :] = values[:, j * LANES : (j + 1) * LANES]

    def head_scale(part):
        lanes = part.shape[1]
        mean = matmul((part * part).astype(jnp.bfloat16), spread_heads[:lanes, :lanes])
        return lax.rsqrt(mean + EPSILON)

    halo_out, halo_in = ref.halo_out, ref.halo_in

    def store_key_values(rows, low, inside=None):
        high = pltpu.roll(low, head, 1)
        is_low = lane_index(low.shape) < head
        key_low[rows, :] = jnp.where(is_low, low, 0.0).astype(jnp.bfloat16)
        key_high[rows, :] = jnp.where(is_low, 0.0, high).astype(jnp.bfloat16)
        keep_low = is_low if inside is None else is_low & inside
        keep_high = ~is_low if inside is None else ~is_low & inside
        value_low[rows, :LANES] = jnp.where(keep_low, high, 0.0).astype(jnp.bfloat16)
        value_high[rows, :LANES] = jnp.where(keep_high, low, 0.0).astype(jnp.bfloat16)

    @scoped("keys")
    def key_value_block(i, edge=None):
        begin = aligned(i * block, block)
        part = matmul(normed[pl.ds(begin, block), :], kv_all[...])
        scaled = part * head_scale(part) * head_gains[1:2, :LANES]
        low = jnp.where(lane_index(part.shape) < head, scaled, part)
        store_key_values(pl.ds(aligned(begin + WINDOW, WINDOW), block), low)
        if edge is not None:
            halo_out[edge] = low.astype(jnp.bfloat16)

    def push_halo(edge, last):
        where = {"sp": (s + sp + 2 * last - 1) % sp}
        source = halo_out.at[edge, pl.ds(aligned(last * (block - WINDOW), WINDOW), WINDOW), :]
        return push(source, halo_in.at[1 - last], where)

    def fill_halo(copy, last):
        with jax.named_scope("wait_halo"):
            copy.wait_recv()
        outside = (s == 0) & (last == 1) | (s == sp - 1) & (last == 0)
        start = aligned((1 - last) * (WINDOW + count), WINDOW)
        low = halo_in[1 - last].astype(jnp.float32)
        store_key_values(pl.ds(start, WINDOW), low, ~outside)

    ring.take(0, 1)
    forward_tokens(0)
    norm_block(0)
    ring.take(0, 2)
    ring.first(1)
    forward_tokens(1)
    norm_block(1)
    for step in range(3, half):
        ring.take(0, step)
    ring.take(1, 1)
    ring.first(2)
    forward_tokens(2)
    norm_block(2)
    ring.take(0, half)
    gate_block(0)
    gate_block(3)
    edges = [
        push(edge_out.at[1], edge_in.at[0], {"sp": following}),
        push(edge_out.at[0], edge_in.at[1], {"sp": preceding}),
    ]
    ring.take(1, 2)
    forward_tokens(3)
    gate_block(1)
    ring.take(2, 1, 0)
    norm_block(3)
    ring.take(2, 1, 1)
    gate_block(2)
    convolve(1, 2)
    for step in range(3, half):
        ring.take(1, step)
    convolve(2, quarter + 2)
    ring.take(2, 2, 0)
    convolve(quarter + 2, 2 * quarter + 2)
    ring.take(2, 2, 1)
    convolve(2 * quarter + 2, blocks - 1)
    fill_edges()
    convolve(0, 1)
    ring.take(1, half)
    convolve(blocks - 1, blocks)
    stat_pair, part_pair = next(sems), next(sems)
    for i, peer in enumerate((inner, outer, cross)):
        push(stat_out, stat_in.at[i], {"tp": peer}, stat_pair)
    key_value_block(3 * a, 0)
    far_halo = push_halo(0, a)
    for step in range(3, half - 1):
        ring.take(2, step)
    ring.take(2, half - 1, 0)
    key_value_block(3 * (1 - a), 1)
    ring.take(2, half - 1, 1)
    ring.first(3, hold=True)
    pl.when(c == 0)(lambda: ring.start_first(3))
    near_halo = push_halo(1, 1 - a)
    key_value_block(1)
    key_value_block(2)
    pl.when(c == 1)(lambda: ring.start_first(3))

    def feature_rows(i, carry):
        rows = pl.ds(pl.multiple_of(i * LANES, LANES), LANES)
        middle = jnp.sum(stat_rows[pl.ds(i, 1), :] * eye[...], axis=1, keepdims=True)
        scale = jnp.sum(stat_rows[pl.ds(i + blocks, 1), :] * eye[...], axis=1, keepdims=True)
        for j in range(channels // LANES):
            lanes = slice(j * LANES, (j + 1) * LANES)
            value = (convolved[rows, lanes] - middle) * scale * conv_gains[j : j + 1, :]
            mixers[rows, width + j * LANES : width + (j + 1) * LANES] = (
                value * jax.nn.sigmoid(value)
            ).astype(jnp.bfloat16)
        return carry

    starts = ((1 - a) * 2, a * 2)
    give = [pl.ds(pl.multiple_of((base + 1 - c) * block, block), block) for base in starts]
    keep = [pl.ds(pl.multiple_of((base + c) * block, block), block) for base in starts]

    @scoped("features")
    def features_of(f):
        low = starts[f] * (block // LANES)
        lax.fori_loop(low, low + blocks // 2, feature_rows, 0)
        return push(mixers.at[give[f], width:], mixers_other.at[f, :, width:], {"tp": inner})

    @scoped("partial")
    def partial_block(f, i):
        rows = pl.ds(pl.multiple_of((starts[f] + i) * block, block), block)
        owners = [ring.owner(slot) for slot in range(sp - 1)]
        left = jnp.concatenate([normed[rows, kv_columns(o)] for o in owners], axis=1)
        right = jnp.concatenate([query_all[rows_of(o, 0, depth), :] for o in owners], axis=0)
        query_part[i * block : (i + 1) * block, :] = matmul(left, right)

    both = [pl.ds(pl.multiple_of(base * block, block), 2 * block) for base in starts]

    @scoped("queries")
    def query_rows(f):
        owner = ring.owner(sp - 1)
        last = matmul(normed[both[f], kv_columns(owner)], query_all[rows_of(owner, 0, depth), :])
        part = query_part[...] + last
        queries[both[f], :] = (part * head_scale(part) * head_gains[0:1, :]).astype(jnp.bfloat16)

    for i in range(2):
        partial_block(0, i)
    with jax.named_scope("wait_stat"):
        remote(stat_in, stat_in, stat_pair, {"tp": inner}).wait_recv()
    every = [stat_out[...]] + [stat_in[i] for i in range(3)]
    means = [v[:blocks] for v in every]
    center = (means[0] + means[1] + means[2] + means[3]) * 0.25
    spread = sum(v[blocks:] for v in every) + channels * sum(jnp.square(m - center) for m in means)
    stat_rows[:blocks] = center
    stat_rows[blocks:] = lax.rsqrt(spread * (1.0 / (channels * 4)) + EPSILON)

    given_features = [features_of(0)]
    ring.take(2, half)
    query_rows(0)

    shared = {}

    def share(slot, piece):
        owner = ring.owner(slot)
        source, target = proj_all.at[owner, piece], proj_other.at[owner, piece]
        shared[slot, piece] = push(source, target, {"tp": inner})

    def arrived(group, step, piece, way):
        if step < half or way == -1:
            share(ring.slot(step, way), piece)

    ring.arrived = arrived
    share(0, 0)
    share(0, 1)
    head_lanes = lane_index((1, LANES)) < head
    sink_rows = [
        jnp.exp(jnp.where(head_lanes, sinks[2 * i], sinks[2 * i + 1])) for i in range(2)
    ]

    @scoped("attend")
    def attend_rows(first, windows):
        starts_at = [pl.multiple_of(first + w * WINDOW, WINDOW) for w in range(windows)]
        lefts = [
            jnp.concatenate([queries[pl.ds(b, WINDOW), lanes] for lanes in halves], axis=0)
            for b in starts_at
        ]
        shares, vals = [[] for _ in range(windows)], []
        for j in range(windows + 2):
            span = pl.ds(pl.multiple_of(first + j * WINDOW, WINDOW), WINDOW)
            readers = [w for w in range(windows) if 0 <= j - w <= 2]
            left = jnp.concatenate([lefts[w] for w in readers], axis=0)
            right = jnp.concatenate([key_low[span, :], key_high[span, :]], axis=0)
            weights = jnp.exp2(contract_last(left, right))
            for n, w in enumerate(readers):
                weight = weights[n * 2 * WINDOW : (n + 1) * 2 * WINDOW]
                if j - w != 1:
                    mask = band[(j - w) // 2]
                    mask = jnp.concatenate([mask, mask], axis=0)
                    weight = weight * jnp.concatenate([mask, mask], axis=1)
                shares[w].append(weight.astype(jnp.bfloat16))
            vals.append(jnp.concatenate([value_low[span, :], value_high[span, :]], axis=0))
        for w, b in enumerate(starts_at):
            right = jnp.concatenate(vals[w : w + 3], axis=0)
            total = matmul(jnp.concatenate(shares[w], axis=1), right)
            for j in range(2):
                piece = total[j * WINDOW : (j + 1) * WINDOW]
                mixers[pl.ds(b, WINDOW), halves[j]] = (
                    piece[:, :LANES] / (piece[:, LANES:] + sink_rows[j])
                ).astype(jnp.bfloat16)

    halves = (slice(0, LANES), slice(LANES, 2 * LANES))

    def attend_given(f, low=0, size=block):
        here = pl.multiple_of((starts[f] + 1 - c) * block + low, WINDOW)
        attend_rows(here, size // WINDOW)
        target = mixers_other.at[f, pl.ds(aligned(low, WINDOW), size), :width]
        return push(mixers.at[pl.ds(here, size), :width], target, {"tp": inner})

    def attend_kept(f, low=0, size=block):
        attend_rows((starts[f] + c) * block + low, size // WINDOW)

    @scoped("project")
    def project(f, slot, pieces=(0, 1), low=0, size=block):
        owner = ring.owner(slot)
        here = pl.ds(pl.multiple_of((starts[f] + c) * block + low, WINDOW), size)
        left = jnp.concatenate(
            [mixers[here, :], mixers_other[f, pl.ds(aligned(low, WINDOW), size), :]], axis=1
        )
        right = [
            jnp.concatenate([proj_all[owner, piece], proj_other[owner, piece]], axis=0)
            for piece in pieces
        ]
        return matmul(left, jnp.concatenate(right, axis=1))

    def wait_shared(slot, piece):
        with jax.named_scope("wait_shared"):
            shared[slot, piece].wait_recv()

    def send_piece(slot, piece):
        if slot:
            wait_shared(slot, piece)
        far_out[slot, piece] = project(0, slot, (piece,)).astype(jnp.bfloat16)
        target = far_in.at[:, half_columns(slot, piece)]
        push(far_out.at[slot, piece], target, {"tp": outer}, part_pair)

    def half_columns(slot, piece):
        begin = ring.owner(slot) * columns + piece * thin
        return pl.ds(pl.multiple_of(begin, LANES), thin)

    def keep_part(slot):
        near_out[:, out_columns(ring.owner(slot))] = project(1, slot)

    fill_halo(far_halo, a)
    given_heads = [attend_given(0)]
    attend_kept(0)
    given_features[0].wait_recv()
    for piece in range(2):
        wait_shared(0, piece)
    with jax.named_scope("wait_given"):
        given_heads[0].wait_recv()
    for piece in range(2):
        send_piece(0, piece)

    def near_heads():
        fill_halo(near_halo, 1 - a)
        given_heads.append(attend_given(1))

    def near_kept():
        attend_kept(1)
        with jax.named_scope("wait_given"):
            given_features[1].wait_recv()
            given_heads[1].wait_recv()

    work = [
        lambda: partial_block(1, 0),
        lambda: partial_block(1, 1),
        lambda: query_rows(1),
        lambda: given_features.append(features_of(1)),
        near_heads,
        near_kept,
        lambda: keep_part(0),
    ]

    def do_work(most):
        for _ in range(min(most, len(work))):
            work.pop(0)()

    counts = {(1, 0): (1, 0), (1, 1): (1, 2), (2, 0): (1, 1), (2, 1): (1, 2)}
    for step in range(1, half + 1):
        slots = (2 * step - 1, 2 * step) if step < half else (2 * step - 1,)
        for piece in range(2):
            ring.take(3, step, piece)
            before, after = counts.get((step, piece), (1, 1))
            do_work(before)
            for slot in slots:
                send_piece(slot, piece)
            if piece == 1:
                work += [functools.partial(keep_part, slot) for slot in slots]
            do_work(after)
    do_work(len(work))
    with jax.named_scope("wait_part"):
        remote(far_in, far_in, part_pair, {"tp": outer}).wait_recv()
    with jax.named_scope("wait_sends"):
        for copy in sent:
            copy.wait_send()
        for copy in ring.copies.values():
            copy.wait_send()


def recv_count(sp):
    return 9 * 2 * (sp // 2) + 2 * sp + 9 + 2 + 2 + 1 + 1 + 2 + 2


def fits(sp, tp, tokens, query_weight, key_weight, conv_weight, attn_proj, taps, head):
    return (
        tp == 4
        and sp % 2 == 0
        and sp >= 6
        and tokens.shape[0] % (4 * 2 * WINDOW) == 0
        and tokens.shape[1] % LANES == 0
        and WINDOW == LANES
        and 2 * head == LANES
        and key_weight.shape[1] == head
        and query_weight.shape[1] == 4 * head
        and conv_weight.shape[1] == 4 * head
        and query_weight.shape[0] % LANES == 0
        and attn_proj.shape[1] % (2 * LANES) == 0
        and taps.shape[0] <= 31
    )


def fused(
    tokens,
    mix_gain,
    query_weight,
    key_weight,
    value_weight,
    conv_value_weight,
    conv_gate_weight,
    query_gain,
    key_gain,
    sink_logit,
    conv_taps,
    conv_gain,
    attn_proj,
    conv_proj,
):
    sp = lax.axis_size("sp")
    count, features = tokens.shape
    model = features * 4
    depth, width = query_weight.shape
    head = query_gain.shape[0]
    channels = conv_taps.shape[1]
    columns = attn_proj.shape[1]
    block = count // 4
    bf16, f32 = jnp.bfloat16, jnp.float32
    half_pad = 16
    stat = 2 * count // LANES
    padded_rows = count + 2 * WINDOW
    vmem, dma = pltpu.VMEM, pltpu.SemaphoreType.DMA
    inputs = dict(
        tokens=tokens,
        query_w=query_weight,
        key_w=key_weight.T,
        value_w=value_weight.T,
        conv_value_w=conv_value_weight,
        conv_gate_w=conv_gate_weight,
        attn_p=attn_proj,
        conv_p=conv_proj,
        mix_gain=mix_gain.reshape(-1, LANES),
        conv_gain=conv_gain.reshape(-1, LANES),
        query_gain=query_gain.reshape(1, -1),
        key_gain=key_gain.reshape(1, -1),
        sink_logit=sink_logit,
        conv_taps=conv_taps,
    )
    outputs = dict(
        near_out=vmem((block, model), f32),
        far_in=vmem((block, model), bf16),
    )
    scratch = dict(
        whole=vmem((4, count, features), bf16),
        normed=vmem((count, model), bf16),
        query_all=vmem((model, width), bf16),
        kv_own=vmem((2 * head, depth), bf16),
        kv_all=vmem((model, 2 * head), bf16),
        value_all=vmem((model, channels), bf16),
        gate_all=vmem((model, channels), bf16),
        proj_all=vmem((sp, 2, width + channels, columns // 2), bf16),
        proj_other=vmem((sp, 2, width + channels, columns // 2), bf16),
        taps=vmem(conv_taps.shape, f32),
        sinks=pltpu.SMEM(sink_logit.shape, f32),
        mix_rows=vmem((model // LANES, LANES), f32),
        conv_gains=vmem((channels // LANES, LANES), f32),
        query_gains=vmem((1, head), f32),
        key_gains=vmem((1, head), f32),
        head_gains=vmem((2, width), f32),
        spread_heads=vmem((width, width), bf16),
        band=vmem((2, LANES, LANES), f32),
        eye=vmem((LANES, LANES), f32),
        gated=vmem((channels // LANES, count + 2 * half_pad, LANES), f32),
        edge_out=vmem((2, half_pad, channels), bf16),
        edge_in=vmem((2, half_pad, channels), bf16),
        convolved=vmem((count, channels), f32),
        stat_out=vmem((stat, LANES), f32),
        stat_in=vmem((3, stat, LANES), f32),
        stat_rows=vmem((stat, LANES), f32),
        queries=vmem((count, width), bf16),
        query_part=vmem((2 * block, width), f32),
        key_low=vmem((padded_rows, LANES), bf16),
        key_high=vmem((padded_rows, LANES), bf16),
        value_low=vmem((padded_rows, 2 * LANES), bf16),
        value_high=vmem((padded_rows, 2 * LANES), bf16),
        halo_out=vmem((2, block, LANES), bf16),
        halo_in=vmem((2, WINDOW, LANES), bf16),
        mixers=vmem((count, width + channels), bf16),
        mixers_other=vmem((2, block, width + channels), bf16),
        far_out=vmem((sp, 2, block, columns // 2), bf16),
        local_sem=dma,
        ahead_sem=dma,
        send_sem=dma,
        recv_sem=dma((recv_count(sp),)),
    )
    near, far = pl.pallas_call(
        functools.partial(fused_kernel, sp, (*inputs, *outputs, *scratch)),
        out_shape=tuple(outputs.values()),
        in_specs=[pl.BlockSpec(memory_space=pltpu.HBM)] * len(inputs),
        out_specs=[pl.BlockSpec(memory_space=pltpu.VMEM)] * 2,
        scratch_shapes=list(scratch.values()),
        compiler_params=pltpu.CompilerParams(
            collective_id=1, has_side_effects=True, vmem_limit_bytes=60 * 2**20 + 2**19
        ),
    )(*inputs.values())
    return (near + far.astype(f32)).astype(bf16)


def on_device(
    tokens,
    mix_gain,
    query_weight,
    key_weight,
    value_weight,
    conv_value_weight,
    conv_gate_weight,
    query_gain,
    key_gain,
    sink_logit,
    conv_taps,
    conv_gain,
    attn_proj,
    conv_proj,
):
    if fits(
        lax.axis_size("sp"),
        lax.axis_size("tp"),
        tokens,
        query_weight,
        key_weight,
        conv_value_weight,
        attn_proj,
        conv_taps,
        query_gain.shape[0],
    ):
        return fused(
            tokens,
            mix_gain,
            query_weight,
            key_weight,
            value_weight,
            conv_value_weight,
            conv_gate_weight,
            query_gain,
            key_gain,
            sink_logit,
            conv_taps,
            conv_gain,
            attn_proj,
            conv_proj,
        )
    count = tokens.shape[0]
    shards = (query_weight, conv_value_weight, conv_gate_weight, key_weight, value_weight)
    whole, joined = gather_both(tokens, jnp.concatenate(shards, axis=1))
    normed = unit_rows(whole.astype(jnp.float32), mix_gain).astype(jnp.bfloat16)
    product = jnp.dot(normed, joined, preferred_element_type=jnp.float32)
    cuts = []
    for shard in shards[:-1]:
        cuts.append((cuts[-1] if cuts else 0) + shard.shape[1])
    query, conv_value, conv_gate, key_part, value_part = jnp.split(product, cuts, axis=1)
    head_size = query_gain.shape[0]
    local_kv = key_part.shape[1] // head_size
    group = query.shape[1] // head_size // local_kv
    queries = unit_rows(query.reshape(count, local_kv, group, head_size), query_gain).astype(
        jnp.bfloat16
    )
    keys_normed = (
        unit_rows(key_part.reshape(count, local_kv, head_size), key_gain)
        .astype(jnp.bfloat16)
        .reshape(count, -1)
    )
    values_cast = value_part.astype(jnp.bfloat16)
    gated = (conv_value * jax.nn.sigmoid(conv_gate)).astype(jnp.bfloat16)
    reach = (conv_taps.shape[0] - 1) // 2
    kv_width = keys_normed.shape[1]
    paired = jnp.concatenate([keys_normed, values_cast], axis=1)
    extended = padded(paired, (("sp", 0),), WINDOW)
    key_rows = extended[:, :kv_width]
    value_rows = extended[:, kv_width:]
    conv_rows = padded(gated, (("sp", 0),), reach)
    offset = lax.axis_index("sp") * count
    total = count * lax.axis_size("sp")
    span_rows = key_rows.shape[0]
    attended = attend(
        queries,
        key_rows.reshape(span_rows, local_kv, head_size),
        value_rows.reshape(span_rows, local_kv, head_size),
        sink_logit,
        offset,
        total,
    )
    convolved = depthwise(conv_rows, conv_taps, count)
    channels, tp = conv_taps.shape[1], lax.axis_size("tp")
    local_mean = jnp.mean(convolved, axis=1)
    local_square = jnp.sum(jnp.square(convolved - local_mean[:, None]), axis=1)
    slot = (jnp.arange(tp) == lax.axis_index("tp")).astype(jnp.float32)[:, None, None]
    every = lax.psum(slot * jnp.stack([local_mean, local_square])[None], "tp")
    center = jnp.mean(every[:, 0], axis=0)
    spread = jnp.sum(every[:, 1] + channels * jnp.square(every[:, 0] - center), axis=0)
    spread = spread / (channels * tp)
    centered = convolved - center[:, None]
    featured = jax.nn.silu(centered * lax.rsqrt(spread[:, None] + EPSILON) * conv_gain).astype(
        jnp.bfloat16
    )
    stacked, _ = lax.optimization_barrier((jnp.concatenate([attn_proj, conv_proj], axis=0), joined))
    proj_full = lax.all_gather(stacked, "sp", axis=1, tiled=True)
    mixers = jnp.concatenate([attended, featured], axis=1)
    partial = jnp.dot(mixers, proj_full, preferred_element_type=jnp.float32).astype(jnp.bfloat16)
    return lax.psum_scatter(partial, "tp", scatter_dimension=0, tiled=True)


def solution(mesh):
    placed = (
        P("sp", "tp"),
        P(),
        P("sp", "tp"),
        P("sp", "tp"),
        P("sp", "tp"),
        P("sp", "tp"),
        P("sp", "tp"),
        P(),
        P(),
        P("tp"),
        P(None, "tp"),
        P("tp"),
        P("tp", "sp"),
        P("tp", "sp"),
    )
    return jax.shard_map(
        on_device, mesh=mesh, in_specs=placed, out_specs=P(("sp", "tp"), None), check_vma=False
    )
```

```python
import functools
import types

import jax
import jax.numpy as jnp
from jax import lax
from jax.experimental import pallas as pl
from jax.experimental.pallas import tpu as pltpu
from jax.sharding import PartitionSpec as P

WINDOW = 128


EPSILON = 0.1


def padded(value, sides, width):
    for axis, dim in sides:
        size, length = (lax.axis_size(axis), value.shape[dim])
        up = [(i, (i + 1) % size) for i in range(size - 1)]
        down = [(j, i) for i, j in up]
        last = lax.slice_in_dim(value, length - width, length, axis=dim)
        leading = lax.slice_in_dim(value, 0, width, axis=dim)
        before = lax.ppermute(last, axis, up)
        after = lax.ppermute(leading, axis, down)
        value = jnp.concatenate([before, value, after], axis=dim)
    return value


def unit_rows(values, gain):
    return values * lax.rsqrt(jnp.mean(values * values, axis=-1, keepdims=True) + EPSILON) * gain


def attend(queries, keys, values, sinks, offset, total):
    count, local_kv, group, size = queries.shape
    scale = size ** (-0.5)
    blocks = count // WINDOW
    span = 3 * WINDOW

    def windows(rows):
        cut = rows.reshape(blocks + 2, WINDOW, local_kv, size)
        return jnp.concatenate([cut[:blocks], cut[1 : blocks + 1], cut[2:]], axis=1)

    cut_queries = queries.reshape(blocks, WINDOW, local_kv, group, size)
    scores = jnp.einsum(
        "bqkgd,bskd->bkgqs", cut_queries, windows(keys), preferred_element_type=jnp.float32
    )
    query_row = jnp.arange(WINDOW, dtype=jnp.int32)[None, :, None]
    key_row = jnp.arange(span, dtype=jnp.int32)[None, None, :] - WINDOW
    key_pos = offset + WINDOW * jnp.arange(blocks, dtype=jnp.int32)[:, None, None] + key_row
    allowed = (jnp.abs(key_row - query_row) <= WINDOW) & (key_pos >= 0) & (key_pos < total)
    weights = jnp.where(allowed[:, None, None], jnp.exp(scores * scale), 0.0)
    denominator = jnp.sum(weights, axis=-1) + jnp.exp(sinks).reshape(local_kv, group, 1)
    shares = (weights / denominator[..., None]).astype(jnp.bfloat16)
    result = jnp.einsum(
        "bkgqs,bskd->bqkgd", shares, windows(values), preferred_element_type=jnp.float32
    )
    return result.reshape(count, -1).astype(jnp.bfloat16)


def depthwise(extended, kernel_taps, count):
    result = jnp.zeros((count, kernel_taps.shape[1]), jnp.float32)
    for offset in range(kernel_taps.shape[0]):
        result = result + kernel_taps[offset] * extended[offset : offset + count]
    return result


def snake(size):
    if size % 2:
        return (lambda index: index), (lambda place: place)
    half = size // 2

    def place_of(index):
        odd = index % 2
        return (index // 2) * (1 - odd) + (size - 1 - index // 2) * odd

    def index_of(place):
        back = place // half
        return 2 * place * (1 - back) + (2 * (size - 1 - place) + 1) * back

    return place_of, index_of


def plain(size):
    return (lambda index: index), (lambda place: place)


def gather_kernel(rings, *refs):
    count = len(rings)
    shards, outs = refs[:count], refs[count : 2 * count]
    local_sem = refs[2 * count]
    sems = refs[2 * count + 1 :]
    barrier = pltpu.get_barrier_semaphore()
    plans = []
    for number, (axis, size, dim, order) in enumerate(rings):
        place_of, index_of = order(size)
        place = place_of(lax.axis_index(axis))
        at = lambda shift, p=place, f=index_of, n=size: f((p + shift + n) % n)
        plans.append((axis, size, dim, at, shards[number], outs[number], sems[2 * number : 2 * number + 2]))
        for shift in (1, -1):
            pl.semaphore_signal(
                barrier, inc=1, device_id={axis: at(shift)}, device_id_type=pl.DeviceIdType.MESH
            )

    def window(out, dim, shard, index, low, high):
        rows, columns = shard.shape
        if dim == 0:
            begin = pl.multiple_of(index * rows + low, 16)
            return out.at[pl.ds(begin, high - low), :]
        return out.at[pl.ds(low, high - low), pl.ds(pl.multiple_of(index * columns, 128), columns)]

    local = []
    for number, (axis, size, dim, at, shard, out, _) in enumerate(plans):
        copy = pltpu.make_async_copy(
            shard, window(out, dim, shard, at(0), 0, shard.shape[0]), local_sem.at[number]
        )
        copy.start()
        local.append(copy)
    pl.semaphore_wait(barrier, 2 * count)

    def hop(plan, step, way):
        axis, size, dim, at, shard, out, (send, recv) = plan
        rows = shard.shape[0]
        low, high = 0, rows
        if 2 * step == size:
            low, high = (0, rows // 2) if way == 1 else (rows // 2, rows)
        owner = at(-way * (step - 1))
        target = window(out, dim, shard, owner, low, high)
        source = shard.at[pl.ds(low, high - low), :] if step == 1 else target
        slot = 2 * (step - 1) + (way + 1) // 2
        return pltpu.make_async_remote_copy(
            src_ref=source,
            dst_ref=target,
            send_sem=send.at[slot],
            recv_sem=recv.at[slot],
            device_id={axis: at(way)},
            device_id_type=pl.DeviceIdType.MESH,
        )

    pending = {}
    steps = [(n, s) for n, plan in enumerate(plans) for s in range(1, plan[1] // 2 + 1)]
    steps.sort(key=lambda item: ((item[1] - 1) / (plans[item[0]][1] // 2), -plans[item[0]][1]))
    for number, step in steps:
        for way in (1, -1):
            if step > 1:
                pending[number, step - 1, way].wait_recv()
            copy = hop(plans[number], step, way)
            copy.start()
            pending[number, step, way] = copy
    for number, plan in enumerate(plans):
        for way in (1, -1):
            pending[number, plan[1] // 2, way].wait_recv()
    for copy in pending.values():
        copy.wait_send()
    for copy in local:
        copy.wait()


def gather_both(tokens, joined):
    tp, sp = lax.axis_size("tp"), lax.axis_size("sp")
    rings = (("tp", tp, 1, plain), ("sp", sp, 0, snake))
    sems = []
    for _, size, _, _ in rings:
        sems += [pltpu.SemaphoreType.DMA((2 * (size // 2),))] * 2
    return pl.pallas_call(
        functools.partial(gather_kernel, rings),
        out_shape=(
            jax.ShapeDtypeStruct((tokens.shape[0], tokens.shape[1] * tp), tokens.dtype),
            jax.ShapeDtypeStruct((joined.shape[0] * sp, joined.shape[1]), joined.dtype),
        ),
        in_specs=[pl.BlockSpec(memory_space=pltpu.VMEM)] * 2,
        out_specs=[pl.BlockSpec(memory_space=pl.ANY)] * 2,
        scratch_shapes=[pltpu.SemaphoreType.DMA((2,))] + sems,
        compiler_params=pltpu.CompilerParams(collective_id=0, has_side_effects=True),
    )(tokens, joined)


LANES = 128
MESH = pl.DeviceIdType.MESH


def remote(source, target, sems, where):
    return pltpu.make_async_remote_copy(
        src_ref=source,
        dst_ref=target,
        send_sem=sems[0],
        recv_sem=sems[1],
        device_id=where,
        device_id_type=MESH,
    )


def contract_last(left, right):
    return lax.dot_general(
        left, right, (((1,), (1,)), ((), ())), preferred_element_type=jnp.float32
    )


def matmul(left, right):
    return jnp.dot(left, right, preferred_element_type=jnp.float32)


def lane_index(shape):
    return lax.broadcasted_iota(jnp.int32, shape, len(shape) - 1)


def row_index(shape):
    return lax.broadcasted_iota(jnp.int32, shape, len(shape) - 2)


def aligned(value, multiple):
    return value if isinstance(value, int) else pl.multiple_of(value, multiple)


class Ring:
    def __init__(self, size, groups, sems, reuse):
        place_of, index_of = snake(size)
        place = place_of(lax.axis_index("sp"))
        self.at = lambda shift: index_of((place + shift + size) % size)
        self.half = size // 2
        self.groups = groups
        self.sems = sems
        self.reuse = reuse
        self.pairs = {}
        self.copies = {}
        self.arrived = None

    def part(self, group, step, piece, way):
        whole, up, down = self.groups[group][piece]
        if step < self.half:
            return whole
        return None if step > self.half else up if way == 1 else down

    def send(self, group, step, piece, way, source=None, hold=False):
        ref = self.part(group, step, piece, way)(self.at(-way * (step - 1)))
        key = self.reuse.get((group, piece), (group, piece)) + (step, way)
        if key not in self.pairs:
            self.pairs[key] = next(self.sems)
        copy = remote(ref if source is None else source, ref, self.pairs[key], {"sp": self.at(way)})
        self.copies[group, step, piece, way] = copy
        if not hold:
            copy.start()

    def first(self, group, sources=None, hold=False):
        for piece in range(len(self.groups[group])):
            for way in (1, -1):
                source = None if sources is None else sources[piece]
                self.send(group, 1, piece, way, source, hold)

    def start_first(self, group):
        for piece in range(len(self.groups[group])):
            for way in (1, -1):
                self.copies[group, 1, piece, way].start()

    def take(self, group, step, piece=None):
        for number in range(len(self.groups[group])):
            for way in (1, -1):
                if piece not in (None, number * 2 // len(self.groups[group])) or self.part(group, step, number, way) is None:
                    continue
                with jax.named_scope(f"ring{group}_{step}_{number}"):
                    self.copies[group, step, number, way].wait_recv()
                if self.part(group, step + 1, number, way) is not None:
                    self.send(group, step + 1, number, way)
                if self.arrived is not None:
                    self.arrived(group, step, number, way)

    def slot(self, step, way):
        return 2 * self.half - 1 if step == self.half else 2 * step - (1 if way == 1 else 0)

    def owner(self, slot):
        step = (slot + 1) // 2
        return self.at(-step if slot % 2 else step)


def scoped(name):
    def wrap(call):
        def inner(*args):
            with jax.named_scope(name):
                return call(*args)

        return inner

    return wrap


def fused_kernel(sp, names, *all_refs):
    ref = types.SimpleNamespace(**dict(zip(names, all_refs)))
    tokens, query_w, taps_w = ref.tokens, ref.query_w, ref.conv_taps
    whole, normed, gated, convolved = ref.whole, ref.normed, ref.gated, ref.convolved
    query_all, kv_all = ref.query_all, ref.kv_all
    value_all, gate_all = ref.value_all, ref.gate_all
    proj_all, proj_other = ref.proj_all, ref.proj_other
    taps, sinks, mix_rows, conv_gains = ref.taps, ref.sinks, ref.mix_rows, ref.conv_gains
    spread_heads, head_gains = ref.spread_heads, ref.head_gains
    band, eye = ref.band, ref.eye
    stat_out, stat_in, stat_rows = ref.stat_out, ref.stat_in, ref.stat_rows
    queries, query_part = ref.queries, ref.query_part
    key_low, key_high = ref.key_low, ref.key_high
    value_low, value_high = ref.value_low, ref.value_high
    mixers, mixers_other = ref.mixers, ref.mixers_other
    near_out, far_in, far_out = ref.near_out, ref.far_in, ref.far_out

    count, features = tokens.shape
    depth, width = query_w.shape
    model = features * 4
    columns = ref.attn_p.shape[1]
    thin = columns // 2
    block = count // 4
    half_pad = (gated.shape[1] - count) // 2
    reach = (taps.shape[0] - 1) // 2
    head = LANES // 2
    channels = taps.shape[1]
    blocks = count // LANES
    s, t = lax.axis_index("sp"), lax.axis_index("tp")
    a, c = t // 2, t % 2
    inner, outer = t + 1 - 2 * c, (t + 2) % 4
    cross = outer + 1 - 2 * c
    send_sem, recv_sem = ref.send_sem, ref.recv_sem
    local_sem, ahead_sem = ref.local_sem, ref.ahead_sem

    def sem_pairs():
        for i in range(recv_sem.shape[0]):
            yield send_sem, recv_sem.at[i]

    sems = sem_pairs()
    sent = []

    def push(source, target, where, pair=None):
        copy = remote(source, target, pair or next(sems), where)
        copy.start()
        sent.append(copy)
        return copy

    def rows_of(owner, low, high):
        return pl.ds(pl.multiple_of(owner * depth + low, 16), high - low)

    def kv_columns(owner):
        return pl.ds(pl.multiple_of(owner * depth, LANES), depth)

    def out_columns(owner):
        return pl.ds(pl.multiple_of(owner * columns, LANES), columns)

    cut = depth // 4

    def piece_of(target, low, high):
        return lambda o: target.at[rows_of(o, low, high), :]

    def split_piece(target, low, high):
        middle = (low + high) // 2
        return tuple(
            piece_of(target, *span) for span in ((low, high), (low, middle), (middle, high))
        )

    def proj_piece(piece):
        spans = ((0, width + channels), (0, width), (width, width + channels))
        return tuple(
            (lambda o, low=low, high=high: proj_all.at[o, piece, pl.ds(low, high - low), :])
            for low, high in spans
        )

    ring = Ring(
        sp,
        (
            (split_piece(value_all, 0, depth), split_piece(gate_all, 0, depth)),
            (split_piece(kv_all, 0, depth),),
            tuple(split_piece(query_all, i * cut, (i + 1) * cut) for i in range(4)),
            (proj_piece(0), proj_piece(1)),
        ),
        sems,
        {(2, 0): (0, 0), (2, 1): (0, 1), (3, 0): (2, 2), (3, 1): (2, 3)},
    )
    half = ring.half

    barrier = pltpu.get_barrier_semaphore()
    following, preceding = (s + 1) % sp, (s + sp - 1) % sp
    near_devices = [{"sp": ring.at(1)}, {"sp": ring.at(-1)}, {"sp": following}, {"sp": preceding}]
    near_devices += [{"tp": inner}, {"tp": outer}, {"tp": cross}]
    for where in near_devices:
        pl.semaphore_signal(barrier, inc=1, device_id=where, device_id_type=MESH)
    ahead = []
    for source, target in (
        (ref.conv_value_w, value_all.at[rows_of(s, 0, depth), :]),
        (ref.conv_gate_w, gate_all.at[rows_of(s, 0, depth), :]),
    ):
        copy = pltpu.make_async_copy(source, target, ahead_sem)
        copy.start()
        ahead.append(copy)
    local = []
    for source, target in (
            (tokens, whole.at[t]),
            (ref.key_w, ref.kv_own.at[pl.ds(0, head), :]),
            (ref.value_w, ref.kv_own.at[pl.ds(head, head), :]),
            (ref.mix_gain, mix_rows),
            (query_w, query_all.at[rows_of(s, 0, depth), :]),
            (ref.attn_p.at[:, :thin], proj_all.at[s, 0, pl.ds(0, width), :]),
            (ref.attn_p.at[:, thin:], proj_all.at[s, 1, pl.ds(0, width), :]),
            (ref.conv_p.at[:, :thin], proj_all.at[s, 0, pl.ds(width, channels), :]),
            (ref.conv_p.at[:, thin:], proj_all.at[s, 1, pl.ds(width, channels), :]),
            (taps_w, taps),
            (ref.sink_logit, sinks),
            (ref.conv_gain, conv_gains),
            (ref.query_gain, ref.query_gains),
            (ref.key_gain, ref.key_gains),
    ):
        copy = pltpu.make_async_copy(source, target, local_sem)
        copy.start()
        local.append(copy)
    with jax.named_scope("wait_barrier"):
        pl.semaphore_wait(barrier, len(near_devices))

    with jax.named_scope("wait_ahead"):
        for copy in ahead:
            copy.wait()
    ring.first(0)
    over = []
    row_order = (0, 3, 1, 2)
    for i in row_order:
        rows = pl.ds(i * block, block)
        over.append(push(tokens.at[rows, :], whole.at[t, rows, :], {"tp": outer}))
    beside = push(tokens, whole.at[t], {"tp": inner})
    with jax.named_scope("wait_local"):
        for copy in local:
            copy.wait()

    turned = jnp.transpose(ref.kv_own[...].astype(jnp.float32))
    kv_all[rows_of(s, 0, depth), :] = turned.astype(jnp.bfloat16)
    square = (width, width)
    spread_heads[...] = jnp.where(
        row_index(square) // head == lane_index(square) // head, 1.0 / head, 0.0
    ).astype(jnp.bfloat16)
    tile = (LANES, LANES)
    row, lane = row_index(tile), lane_index(tile)
    band[0] = (lane >= row).astype(jnp.float32)
    band[1] = (lane <= row).astype(jnp.float32)
    eye[...] = (lane == row).astype(jnp.float32)
    exponent = head ** (-0.5) * 1.4426950408889634
    query_gain, key_gain = ref.query_gains[...], ref.key_gains[...]
    plain_lanes = jnp.ones_like(key_gain)
    head_gains[0:1, :] = jnp.concatenate([query_gain * exponent] * 4, axis=1)
    head_gains[1:2, :LANES] = jnp.concatenate([key_gain, plain_lanes], axis=1)
    ones_low = jnp.where(lane < head, 1.0, 0.0)
    for i in range(value_low.shape[0] // LANES):
        rows = pl.ds(i * LANES, LANES)
        low, high = ones_low, 1.0 - ones_low
        if i == 0:
            low, high = (jnp.where(s > 0, v, 0.0) for v in (low, high))
        if i == value_low.shape[0] // LANES - 1:
            low, high = (jnp.where(s < sp - 1, v, 0.0) for v in (low, high))
        value_low[rows, LANES:] = low.astype(jnp.bfloat16)
        value_high[rows, LANES:] = high.astype(jnp.bfloat16)

    step_rows = 64

    def norm_rows(i, carry):
        rows = pl.ds(pl.multiple_of(i * step_rows, step_rows), step_rows)
        total = jnp.zeros((step_rows, LANES), jnp.float32)
        for j in range(4):
            for k in range(features // LANES):
                x = whole[j, rows, k * LANES : (k + 1) * LANES].astype(jnp.float32)
                total = total + x * x
        mean = jnp.sum(total, axis=1, keepdims=True) * (1.0 / model)
        scale = jnp.broadcast_to(lax.rsqrt(mean + EPSILON), (step_rows, LANES))
        for j in range(4):
            for k in range(features // LANES):
                x = whole[j, rows, k * LANES : (k + 1) * LANES].astype(jnp.float32)
                place = j * (features // LANES) + k
                gain = mix_rows[place : place + 1, :]
                normed[rows, place * LANES : (place + 1) * LANES] = (x * scale * gain).astype(
                    jnp.bfloat16
                )
        return carry

    forwards = []

    def forward_tokens(i):
        with jax.named_scope("wait_over"):
            over[i].wait_recv()
        source = whole.at[outer, pl.ds(row_order[i] * block, block), :]
        forwards.append(push(source, source, {"tp": inner}))

    def norm_block(i):
        with jax.named_scope("wait_forward"):
            if i == 0:
                beside.wait_recv()
            forwards[i].wait_recv()
        with jax.named_scope("norm"):
            per = block // step_rows
            begin = row_order[i] * per
            lax.fori_loop(begin, begin + per, norm_rows, 0)

    edge_out, edge_in = ref.edge_out, ref.edge_in

    @scoped("gate")
    def gate_block(i):
        left = normed[i * block : (i + 1) * block, :]
        value = matmul(left, value_all[...])
        gate = matmul(left, gate_all[...])
        result = (value * jax.nn.sigmoid(gate)).astype(jnp.bfloat16)
        wide = result.astype(jnp.float32)
        for j in range(channels // LANES):
            gated[j, i * block + half_pad : (i + 1) * block + half_pad, :] = wide[
                :, j * LANES : (j + 1) * LANES
            ]
        if i == 0:
            edge_out[0] = result[:half_pad, :]
        if i == 3:
            edge_out[1] = result[block - half_pad :, :]

    def conv_rows(i, carry):
        start = i * LANES
        parts = []
        for j in range(channels // LANES):
            lanes = slice(j * LANES, (j + 1) * LANES)
            total = jnp.zeros((LANES, LANES), jnp.float32)
            first = half_pad - reach
            for shift in range(8):
                offsets = [o for o in range(first, first + 2 * reach + 1) if o % 8 == shift]
                high = offsets[-1] - shift
                rows = gated[j, pl.ds(start + shift, LANES + high), :]
                for o in offsets:
                    tap = taps[o - first : o - first + 1, lanes]
                    total = total + tap * rows[o - shift : o - shift + LANES]
            convolved[pl.ds(pl.multiple_of(start, LANES), LANES), lanes] = total
            parts.append(total)
        mean = jnp.sum(sum(parts[1:], parts[0]), axis=1, keepdims=True) * (1.0 / channels)
        squares = [jnp.square(part - mean) for part in parts]
        square_sum = jnp.sum(sum(squares[1:], squares[0]), axis=1, keepdims=True)
        stat_out[pl.ds(i, 1), :] = jnp.sum(mean * eye[...], axis=0, keepdims=True)
        stat_out[pl.ds(i + blocks, 1), :] = jnp.sum(square_sum * eye[...], axis=0, keepdims=True)
        return carry

    @scoped("conv")
    def convolve(low, high):
        lax.fori_loop(low, high, conv_rows, 0)

    quarter = blocks // 4

    def fill_edges():
        for side, edge in enumerate(edges):
            with jax.named_scope("wait_edge"):
                edge.wait_recv()
            inside = s > 0 if side == 0 else s < sp - 1
            values = jnp.where(inside, edge_in[side].astype(jnp.float32), 0.0)
            start = 0 if side == 0 else count + half_pad
            for j in range(channels // LANES):
                gated[j, start : start + half_pad, :] = values[:, j * LANES : (j + 1) * LANES]

    def head_scale(part):
        lanes = part.shape[1]
        mean = matmul((part * part).astype(jnp.bfloat16), spread_heads[:lanes, :lanes])
        return lax.rsqrt(mean + EPSILON)

    halo_out, halo_in = ref.halo_out, ref.halo_in

    def store_key_values(rows, low, inside=None):
        high = pltpu.roll(low, head, 1)
        is_low = lane_index(low.shape) < head
        key_low[rows, :] = jnp.where(is_low, low, 0.0).astype(jnp.bfloat16)
        key_high[rows, :] = jnp.where(is_low, 0.0, high).astype(jnp.bfloat16)
        keep_low = is_low if inside is None else is_low & inside
        keep_high = ~is_low if inside is None else ~is_low & inside
        value_low[rows, :LANES] = jnp.where(keep_low, high, 0.0).astype(jnp.bfloat16)
        value_high[rows, :LANES] = jnp.where(keep_high, low, 0.0).astype(jnp.bfloat16)

    @scoped("keys")
    def key_value_block(i, edge=None):
        begin = aligned(i * block, block)
        part = matmul(normed[pl.ds(begin, block), :], kv_all[...])
        scaled = part * head_scale(part) * head_gains[1:2, :LANES]
        low = jnp.where(lane_index(part.shape) < head, scaled, part)
        store_key_values(pl.ds(aligned(begin + WINDOW, WINDOW), block), low)
        if edge is not None:
            halo_out[edge] = low.astype(jnp.bfloat16)

    def push_halo(edge, last):
        where = {"sp": (s + sp + 2 * last - 1) % sp}
        source = halo_out.at[edge, pl.ds(aligned(last * (block - WINDOW), WINDOW), WINDOW), :]
        return push(source, halo_in.at[1 - last], where)

    def fill_halo(copy, last):
        with jax.named_scope("wait_halo"):
            copy.wait_recv()
        outside = (s == 0) & (last == 1) | (s == sp - 1) & (last == 0)
        start = aligned((1 - last) * (WINDOW + count), WINDOW)
        low = halo_in[1 - last].astype(jnp.float32)
        store_key_values(pl.ds(start, WINDOW), low, ~outside)

    ring.take(0, 1)
    forward_tokens(0)
    norm_block(0)
    ring.take(0, 2)
    ring.first(1)
    forward_tokens(1)
    norm_block(1)
    for step in range(3, half):
        ring.take(0, step)
    ring.take(1, 1)
    ring.first(2)
    forward_tokens(2)
    norm_block(2)
    ring.take(0, half)
    gate_block(0)
    gate_block(3)
    edges = [
        push(edge_out.at[1], edge_in.at[0], {"sp": following}),
        push(edge_out.at[0], edge_in.at[1], {"sp": preceding}),
    ]
    ring.take(1, 2)
    forward_tokens(3)
    gate_block(1)
    ring.take(2, 1, 0)
    norm_block(3)
    ring.take(2, 1, 1)
    gate_block(2)
    convolve(1, 2)
    for step in range(3, half):
        ring.take(1, step)
    convolve(2, quarter + 2)
    ring.take(2, 2, 0)
    convolve(quarter + 2, 2 * quarter + 2)
    ring.take(2, 2, 1)
    convolve(2 * quarter + 2, blocks - 1)
    fill_edges()
    convolve(0, 1)
    ring.take(1, half)
    convolve(blocks - 1, blocks)
    stat_pair, part_pair = next(sems), next(sems)
    for i, peer in enumerate((inner, outer, cross)):
        push(stat_out, stat_in.at[i], {"tp": peer}, stat_pair)
    key_value_block(3 * a, 0)
    far_halo = push_halo(0, a)
    for step in range(3, half - 1):
        ring.take(2, step)
    ring.take(2, half - 1, 0)
    key_value_block(3 * (1 - a), 1)
    ring.take(2, half - 1, 1)
    ring.first(3, hold=True)
    pl.when(c == 0)(lambda: ring.start_first(3))
    near_halo = push_halo(1, 1 - a)
    key_value_block(1)
    key_value_block(2)
    pl.when(c == 1)(lambda: ring.start_first(3))

    def feature_rows(i, carry):
        rows = pl.ds(pl.multiple_of(i * LANES, LANES), LANES)
        middle = jnp.sum(stat_rows[pl.ds(i, 1), :] * eye[...], axis=1, keepdims=True)
        scale = jnp.sum(stat_rows[pl.ds(i + blocks, 1), :] * eye[...], axis=1, keepdims=True)
        for j in range(channels // LANES):
            lanes = slice(j * LANES, (j + 1) * LANES)
            value = (convolved[rows, lanes] - middle) * scale * conv_gains[j : j + 1, :]
            mixers[rows, width + j * LANES : width + (j + 1) * LANES] = (
                value * jax.nn.sigmoid(value)
            ).astype(jnp.bfloat16)
        return carry

    starts = ((1 - a) * 2, a * 2)
    give = [pl.ds(pl.multiple_of((base + 1 - c) * block, block), block) for base in starts]
    keep = [pl.ds(pl.multiple_of((base + c) * block, block), block) for base in starts]

    @scoped("features")
    def features_of(f):
        low = starts[f] * (block // LANES)
        lax.fori_loop(low, low + blocks // 2, feature_rows, 0)
        return push(mixers.at[give[f], width:], mixers_other.at[f, :, width:], {"tp": inner})

    @scoped("partial")
    def partial_block(f, i):
        rows = pl.ds(pl.multiple_of((starts[f] + i) * block, block), block)
        owners = [ring.owner(slot) for slot in range(sp - 1)]
        left = jnp.concatenate([normed[rows, kv_columns(o)] for o in owners], axis=1)
        right = jnp.concatenate([query_all[rows_of(o, 0, depth), :] for o in owners], axis=0)
        query_part[i * block : (i + 1) * block, :] = matmul(left, right)

    both = [pl.ds(pl.multiple_of(base * block, block), 2 * block) for base in starts]

    @scoped("queries")
    def query_rows(f):
        owner = ring.owner(sp - 1)
        last = matmul(normed[both[f], kv_columns(owner)], query_all[rows_of(owner, 0, depth), :])
        part = query_part[...] + last
        queries[both[f], :] = (part * head_scale(part) * head_gains[0:1, :]).astype(jnp.bfloat16)

    for i in range(2):
        partial_block(0, i)
    with jax.named_scope("wait_stat"):
        remote(stat_in, stat_in, stat_pair, {"tp": inner}).wait_recv()
    every = [stat_out[...]] + [stat_in[i] for i in range(3)]
    means = [v[:blocks] for v in every]
    center = (means[0] + means[1] + means[2] + means[3]) * 0.25
    spread = sum(v[blocks:] for v in every) + channels * sum(jnp.square(m - center) for m in means)
    stat_rows[:blocks] = center
    stat_rows[blocks:] = lax.rsqrt(spread * (1.0 / (channels * 4)) + EPSILON)

    given_features = [features_of(0)]
    ring.take(2, half)
    query_rows(0)

    shared = {}

    def share(slot, piece):
        owner = ring.owner(slot)
        source, target = proj_all.at[owner, piece], proj_other.at[owner, piece]
        shared[slot, piece] = push(source, target, {"tp": inner})

    def arrived(group, step, piece, way):
        if step < half or way == -1:
            share(ring.slot(step, way), piece)

    ring.arrived = arrived
    share(0, 0)
    share(0, 1)
    head_lanes = lane_index((1, LANES)) < head
    sink_rows = [
        jnp.exp(jnp.where(head_lanes, sinks[2 * i], sinks[2 * i + 1])) for i in range(2)
    ]

    @scoped("attend")
    def attend_rows(first, windows):
        starts_at = [pl.multiple_of(first + w * WINDOW, WINDOW) for w in range(windows)]
        lefts = [
            jnp.concatenate([queries[pl.ds(b, WINDOW), lanes] for lanes in halves], axis=0)
            for b in starts_at
        ]
        shares, vals = [[] for _ in range(windows)], []
        for j in range(windows + 2):
            span = pl.ds(pl.multiple_of(first + j * WINDOW, WINDOW), WINDOW)
            readers = [w for w in range(windows) if 0 <= j - w <= 2]
            left = jnp.concatenate([lefts[w] for w in readers], axis=0)
            right = jnp.concatenate([key_low[span, :], key_high[span, :]], axis=0)
            weights = jnp.exp2(contract_last(left, right))
            for n, w in enumerate(readers):
                weight = weights[n * 2 * WINDOW : (n + 1) * 2 * WINDOW]
                if j - w != 1:
                    mask = band[(j - w) // 2]
                    mask = jnp.concatenate([mask, mask], axis=0)
                    weight = weight * jnp.concatenate([mask, mask], axis=1)
                shares[w].append(weight.astype(jnp.bfloat16))
            vals.append(jnp.concatenate([value_low[span, :], value_high[span, :]], axis=0))
        for w, b in enumerate(starts_at):
            right = jnp.concatenate(vals[w : w + 3], axis=0)
            total = matmul(jnp.concatenate(shares[w], axis=1), right)
            for j in range(2):
                piece = total[j * WINDOW : (j + 1) * WINDOW]
                mixers[pl.ds(b, WINDOW), halves[j]] = (
                    piece[:, :LANES] / (piece[:, LANES:] + sink_rows[j])
                ).astype(jnp.bfloat16)

    halves = (slice(0, LANES), slice(LANES, 2 * LANES))

    def attend_given(f, low=0, size=block):
        here = pl.multiple_of((starts[f] + 1 - c) * block + low, WINDOW)
        attend_rows(here, size // WINDOW)
        target = mixers_other.at[f, pl.ds(aligned(low, WINDOW), size), :width]
        return push(mixers.at[pl.ds(here, size), :width], target, {"tp": inner})

    def attend_kept(f, low=0, size=block):
        attend_rows((starts[f] + c) * block + low, size // WINDOW)

    @scoped("project")
    def project(f, slot, pieces=(0, 1), low=0, size=block):
        owner = ring.owner(slot)
        here = pl.ds(pl.multiple_of((starts[f] + c) * block + low, WINDOW), size)
        left = jnp.concatenate(
            [mixers[here, :], mixers_other[f, pl.ds(aligned(low, WINDOW), size), :]], axis=1
        )
        right = [
            jnp.concatenate([proj_all[owner, piece], proj_other[owner, piece]], axis=0)
            for piece in pieces
        ]
        return matmul(left, jnp.concatenate(right, axis=1))

    def wait_shared(slot, piece):
        with jax.named_scope("wait_shared"):
            shared[slot, piece].wait_recv()

    def send_piece(slot, piece):
        if slot:
            wait_shared(slot, piece)
        far_out[slot, piece] = project(0, slot, (piece,)).astype(jnp.bfloat16)
        target = far_in.at[:, half_columns(slot, piece)]
        push(far_out.at[slot, piece], target, {"tp": outer}, part_pair)

    def half_columns(slot, piece):
        begin = ring.owner(slot) * columns + piece * thin
        return pl.ds(pl.multiple_of(begin, LANES), thin)

    def keep_part(slot):
        near_out[:, out_columns(ring.owner(slot))] = project(1, slot)

    fill_halo(far_halo, a)
    given_heads = [attend_given(0)]
    attend_kept(0)
    given_features[0].wait_recv()
    for piece in range(2):
        wait_shared(0, piece)
    with jax.named_scope("wait_given"):
        given_heads[0].wait_recv()
    for piece in range(2):
        send_piece(0, piece)

    def near_heads():
        fill_halo(near_halo, 1 - a)
        given_heads.append(attend_given(1))

    def near_kept():
        attend_kept(1)
        with jax.named_scope("wait_given"):
            given_features[1].wait_recv()
            given_heads[1].wait_recv()

    work = [
        lambda: partial_block(1, 0),
        lambda: partial_block(1, 1),
        lambda: query_rows(1),
        lambda: given_features.append(features_of(1)),
        near_heads,
        near_kept,
        lambda: keep_part(0),
    ]

    def do_work(most):
        for _ in range(min(most, len(work))):
            work.pop(0)()

    counts = {(1, 0): (1, 0), (1, 1): (1, 2), (2, 0): (1, 1), (2, 1): (1, 2)}
    for step in range(1, half + 1):
        slots = (2 * step - 1, 2 * step) if step < half else (2 * step - 1,)
        for piece in range(2):
            ring.take(3, step, piece)
            before, after = counts.get((step, piece), (1, 1))
            do_work(before)
            for slot in slots:
                send_piece(slot, piece)
            if piece == 1:
                work += [functools.partial(keep_part, slot) for slot in slots]
            do_work(after)
    do_work(len(work))
    with jax.named_scope("wait_part"):
        remote(far_in, far_in, part_pair, {"tp": outer}).wait_recv()
    with jax.named_scope("wait_sends"):
        for copy in sent:
            copy.wait_send()
        for copy in ring.copies.values():
            copy.wait_send()


def recv_count(sp):
    return 5 * 2 * (sp // 2) + 2 * sp + 9 + 2 + 2 + 1 + 1 + 2 + 2


def fits(sp, tp, tokens, query_weight, key_weight, conv_weight, attn_proj, taps, head):
    return (
        tp == 4
        and sp % 2 == 0
        and sp >= 6
        and tokens.shape[0] % (4 * 2 * WINDOW) == 0
        and tokens.shape[1] % LANES == 0
        and WINDOW == LANES
        and 2 * head == LANES
        and key_weight.shape[1] == head
        and query_weight.shape[1] == 4 * head
        and conv_weight.shape[1] == 4 * head
        and query_weight.shape[0] % LANES == 0
        and attn_proj.shape[1] % (2 * LANES) == 0
        and taps.shape[0] <= 31
    )


def fused(
    tokens,
    mix_gain,
    query_weight,
    key_weight,
    value_weight,
    conv_value_weight,
    conv_gate_weight,
    query_gain,
    key_gain,
    sink_logit,
    conv_taps,
    conv_gain,
    attn_proj,
    conv_proj,
):
    sp = lax.axis_size("sp")
    count, features = tokens.shape
    model = features * 4
    depth, width = query_weight.shape
    head = query_gain.shape[0]
    channels = conv_taps.shape[1]
    columns = attn_proj.shape[1]
    block = count // 4
    bf16, f32 = jnp.bfloat16, jnp.float32
    half_pad = 16
    stat = 2 * count // LANES
    padded_rows = count + 2 * WINDOW
    vmem, dma = pltpu.VMEM, pltpu.SemaphoreType.DMA
    inputs = dict(
        tokens=tokens,
        query_w=query_weight,
        key_w=key_weight.T,
        value_w=value_weight.T,
        conv_value_w=conv_value_weight,
        conv_gate_w=conv_gate_weight,
        attn_p=attn_proj,
        conv_p=conv_proj,
        mix_gain=mix_gain.reshape(-1, LANES),
        conv_gain=conv_gain.reshape(-1, LANES),
        query_gain=query_gain.reshape(1, -1),
        key_gain=key_gain.reshape(1, -1),
        sink_logit=sink_logit,
        conv_taps=conv_taps,
    )
    outputs = dict(
        near_out=vmem((block, model), f32),
        far_in=vmem((block, model), bf16),
    )
    scratch = dict(
        whole=vmem((4, count, features), bf16),
        normed=vmem((count, model), bf16),
        query_all=vmem((model, width), bf16),
        kv_own=vmem((2 * head, depth), bf16),
        kv_all=vmem((model, 2 * head), bf16),
        value_all=vmem((model, channels), bf16),
        gate_all=vmem((model, channels), bf16),
        proj_all=vmem((sp, 2, width + channels, columns // 2), bf16),
        proj_other=vmem((sp, 2, width + channels, columns // 2), bf16),
        taps=vmem(conv_taps.shape, f32),
        sinks=pltpu.SMEM(sink_logit.shape, f32),
        mix_rows=vmem((model // LANES, LANES), f32),
        conv_gains=vmem((channels // LANES, LANES), f32),
        query_gains=vmem((1, head), f32),
        key_gains=vmem((1, head), f32),
        head_gains=vmem((2, width), f32),
        spread_heads=vmem((width, width), bf16),
        band=vmem((2, LANES, LANES), f32),
        eye=vmem((LANES, LANES), f32),
        gated=vmem((channels // LANES, count + 2 * half_pad, LANES), f32),
        edge_out=vmem((2, half_pad, channels), bf16),
        edge_in=vmem((2, half_pad, channels), bf16),
        convolved=vmem((count, channels), f32),
        stat_out=vmem((stat, LANES), f32),
        stat_in=vmem((3, stat, LANES), f32),
        stat_rows=vmem((stat, LANES), f32),
        queries=vmem((count, width), bf16),
        query_part=vmem((2 * block, width), f32),
        key_low=vmem((padded_rows, LANES), bf16),
        key_high=vmem((padded_rows, LANES), bf16),
        value_low=vmem((padded_rows, 2 * LANES), bf16),
        value_high=vmem((padded_rows, 2 * LANES), bf16),
        halo_out=vmem((2, block, LANES), bf16),
        halo_in=vmem((2, WINDOW, LANES), bf16),
        mixers=vmem((count, width + channels), bf16),
        mixers_other=vmem((2, block, width + channels), bf16),
        far_out=vmem((sp, 2, block, columns // 2), bf16),
        local_sem=dma,
        ahead_sem=dma,
        send_sem=dma,
        recv_sem=dma((recv_count(sp),)),
    )
    near, far = pl.pallas_call(
        functools.partial(fused_kernel, sp, (*inputs, *outputs, *scratch)),
        out_shape=tuple(outputs.values()),
        in_specs=[pl.BlockSpec(memory_space=pltpu.HBM)] * len(inputs),
        out_specs=[pl.BlockSpec(memory_space=pltpu.VMEM)] * 2,
        scratch_shapes=list(scratch.values()),
        compiler_params=pltpu.CompilerParams(
            collective_id=1, has_side_effects=True, vmem_limit_bytes=60 * 2**20 + 2**19
        ),
    )(*inputs.values())
    return (near + far.astype(f32)).astype(bf16)


def on_device(
    tokens,
    mix_gain,
    query_weight,
    key_weight,
    value_weight,
    conv_value_weight,
    conv_gate_weight,
    query_gain,
    key_gain,
    sink_logit,
    conv_taps,
    conv_gain,
    attn_proj,
    conv_proj,
):
    if fits(
        lax.axis_size("sp"),
        lax.axis_size("tp"),
        tokens,
        query_weight,
        key_weight,
        conv_value_weight,
        attn_proj,
        conv_taps,
        query_gain.shape[0],
    ):
        return fused(
            tokens,
            mix_gain,
            query_weight,
            key_weight,
            value_weight,
            conv_value_weight,
            conv_gate_weight,
            query_gain,
            key_gain,
            sink_logit,
            conv_taps,
            conv_gain,
            attn_proj,
            conv_proj,
        )
    count = tokens.shape[0]
    shards = (query_weight, conv_value_weight, conv_gate_weight, key_weight, value_weight)
    whole, joined = gather_both(tokens, jnp.concatenate(shards, axis=1))
    normed = unit_rows(whole.astype(jnp.float32), mix_gain).astype(jnp.bfloat16)
    product = jnp.dot(normed, joined, preferred_element_type=jnp.float32)
    cuts = []
    for shard in shards[:-1]:
        cuts.append((cuts[-1] if cuts else 0) + shard.shape[1])
    query, conv_value, conv_gate, key_part, value_part = jnp.split(product, cuts, axis=1)
    head_size = query_gain.shape[0]
    local_kv = key_part.shape[1] // head_size
    group = query.shape[1] // head_size // local_kv
    queries = unit_rows(query.reshape(count, local_kv, group, head_size), query_gain).astype(
        jnp.bfloat16
    )
    keys_normed = (
        unit_rows(key_part.reshape(count, local_kv, head_size), key_gain)
        .astype(jnp.bfloat16)
        .reshape(count, -1)
    )
    values_cast = value_part.astype(jnp.bfloat16)
    gated = (conv_value * jax.nn.sigmoid(conv_gate)).astype(jnp.bfloat16)
    reach = (conv_taps.shape[0] - 1) // 2
    kv_width = keys_normed.shape[1]
    paired = jnp.concatenate([keys_normed, values_cast], axis=1)
    extended = padded(paired, (("sp", 0),), WINDOW)
    key_rows = extended[:, :kv_width]
    value_rows = extended[:, kv_width:]
    conv_rows = padded(gated, (("sp", 0),), reach)
    offset = lax.axis_index("sp") * count
    total = count * lax.axis_size("sp")
    span_rows = key_rows.shape[0]
    attended = attend(
        queries,
        key_rows.reshape(span_rows, local_kv, head_size),
        value_rows.reshape(span_rows, local_kv, head_size),
        sink_logit,
        offset,
        total,
    )
    convolved = depthwise(conv_rows, conv_taps, count)
    channels, tp = conv_taps.shape[1], lax.axis_size("tp")
    local_mean = jnp.mean(convolved, axis=1)
    local_square = jnp.sum(jnp.square(convolved - local_mean[:, None]), axis=1)
    slot = (jnp.arange(tp) == lax.axis_index("tp")).astype(jnp.float32)[:, None, None]
    every = lax.psum(slot * jnp.stack([local_mean, local_square])[None], "tp")
    center = jnp.mean(every[:, 0], axis=0)
    spread = jnp.sum(every[:, 1] + channels * jnp.square(every[:, 0] - center), axis=0)
    spread = spread / (channels * tp)
    centered = convolved - center[:, None]
    featured = jax.nn.silu(centered * lax.rsqrt(spread[:, None] + EPSILON) * conv_gain).astype(
        jnp.bfloat16
    )
    stacked, _ = lax.optimization_barrier((jnp.concatenate([attn_proj, conv_proj], axis=0), joined))
    proj_full = lax.all_gather(stacked, "sp", axis=1, tiled=True)
    mixers = jnp.concatenate([attended, featured], axis=1)
    partial = jnp.dot(mixers, proj_full, preferred_element_type=jnp.float32).astype(jnp.bfloat16)
    return lax.psum_scatter(partial, "tp", scatter_dimension=0, tiled=True)


def solution(mesh):
    placed = (
        P("sp", "tp"),
        P(),
        P("sp", "tp"),
        P("sp", "tp"),
        P("sp", "tp"),
        P("sp", "tp"),
        P("sp", "tp"),
        P(),
        P(),
        P("tp"),
        P(None, "tp"),
        P("tp"),
        P("tp", "sp"),
        P("tp", "sp"),
    )
    return jax.shard_map(
        on_device, mesh=mesh, in_specs=placed, out_specs=P(("sp", "tp"), None), check_vma=False
    )
```

```python
import functools
import types

import jax
import jax.numpy as jnp
from jax import lax
from jax.experimental import pallas as pl
from jax.experimental.pallas import tpu as pltpu
from jax.sharding import PartitionSpec as P

WINDOW = 128


EPSILON = 0.1


def padded(value, sides, width):
    for axis, dim in sides:
        size, length = (lax.axis_size(axis), value.shape[dim])
        up = [(i, (i + 1) % size) for i in range(size - 1)]
        down = [(j, i) for i, j in up]
        last = lax.slice_in_dim(value, length - width, length, axis=dim)
        leading = lax.slice_in_dim(value, 0, width, axis=dim)
        before = lax.ppermute(last, axis, up)
        after = lax.ppermute(leading, axis, down)
        value = jnp.concatenate([before, value, after], axis=dim)
    return value


def unit_rows(values, gain):
    return values * lax.rsqrt(jnp.mean(values * values, axis=-1, keepdims=True) + EPSILON) * gain


def attend(queries, keys, values, sinks, offset, total):
    count, local_kv, group, size = queries.shape
    scale = size ** (-0.5)
    blocks = count // WINDOW
    span = 3 * WINDOW

    def windows(rows):
        cut = rows.reshape(blocks + 2, WINDOW, local_kv, size)
        return jnp.concatenate([cut[:blocks], cut[1 : blocks + 1], cut[2:]], axis=1)

    cut_queries = queries.reshape(blocks, WINDOW, local_kv, group, size)
    scores = jnp.einsum(
        "bqkgd,bskd->bkgqs", cut_queries, windows(keys), preferred_element_type=jnp.float32
    )
    query_row = jnp.arange(WINDOW, dtype=jnp.int32)[None, :, None]
    key_row = jnp.arange(span, dtype=jnp.int32)[None, None, :] - WINDOW
    key_pos = offset + WINDOW * jnp.arange(blocks, dtype=jnp.int32)[:, None, None] + key_row
    allowed = (jnp.abs(key_row - query_row) <= WINDOW) & (key_pos >= 0) & (key_pos < total)
    weights = jnp.where(allowed[:, None, None], jnp.exp(scores * scale), 0.0)
    denominator = jnp.sum(weights, axis=-1) + jnp.exp(sinks).reshape(local_kv, group, 1)
    shares = (weights / denominator[..., None]).astype(jnp.bfloat16)
    result = jnp.einsum(
        "bkgqs,bskd->bqkgd", shares, windows(values), preferred_element_type=jnp.float32
    )
    return result.reshape(count, -1).astype(jnp.bfloat16)


def depthwise(extended, kernel_taps, count):
    result = jnp.zeros((count, kernel_taps.shape[1]), jnp.float32)
    for offset in range(kernel_taps.shape[0]):
        result = result + kernel_taps[offset] * extended[offset : offset + count]
    return result


def snake(size):
    if size % 2:
        return (lambda index: index), (lambda place: place)
    half = size // 2

    def place_of(index):
        odd = index % 2
        return (index // 2) * (1 - odd) + (size - 1 - index // 2) * odd

    def index_of(place):
        back = place // half
        return 2 * place * (1 - back) + (2 * (size - 1 - place) + 1) * back

    return place_of, index_of


def plain(size):
    return (lambda index: index), (lambda place: place)


def gather_kernel(rings, *refs):
    count = len(rings)
    shards, outs = refs[:count], refs[count : 2 * count]
    local_sem = refs[2 * count]
    sems = refs[2 * count + 1 :]
    barrier = pltpu.get_barrier_semaphore()
    plans = []
    for number, (axis, size, dim, order) in enumerate(rings):
        place_of, index_of = order(size)
        place = place_of(lax.axis_index(axis))
        at = lambda shift, p=place, f=index_of, n=size: f((p + shift + n) % n)
        plans.append((axis, size, dim, at, shards[number], outs[number], sems[2 * number : 2 * number + 2]))
        for shift in (1, -1):
            pl.semaphore_signal(
                barrier, inc=1, device_id={axis: at(shift)}, device_id_type=pl.DeviceIdType.MESH
            )

    def window(out, dim, shard, index, low, high):
        rows, columns = shard.shape
        if dim == 0:
            begin = pl.multiple_of(index * rows + low, 16)
            return out.at[pl.ds(begin, high - low), :]
        return out.at[pl.ds(low, high - low), pl.ds(pl.multiple_of(index * columns, 128), columns)]

    local = []
    for number, (axis, size, dim, at, shard, out, _) in enumerate(plans):
        copy = pltpu.make_async_copy(
            shard, window(out, dim, shard, at(0), 0, shard.shape[0]), local_sem.at[number]
        )
        copy.start()
        local.append(copy)
    pl.semaphore_wait(barrier, 2 * count)

    def hop(plan, step, way):
        axis, size, dim, at, shard, out, (send, recv) = plan
        rows = shard.shape[0]
        low, high = 0, rows
        if 2 * step == size:
            low, high = (0, rows // 2) if way == 1 else (rows // 2, rows)
        owner = at(-way * (step - 1))
        target = window(out, dim, shard, owner, low, high)
        source = shard.at[pl.ds(low, high - low), :] if step == 1 else target
        slot = 2 * (step - 1) + (way + 1) // 2
        return pltpu.make_async_remote_copy(
            src_ref=source,
            dst_ref=target,
            send_sem=send.at[slot],
            recv_sem=recv.at[slot],
            device_id={axis: at(way)},
            device_id_type=pl.DeviceIdType.MESH,
        )

    pending = {}
    steps = [(n, s) for n, plan in enumerate(plans) for s in range(1, plan[1] // 2 + 1)]
    steps.sort(key=lambda item: ((item[1] - 1) / (plans[item[0]][1] // 2), -plans[item[0]][1]))
    for number, step in steps:
        for way in (1, -1):
            if step > 1:
                pending[number, step - 1, way].wait_recv()
            copy = hop(plans[number], step, way)
            copy.start()
            pending[number, step, way] = copy
    for number, plan in enumerate(plans):
        for way in (1, -1):
            pending[number, plan[1] // 2, way].wait_recv()
    for copy in pending.values():
        copy.wait_send()
    for copy in local:
        copy.wait()


def gather_both(tokens, joined):
    tp, sp = lax.axis_size("tp"), lax.axis_size("sp")
    rings = (("tp", tp, 1, plain), ("sp", sp, 0, snake))
    sems = []
    for _, size, _, _ in rings:
        sems += [pltpu.SemaphoreType.DMA((2 * (size // 2),))] * 2
    return pl.pallas_call(
        functools.partial(gather_kernel, rings),
        out_shape=(
            jax.ShapeDtypeStruct((tokens.shape[0], tokens.shape[1] * tp), tokens.dtype),
            jax.ShapeDtypeStruct((joined.shape[0] * sp, joined.shape[1]), joined.dtype),
        ),
        in_specs=[pl.BlockSpec(memory_space=pltpu.VMEM)] * 2,
        out_specs=[pl.BlockSpec(memory_space=pl.ANY)] * 2,
        scratch_shapes=[pltpu.SemaphoreType.DMA((2,))] + sems,
        compiler_params=pltpu.CompilerParams(collective_id=0, has_side_effects=True),
    )(tokens, joined)


LANES = 128
MESH = pl.DeviceIdType.MESH


def remote(source, target, sems, where):
    return pltpu.make_async_remote_copy(
        src_ref=source,
        dst_ref=target,
        send_sem=sems[0],
        recv_sem=sems[1],
        device_id=where,
        device_id_type=MESH,
    )


def contract_last(left, right):
    return lax.dot_general(
        left, right, (((1,), (1,)), ((), ())), preferred_element_type=jnp.float32
    )


def matmul(left, right):
    return jnp.dot(left, right, preferred_element_type=jnp.float32)


def lane_index(shape):
    return lax.broadcasted_iota(jnp.int32, shape, len(shape) - 1)


def row_index(shape):
    return lax.broadcasted_iota(jnp.int32, shape, len(shape) - 2)


def aligned(value, multiple):
    return value if isinstance(value, int) else pl.multiple_of(value, multiple)


class Ring:
    def __init__(self, size, groups, sems, reuse):
        place_of, index_of = snake(size)
        place = place_of(lax.axis_index("sp"))
        self.at = lambda shift: index_of((place + shift + size) % size)
        self.half = size // 2
        self.groups = groups
        self.sems = sems
        self.reuse = reuse
        self.pairs = {}
        self.copies = {}
        self.arrived = None

    def part(self, group, step, piece, way):
        whole, up, down = self.groups[group][piece]
        if step < self.half:
            return whole
        return None if step > self.half else up if way == 1 else down

    def send(self, group, step, piece, way, source=None, hold=False):
        ref = self.part(group, step, piece, way)(self.at(-way * (step - 1)))
        key = self.reuse.get((group, piece), (group, piece)) + (step, way)
        if key not in self.pairs:
            self.pairs[key] = next(self.sems)
        copy = remote(ref if source is None else source, ref, self.pairs[key], {"sp": self.at(way)})
        self.copies[group, step, piece, way] = copy
        if not hold:
            copy.start()

    def first(self, group, sources=None, hold=False):
        for piece in range(len(self.groups[group])):
            for way in (1, -1):
                source = None if sources is None else sources[piece]
                self.send(group, 1, piece, way, source, hold)

    def start_first(self, group):
        for piece in range(len(self.groups[group])):
            for way in (1, -1):
                self.copies[group, 1, piece, way].start()

    def take(self, group, step, piece=None):
        for number in range(len(self.groups[group])):
            for way in (1, -1):
                if piece not in (None, number * 2 // len(self.groups[group])) or self.part(group, step, number, way) is None:
                    continue
                with jax.named_scope(f"ring{group}_{step}_{number}"):
                    self.copies[group, step, number, way].wait_recv()
                if self.part(group, step + 1, number, way) is not None:
                    self.send(group, step + 1, number, way)
                if self.arrived is not None:
                    self.arrived(group, step, number, way)

    def slot(self, step, way):
        return 2 * self.half - 1 if step == self.half else 2 * step - (1 if way == 1 else 0)

    def owner(self, slot):
        step = (slot + 1) // 2
        return self.at(-step if slot % 2 else step)


def scoped(name):
    def wrap(call):
        def inner(*args):
            with jax.named_scope(name):
                return call(*args)

        return inner

    return wrap


def fused_kernel(sp, names, *all_refs):
    ref = types.SimpleNamespace(**dict(zip(names, all_refs)))
    tokens, query_w, taps_w = ref.tokens, ref.query_w, ref.conv_taps
    whole, normed, gated, convolved = ref.whole, ref.normed, ref.gated, ref.convolved
    query_all, kv_all = ref.query_all, ref.kv_all
    value_all, gate_all = ref.value_all, ref.gate_all
    proj_all, proj_other = ref.proj_all, ref.proj_other
    taps, sinks, mix_rows, conv_gains = ref.taps, ref.sinks, ref.mix_rows, ref.conv_gains
    spread_heads, head_gains = ref.spread_heads, ref.head_gains
    band, eye = ref.band, ref.eye
    stat_out, stat_in, stat_rows = ref.stat_out, ref.stat_in, ref.stat_rows
    queries, query_part = ref.queries, ref.query_part
    key_low, key_high = ref.key_low, ref.key_high
    value_low, value_high = ref.value_low, ref.value_high
    mixers, mixers_other = ref.mixers, ref.mixers_other
    near_out, far_in, far_out = ref.near_out, ref.far_in, ref.far_out

    count, features = tokens.shape
    depth, width = query_w.shape
    model = features * 4
    columns = ref.attn_p.shape[1]
    thin = columns // 2
    block = count // 4
    half_pad = (gated.shape[1] - count) // 2
    reach = (taps.shape[0] - 1) // 2
    head = LANES // 2
    channels = taps.shape[1]
    blocks = count // LANES
    s, t = lax.axis_index("sp"), lax.axis_index("tp")
    a, c = t // 2, t % 2
    inner, outer = t + 1 - 2 * c, (t + 2) % 4
    cross = outer + 1 - 2 * c
    send_sem, recv_sem = ref.send_sem, ref.recv_sem
    local_sem, ahead_sem = ref.local_sem, ref.ahead_sem

    def sem_pairs():
        for i in range(recv_sem.shape[0]):
            yield send_sem, recv_sem.at[i]

    sems = sem_pairs()
    sent = []

    def push(source, target, where, pair=None):
        copy = remote(source, target, pair or next(sems), where)
        copy.start()
        sent.append(copy)
        return copy

    def rows_of(owner, low, high):
        return pl.ds(pl.multiple_of(owner * depth + low, 16), high - low)

    def kv_columns(owner):
        return pl.ds(pl.multiple_of(owner * depth, LANES), depth)

    def out_columns(owner):
        return pl.ds(pl.multiple_of(owner * columns, LANES), columns)

    cut = depth // 4

    def piece_of(target, low, high):
        return lambda o: target.at[rows_of(o, low, high), :]

    def split_piece(target, low, high):
        middle = (low + high) // 2
        return tuple(
            piece_of(target, *span) for span in ((low, high), (low, middle), (middle, high))
        )

    def proj_piece(piece):
        spans = ((0, width + channels), (0, width), (width, width + channels))
        return tuple(
            (lambda o, low=low, high=high: proj_all.at[o, piece, pl.ds(low, high - low), :])
            for low, high in spans
        )

    ring = Ring(
        sp,
        (
            (split_piece(value_all, 0, depth), split_piece(gate_all, 0, depth)),
            (split_piece(kv_all, 0, depth),),
            tuple(split_piece(query_all, i * cut, (i + 1) * cut) for i in range(4)),
            (proj_piece(0), proj_piece(1)),
        ),
        sems,
        {(2, 0): (0, 0), (2, 1): (0, 1), (3, 0): (2, 2), (3, 1): (2, 3)},
    )
    half = ring.half

    barrier = pltpu.get_barrier_semaphore()
    following, preceding = (s + 1) % sp, (s + sp - 1) % sp
    near_devices = [{"sp": ring.at(1)}, {"sp": ring.at(-1)}, {"sp": following}, {"sp": preceding}]
    near_devices += [{"tp": inner}, {"tp": outer}, {"tp": cross}]
    for where in near_devices:
        pl.semaphore_signal(barrier, inc=1, device_id=where, device_id_type=MESH)
    ahead = []
    for source, target in (
        (ref.conv_value_w, value_all.at[rows_of(s, 0, depth), :]),
        (ref.conv_gate_w, gate_all.at[rows_of(s, 0, depth), :]),
    ):
        copy = pltpu.make_async_copy(source, target, ahead_sem)
        copy.start()
        ahead.append(copy)
    local = []
    for source, target in (
            (tokens, whole.at[t]),
            (ref.key_w, ref.kv_own.at[pl.ds(0, head), :]),
            (ref.value_w, ref.kv_own.at[pl.ds(head, head), :]),
            (ref.mix_gain, mix_rows),
            (query_w, query_all.at[rows_of(s, 0, depth), :]),
            (ref.attn_p.at[:, :thin], proj_all.at[s, 0, pl.ds(0, width), :]),
            (ref.attn_p.at[:, thin:], proj_all.at[s, 1, pl.ds(0, width), :]),
            (ref.conv_p.at[:, :thin], proj_all.at[s, 0, pl.ds(width, channels), :]),
            (ref.conv_p.at[:, thin:], proj_all.at[s, 1, pl.ds(width, channels), :]),
            (taps_w, taps),
            (ref.sink_logit, sinks),
            (ref.conv_gain, conv_gains),
            (ref.query_gain, ref.query_gains),
            (ref.key_gain, ref.key_gains),
    ):
        copy = pltpu.make_async_copy(source, target, local_sem)
        copy.start()
        local.append(copy)
    with jax.named_scope("wait_barrier"):
        pl.semaphore_wait(barrier, len(near_devices))

    with jax.named_scope("wait_ahead"):
        for copy in ahead:
            copy.wait()
    ring.first(0)
    over, token_pairs = [], [next(sems) for _ in range(8)]
    row_order = (0, 3, 1, 2)
    for i in row_order:
        rows = pl.ds(i * block, block)
        over.append(push(tokens.at[rows, :], whole.at[t, rows, :], {"tp": outer}, token_pairs[len(over)]))
    beside = push(tokens, whole.at[t], {"tp": inner})
    with jax.named_scope("wait_local"):
        for copy in local:
            copy.wait()

    turned = jnp.transpose(ref.kv_own[...].astype(jnp.float32))
    kv_all[rows_of(s, 0, depth), :] = turned.astype(jnp.bfloat16)
    square = (width, width)
    spread_heads[...] = jnp.where(
        row_index(square) // head == lane_index(square) // head, 1.0 / head, 0.0
    ).astype(jnp.bfloat16)
    tile = (LANES, LANES)
    row, lane = row_index(tile), lane_index(tile)
    band[0] = (lane >= row).astype(jnp.float32)
    band[1] = (lane <= row).astype(jnp.float32)
    eye[...] = (lane == row).astype(jnp.float32)
    exponent = head ** (-0.5) * 1.4426950408889634
    query_gain, key_gain = ref.query_gains[...], ref.key_gains[...]
    plain_lanes = jnp.ones_like(key_gain)
    head_gains[0:1, :] = jnp.concatenate([query_gain * exponent] * 4, axis=1)
    head_gains[1:2, :LANES] = jnp.concatenate([key_gain, plain_lanes], axis=1)
    ones_low = jnp.where(lane < head, 1.0, 0.0)
    for i in range(value_low.shape[0] // LANES):
        rows = pl.ds(i * LANES, LANES)
        low, high = ones_low, 1.0 - ones_low
        if i == 0:
            low, high = (jnp.where(s > 0, v, 0.0) for v in (low, high))
        if i == value_low.shape[0] // LANES - 1:
            low, high = (jnp.where(s < sp - 1, v, 0.0) for v in (low, high))
        value_low[rows, LANES:] = low.astype(jnp.bfloat16)
        value_high[rows, LANES:] = high.astype(jnp.bfloat16)

    step_rows = 64

    def norm_rows(i, carry):
        rows = pl.ds(pl.multiple_of(i * step_rows, step_rows), step_rows)
        total = jnp.zeros((step_rows, LANES), jnp.float32)
        for j in range(4):
            for k in range(features // LANES):
                x = whole[j, rows, k * LANES : (k + 1) * LANES].astype(jnp.float32)
                total = total + x * x
        mean = jnp.sum(total, axis=1, keepdims=True) * (1.0 / model)
        scale = jnp.broadcast_to(lax.rsqrt(mean + EPSILON), (step_rows, LANES))
        for j in range(4):
            for k in range(features // LANES):
                x = whole[j, rows, k * LANES : (k + 1) * LANES].astype(jnp.float32)
                place = j * (features // LANES) + k
                gain = mix_rows[place : place + 1, :]
                normed[rows, place * LANES : (place + 1) * LANES] = (x * scale * gain).astype(
                    jnp.bfloat16
                )
        return carry

    forwards = []

    def forward_tokens(i):
        with jax.named_scope("wait_over"):
            over[i].wait_recv()
        source = whole.at[outer, pl.ds(row_order[i] * block, block), :]
        forwards.append(push(source, source, {"tp": inner}, token_pairs[4 + i]))

    def norm_block(i):
        with jax.named_scope("wait_forward"):
            if i == 0:
                beside.wait_recv()
            forwards[i].wait_recv()
        with jax.named_scope("norm"):
            per = block // step_rows
            begin = row_order[i] * per
            lax.fori_loop(begin, begin + per, norm_rows, 0)

    edge_out, edge_in = ref.edge_out, ref.edge_in

    @scoped("gate")
    def gate_block(i):
        left = normed[i * block : (i + 1) * block, :]
        value = matmul(left, value_all[...])
        gate = matmul(left, gate_all[...])
        result = (value * jax.nn.sigmoid(gate)).astype(jnp.bfloat16)
        wide = result.astype(jnp.float32)
        for j in range(channels // LANES):
            gated[j, i * block + half_pad : (i + 1) * block + half_pad, :] = wide[
                :, j * LANES : (j + 1) * LANES
            ]
        if i == 0:
            edge_out[0] = result[:half_pad, :]
        if i == 3:
            edge_out[1] = result[block - half_pad :, :]

    def conv_rows(i, carry):
        start = i * LANES
        parts = []
        for j in range(channels // LANES):
            lanes = slice(j * LANES, (j + 1) * LANES)
            total = jnp.zeros((LANES, LANES), jnp.float32)
            first = half_pad - reach
            for shift in range(8):
                offsets = [o for o in range(first, first + 2 * reach + 1) if o % 8 == shift]
                high = offsets[-1] - shift
                rows = gated[j, pl.ds(start + shift, LANES + high), :]
                for o in offsets:
                    tap = taps[o - first : o - first + 1, lanes]
                    total = total + tap * rows[o - shift : o - shift + LANES]
            convolved[pl.ds(pl.multiple_of(start, LANES), LANES), lanes] = total
            parts.append(total)
        mean = jnp.sum(sum(parts[1:], parts[0]), axis=1, keepdims=True) * (1.0 / channels)
        squares = [jnp.square(part - mean) for part in parts]
        square_sum = jnp.sum(sum(squares[1:], squares[0]), axis=1, keepdims=True)
        stat_out[pl.ds(i, 1), :] = jnp.sum(mean * eye[...], axis=0, keepdims=True)
        stat_out[pl.ds(i + blocks, 1), :] = jnp.sum(square_sum * eye[...], axis=0, keepdims=True)
        return carry

    @scoped("conv")
    def convolve(low, high):
        lax.fori_loop(low, high, conv_rows, 0)

    quarter = blocks // 4

    def fill_edges():
        for side, edge in enumerate(edges):
            with jax.named_scope("wait_edge"):
                edge.wait_recv()
            inside = s > 0 if side == 0 else s < sp - 1
            values = jnp.where(inside, edge_in[side].astype(jnp.float32), 0.0)
            start = 0 if side == 0 else count + half_pad
            for j in range(channels // LANES):
                gated[j, start : start + half_pad, :] = values[:, j * LANES : (j + 1) * LANES]

    def head_scale(part):
        lanes = part.shape[1]
        mean = matmul((part * part).astype(jnp.bfloat16), spread_heads[:lanes, :lanes])
        return lax.rsqrt(mean + EPSILON)

    halo_out, halo_in = ref.halo_out, ref.halo_in

    def store_key_values(rows, low, inside=None):
        high = pltpu.roll(low, head, 1)
        is_low = lane_index(low.shape) < head
        key_low[rows, :] = jnp.where(is_low, low, 0.0).astype(jnp.bfloat16)
        key_high[rows, :] = jnp.where(is_low, 0.0, high).astype(jnp.bfloat16)
        keep_low = is_low if inside is None else is_low & inside
        keep_high = ~is_low if inside is None else ~is_low & inside
        value_low[rows, :LANES] = jnp.where(keep_low, high, 0.0).astype(jnp.bfloat16)
        value_high[rows, :LANES] = jnp.where(keep_high, low, 0.0).astype(jnp.bfloat16)

    @scoped("keys")
    def key_value_block(i, edge=None):
        begin = aligned(i * block, block)
        part = matmul(normed[pl.ds(begin, block), :], kv_all[...])
        scaled = part * head_scale(part) * head_gains[1:2, :LANES]
        low = jnp.where(lane_index(part.shape) < head, scaled, part)
        store_key_values(pl.ds(aligned(begin + WINDOW, WINDOW), block), low)
        if edge is not None:
            halo_out[edge] = low.astype(jnp.bfloat16)

    def push_halo(edge, last):
        where = {"sp": (s + sp + 2 * last - 1) % sp}
        source = halo_out.at[edge, pl.ds(aligned(last * (block - WINDOW), WINDOW), WINDOW), :]
        return push(source, halo_in.at[1 - last], where)

    def fill_halo(copy, last):
        with jax.named_scope("wait_halo"):
            copy.wait_recv()
        outside = (s == 0) & (last == 1) | (s == sp - 1) & (last == 0)
        start = aligned((1 - last) * (WINDOW + count), WINDOW)
        low = halo_in[1 - last].astype(jnp.float32)
        store_key_values(pl.ds(start, WINDOW), low, ~outside)

    ring.take(0, 1)
    forward_tokens(0)
    norm_block(0)
    ring.take(0, 2)
    ring.first(1)
    forward_tokens(1)
    norm_block(1)
    for step in range(3, half):
        ring.take(0, step)
    ring.take(1, 1)
    ring.first(2)
    forward_tokens(2)
    norm_block(2)
    ring.take(0, half)
    gate_block(0)
    gate_block(3)
    edges = [
        push(edge_out.at[1], edge_in.at[0], {"sp": following}),
        push(edge_out.at[0], edge_in.at[1], {"sp": preceding}),
    ]
    ring.take(1, 2)
    forward_tokens(3)
    gate_block(1)
    ring.take(2, 1, 0)
    norm_block(3)
    ring.take(2, 1, 1)
    gate_block(2)
    convolve(1, 2)
    for step in range(3, half):
        ring.take(1, step)
    convolve(2, quarter + 2)
    ring.take(2, 2, 0)
    convolve(quarter + 2, 2 * quarter + 2)
    ring.take(2, 2, 1)
    convolve(2 * quarter + 2, blocks - 1)
    fill_edges()
    convolve(0, 1)
    ring.take(1, half)
    convolve(blocks - 1, blocks)
    stat_pair, part_pair = next(sems), next(sems)
    for i, peer in enumerate((inner, outer, cross)):
        push(stat_out, stat_in.at[i], {"tp": peer}, stat_pair)
    key_value_block(3 * a, 0)
    far_halo = push_halo(0, a)
    for step in range(3, half - 1):
        ring.take(2, step)
    ring.take(2, half - 1, 0)
    key_value_block(3 * (1 - a), 1)
    ring.take(2, half - 1, 1)
    ring.first(3, hold=True)
    pl.when(c == 0)(lambda: ring.start_first(3))
    near_halo = push_halo(1, 1 - a)
    key_value_block(1)
    key_value_block(2)
    pl.when(c == 1)(lambda: ring.start_first(3))

    def feature_rows(i, carry):
        rows = pl.ds(pl.multiple_of(i * LANES, LANES), LANES)
        middle = jnp.sum(stat_rows[pl.ds(i, 1), :] * eye[...], axis=1, keepdims=True)
        scale = jnp.sum(stat_rows[pl.ds(i + blocks, 1), :] * eye[...], axis=1, keepdims=True)
        for j in range(channels // LANES):
            lanes = slice(j * LANES, (j + 1) * LANES)
            value = (convolved[rows, lanes] - middle) * scale * conv_gains[j : j + 1, :]
            mixers[rows, width + j * LANES : width + (j + 1) * LANES] = (
                value * jax.nn.sigmoid(value)
            ).astype(jnp.bfloat16)
        return carry

    starts = ((1 - a) * 2, a * 2)
    give = [pl.ds(pl.multiple_of((base + 1 - c) * block, block), block) for base in starts]
    keep = [pl.ds(pl.multiple_of((base + c) * block, block), block) for base in starts]

    @scoped("features")
    def features_of(f):
        low = starts[f] * (block // LANES)
        lax.fori_loop(low, low + blocks // 2, feature_rows, 0)
        return push(mixers.at[give[f], width:], mixers_other.at[f, :, width:], {"tp": inner})

    @scoped("partial")
    def partial_block(f, i):
        rows = pl.ds(pl.multiple_of((starts[f] + i) * block, block), block)
        owners = [ring.owner(slot) for slot in range(sp - 1)]
        left = jnp.concatenate([normed[rows, kv_columns(o)] for o in owners], axis=1)
        right = jnp.concatenate([query_all[rows_of(o, 0, depth), :] for o in owners], axis=0)
        query_part[i * block : (i + 1) * block, :] = matmul(left, right)

    both = [pl.ds(pl.multiple_of(base * block, block), 2 * block) for base in starts]

    @scoped("queries")
    def query_rows(f):
        owner = ring.owner(sp - 1)
        last = matmul(normed[both[f], kv_columns(owner)], query_all[rows_of(owner, 0, depth), :])
        part = query_part[...] + last
        queries[both[f], :] = (part * head_scale(part) * head_gains[0:1, :]).astype(jnp.bfloat16)

    for i in range(2):
        partial_block(0, i)
    with jax.named_scope("wait_stat"):
        remote(stat_in, stat_in, stat_pair, {"tp": inner}).wait_recv()
    every = [stat_out[...]] + [stat_in[i] for i in range(3)]
    means = [v[:blocks] for v in every]
    center = (means[0] + means[1] + means[2] + means[3]) * 0.25
    spread = sum(v[blocks:] for v in every) + channels * sum(jnp.square(m - center) for m in means)
    stat_rows[:blocks] = center
    stat_rows[blocks:] = lax.rsqrt(spread * (1.0 / (channels * 4)) + EPSILON)

    given_features = [features_of(0)]
    ring.take(2, half)
    query_rows(0)

    shared = {}
    spare = iter([pair for key, pair in ring.pairs.items() if key[0] == 1] + token_pairs)

    def share(slot, piece):
        owner = ring.owner(slot)
        source, target = proj_all.at[owner, piece], proj_other.at[owner, piece]
        shared[slot, piece] = push(source, target, {"tp": inner}, next(spare, None))

    def arrived(group, step, piece, way):
        if step < half or way == -1:
            share(ring.slot(step, way), piece)

    ring.arrived = arrived
    share(0, 0)
    share(0, 1)
    head_lanes = lane_index((1, LANES)) < head
    sink_rows = [
        jnp.exp(jnp.where(head_lanes, sinks[2 * i], sinks[2 * i + 1])) for i in range(2)
    ]

    @scoped("attend")
    def attend_rows(first, windows):
        starts_at = [pl.multiple_of(first + w * WINDOW, WINDOW) for w in range(windows)]
        lefts = [
            jnp.concatenate([queries[pl.ds(b, WINDOW), lanes] for lanes in halves], axis=0)
            for b in starts_at
        ]
        shares, vals = [[] for _ in range(windows)], []
        for j in range(windows + 2):
            span = pl.ds(pl.multiple_of(first + j * WINDOW, WINDOW), WINDOW)
            readers = [w for w in range(windows) if 0 <= j - w <= 2]
            left = jnp.concatenate([lefts[w] for w in readers], axis=0)
            right = jnp.concatenate([key_low[span, :], key_high[span, :]], axis=0)
            weights = jnp.exp2(contract_last(left, right))
            for n, w in enumerate(readers):
                weight = weights[n * 2 * WINDOW : (n + 1) * 2 * WINDOW]
                if j - w != 1:
                    mask = band[(j - w) // 2]
                    mask = jnp.concatenate([mask, mask], axis=0)
                    weight = weight * jnp.concatenate([mask, mask], axis=1)
                shares[w].append(weight.astype(jnp.bfloat16))
            vals.append(jnp.concatenate([value_low[span, :], value_high[span, :]], axis=0))
        for w, b in enumerate(starts_at):
            right = jnp.concatenate(vals[w : w + 3], axis=0)
            total = matmul(jnp.concatenate(shares[w], axis=1), right)
            for j in range(2):
                piece = total[j * WINDOW : (j + 1) * WINDOW]
                mixers[pl.ds(b, WINDOW), halves[j]] = (
                    piece[:, :LANES] / (piece[:, LANES:] + sink_rows[j])
                ).astype(jnp.bfloat16)

    halves = (slice(0, LANES), slice(LANES, 2 * LANES))

    def attend_given(f, low=0, size=block):
        here = pl.multiple_of((starts[f] + 1 - c) * block + low, WINDOW)
        attend_rows(here, size // WINDOW)
        target = mixers_other.at[f, pl.ds(aligned(low, WINDOW), size), :width]
        return push(mixers.at[pl.ds(here, size), :width], target, {"tp": inner})

    def attend_kept(f, low=0, size=block):
        attend_rows((starts[f] + c) * block + low, size // WINDOW)

    @scoped("project")
    def project(f, slot, pieces=(0, 1), low=0, size=block):
        owner = ring.owner(slot)
        here = pl.ds(pl.multiple_of((starts[f] + c) * block + low, WINDOW), size)
        left = jnp.concatenate(
            [mixers[here, :], mixers_other[f, pl.ds(aligned(low, WINDOW), size), :]], axis=1
        )
        right = [
            jnp.concatenate([proj_all[owner, piece], proj_other[owner, piece]], axis=0)
            for piece in pieces
        ]
        return matmul(left, jnp.concatenate(right, axis=1))

    def wait_shared(slot, piece):
        with jax.named_scope("wait_shared"):
            shared[slot, piece].wait_recv()

    def send_piece(slot, piece):
        if slot:
            wait_shared(slot, piece)
        far_out[slot, piece] = project(0, slot, (piece,)).astype(jnp.bfloat16)
        target = far_in.at[:, half_columns(slot, piece)]
        push(far_out.at[slot, piece], target, {"tp": outer}, part_pair)

    def half_columns(slot, piece):
        begin = ring.owner(slot) * columns + piece * thin
        return pl.ds(pl.multiple_of(begin, LANES), thin)

    def keep_part(slot):
        near_out[:, out_columns(ring.owner(slot))] = project(1, slot)

    fill_halo(far_halo, a)
    given_heads = [attend_given(0)]
    attend_kept(0)
    given_features[0].wait_recv()
    for piece in range(2):
        wait_shared(0, piece)
    with jax.named_scope("wait_given"):
        given_heads[0].wait_recv()
    for piece in range(2):
        send_piece(0, piece)

    def near_heads():
        fill_halo(near_halo, 1 - a)
        given_heads.append(attend_given(1))

    def near_kept():
        attend_kept(1)
        with jax.named_scope("wait_given"):
            given_features[1].wait_recv()
            given_heads[1].wait_recv()

    work = [
        lambda: partial_block(1, 0),
        lambda: partial_block(1, 1),
        lambda: query_rows(1),
        lambda: given_features.append(features_of(1)),
        near_heads,
        near_kept,
        lambda: keep_part(0),
    ]

    def do_work(most):
        for _ in range(min(most, len(work))):
            work.pop(0)()

    counts = {(1, 0): (1, 0), (1, 1): (1, 2), (2, 0): (1, 1), (2, 1): (1, 2)}
    for step in range(1, half + 1):
        slots = (2 * step - 1, 2 * step) if step < half else (2 * step - 1,)
        for piece in range(2):
            ring.take(3, step, piece)
            before, after = counts.get((step, piece), (1, 1))
            do_work(before)
            for slot in slots:
                send_piece(slot, piece)
            if piece == 1:
                work += [functools.partial(keep_part, slot) for slot in slots]
            do_work(after)
    do_work(len(work))
    with jax.named_scope("wait_part"):
        remote(far_in, far_in, part_pair, {"tp": outer}).wait_recv()
    with jax.named_scope("wait_sends"):
        for copy in sent:
            copy.wait_send()
        for copy in ring.copies.values():
            copy.wait_send()


def recv_count(sp):
    return 5 * 2 * (sp // 2) + max(0, 2 * sp - sp - 8) + 9 + 2 + 2 + 1 + 1 + 2 + 2


def fits(sp, tp, tokens, query_weight, key_weight, conv_weight, attn_proj, taps, head):
    return (
        tp == 4
        and sp % 2 == 0
        and sp >= 6
        and tokens.shape[0] % (4 * 2 * WINDOW) == 0
        and tokens.shape[1] % LANES == 0
        and WINDOW == LANES
        and 2 * head == LANES
        and key_weight.shape[1] == head
        and query_weight.shape[1] == 4 * head
        and conv_weight.shape[1] == 4 * head
        and query_weight.shape[0] % LANES == 0
        and attn_proj.shape[1] % (2 * LANES) == 0
        and taps.shape[0] <= 31
    )


def fused(
    tokens,
    mix_gain,
    query_weight,
    key_weight,
    value_weight,
    conv_value_weight,
    conv_gate_weight,
    query_gain,
    key_gain,
    sink_logit,
    conv_taps,
    conv_gain,
    attn_proj,
    conv_proj,
):
    sp = lax.axis_size("sp")
    count, features = tokens.shape
    model = features * 4
    depth, width = query_weight.shape
    head = query_gain.shape[0]
    channels = conv_taps.shape[1]
    columns = attn_proj.shape[1]
    block = count // 4
    bf16, f32 = jnp.bfloat16, jnp.float32
    half_pad = 16
    stat = 2 * count // LANES
    padded_rows = count + 2 * WINDOW
    vmem, dma = pltpu.VMEM, pltpu.SemaphoreType.DMA
    inputs = dict(
        tokens=tokens,
        query_w=query_weight,
        key_w=key_weight.T,
        value_w=value_weight.T,
        conv_value_w=conv_value_weight,
        conv_gate_w=conv_gate_weight,
        attn_p=attn_proj,
        conv_p=conv_proj,
        mix_gain=mix_gain.reshape(-1, LANES),
        conv_gain=conv_gain.reshape(-1, LANES),
        query_gain=query_gain.reshape(1, -1),
        key_gain=key_gain.reshape(1, -1),
        sink_logit=sink_logit,
        conv_taps=conv_taps,
    )
    outputs = dict(
        near_out=vmem((block, model), f32),
        far_in=vmem((block, model), bf16),
    )
    scratch = dict(
        whole=vmem((4, count, features), bf16),
        normed=vmem((count, model), bf16),
        query_all=vmem((model, width), bf16),
        kv_own=vmem((2 * head, depth), bf16),
        kv_all=vmem((model, 2 * head), bf16),
        value_all=vmem((model, channels), bf16),
        gate_all=vmem((model, channels), bf16),
        proj_all=vmem((sp, 2, width + channels, columns // 2), bf16),
        proj_other=vmem((sp, 2, width + channels, columns // 2), bf16),
        taps=vmem(conv_taps.shape, f32),
        sinks=pltpu.SMEM(sink_logit.shape, f32),
        mix_rows=vmem((model // LANES, LANES), f32),
        conv_gains=vmem((channels // LANES, LANES), f32),
        query_gains=vmem((1, head), f32),
        key_gains=vmem((1, head), f32),
        head_gains=vmem((2, width), f32),
        spread_heads=vmem((width, width), bf16),
        band=vmem((2, LANES, LANES), f32),
        eye=vmem((LANES, LANES), f32),
        gated=vmem((channels // LANES, count + 2 * half_pad, LANES), f32),
        edge_out=vmem((2, half_pad, channels), bf16),
        edge_in=vmem((2, half_pad, channels), bf16),
        convolved=vmem((count, channels), f32),
        stat_out=vmem((stat, LANES), f32),
        stat_in=vmem((3, stat, LANES), f32),
        stat_rows=vmem((stat, LANES), f32),
        queries=vmem((count, width), bf16),
        query_part=vmem((2 * block, width), f32),
        key_low=vmem((padded_rows, LANES), bf16),
        key_high=vmem((padded_rows, LANES), bf16),
        value_low=vmem((padded_rows, 2 * LANES), bf16),
        value_high=vmem((padded_rows, 2 * LANES), bf16),
        halo_out=vmem((2, block, LANES), bf16),
        halo_in=vmem((2, WINDOW, LANES), bf16),
        mixers=vmem((count, width + channels), bf16),
        mixers_other=vmem((2, block, width + channels), bf16),
        far_out=vmem((sp, 2, block, columns // 2), bf16),
        local_sem=dma,
        ahead_sem=dma,
        send_sem=dma,
        recv_sem=dma((recv_count(sp),)),
    )
    near, far = pl.pallas_call(
        functools.partial(fused_kernel, sp, (*inputs, *outputs, *scratch)),
        out_shape=tuple(outputs.values()),
        in_specs=[pl.BlockSpec(memory_space=pltpu.HBM)] * len(inputs),
        out_specs=[pl.BlockSpec(memory_space=pltpu.VMEM)] * 2,
        scratch_shapes=list(scratch.values()),
        compiler_params=pltpu.CompilerParams(
            collective_id=1, has_side_effects=True, vmem_limit_bytes=60 * 2**20 + 2**19
        ),
    )(*inputs.values())
    return (near + far.astype(f32)).astype(bf16)


def on_device(
    tokens,
    mix_gain,
    query_weight,
    key_weight,
    value_weight,
    conv_value_weight,
    conv_gate_weight,
    query_gain,
    key_gain,
    sink_logit,
    conv_taps,
    conv_gain,
    attn_proj,
    conv_proj,
):
    if fits(
        lax.axis_size("sp"),
        lax.axis_size("tp"),
        tokens,
        query_weight,
        key_weight,
        conv_value_weight,
        attn_proj,
        conv_taps,
        query_gain.shape[0],
    ):
        return fused(
            tokens,
            mix_gain,
            query_weight,
            key_weight,
            value_weight,
            conv_value_weight,
            conv_gate_weight,
            query_gain,
            key_gain,
            sink_logit,
            conv_taps,
            conv_gain,
            attn_proj,
            conv_proj,
        )
    count = tokens.shape[0]
    shards = (query_weight, conv_value_weight, conv_gate_weight, key_weight, value_weight)
    whole, joined = gather_both(tokens, jnp.concatenate(shards, axis=1))
    normed = unit_rows(whole.astype(jnp.float32), mix_gain).astype(jnp.bfloat16)
    product = jnp.dot(normed, joined, preferred_element_type=jnp.float32)
    cuts = []
    for shard in shards[:-1]:
        cuts.append((cuts[-1] if cuts else 0) + shard.shape[1])
    query, conv_value, conv_gate, key_part, value_part = jnp.split(product, cuts, axis=1)
    head_size = query_gain.shape[0]
    local_kv = key_part.shape[1] // head_size
    group = query.shape[1] // head_size // local_kv
    queries = unit_rows(query.reshape(count, local_kv, group, head_size), query_gain).astype(
        jnp.bfloat16
    )
    keys_normed = (
        unit_rows(key_part.reshape(count, local_kv, head_size), key_gain)
        .astype(jnp.bfloat16)
        .reshape(count, -1)
    )
    values_cast = value_part.astype(jnp.bfloat16)
    gated = (conv_value * jax.nn.sigmoid(conv_gate)).astype(jnp.bfloat16)
    reach = (conv_taps.shape[0] - 1) // 2
    kv_width = keys_normed.shape[1]
    paired = jnp.concatenate([keys_normed, values_cast], axis=1)
    extended = padded(paired, (("sp", 0),), WINDOW)
    key_rows = extended[:, :kv_width]
    value_rows = extended[:, kv_width:]
    conv_rows = padded(gated, (("sp", 0),), reach)
    offset = lax.axis_index("sp") * count
    total = count * lax.axis_size("sp")
    span_rows = key_rows.shape[0]
    attended = attend(
        queries,
        key_rows.reshape(span_rows, local_kv, head_size),
        value_rows.reshape(span_rows, local_kv, head_size),
        sink_logit,
        offset,
        total,
    )
    convolved = depthwise(conv_rows, conv_taps, count)
    channels, tp = conv_taps.shape[1], lax.axis_size("tp")
    local_mean = jnp.mean(convolved, axis=1)
    local_square = jnp.sum(jnp.square(convolved - local_mean[:, None]), axis=1)
    slot = (jnp.arange(tp) == lax.axis_index("tp")).astype(jnp.float32)[:, None, None]
    every = lax.psum(slot * jnp.stack([local_mean, local_square])[None], "tp")
    center = jnp.mean(every[:, 0], axis=0)
    spread = jnp.sum(every[:, 1] + channels * jnp.square(every[:, 0] - center), axis=0)
    spread = spread / (channels * tp)
    centered = convolved - center[:, None]
    featured = jax.nn.silu(centered * lax.rsqrt(spread[:, None] + EPSILON) * conv_gain).astype(
        jnp.bfloat16
    )
    stacked, _ = lax.optimization_barrier((jnp.concatenate([attn_proj, conv_proj], axis=0), joined))
    proj_full = lax.all_gather(stacked, "sp", axis=1, tiled=True)
    mixers = jnp.concatenate([attended, featured], axis=1)
    partial = jnp.dot(mixers, proj_full, preferred_element_type=jnp.float32).astype(jnp.bfloat16)
    return lax.psum_scatter(partial, "tp", scatter_dimension=0, tiled=True)


def solution(mesh):
    placed = (
        P("sp", "tp"),
        P(),
        P("sp", "tp"),
        P("sp", "tp"),
        P("sp", "tp"),
        P("sp", "tp"),
        P("sp", "tp"),
        P(),
        P(),
        P("tp"),
        P(None, "tp"),
        P("tp"),
        P("tp", "sp"),
        P("tp", "sp"),
    )
    return jax.shard_map(
        on_device, mesh=mesh, in_specs=placed, out_specs=P(("sp", "tp"), None), check_vma=False
    )
```
